32 devices in a mesh: ep: 8 (over z, x), tp: 4 (over y, core).
Axes of the slice: x: 2, y: 2, z: 4, core: 2. Of those that a mesh axis runs over, the one named last changes fastest.
Arguments:
- memory_query_matrix: bfloat16 [4096, 1024], P('ep', 'tp'), may hold values from -0.59765625 to 2
- memory_key_matrix: bfloat16 [4096, 1024], P('ep', 'tp'), may hold values from -0.59765625 to 2
- memory_value_matrix: bfloat16 [4096, 1024], P('ep', 'tp'), may hold values from -6 to 6
- input_gate_logits: float32 [4, 4096], P('tp', 'ep'), may hold values from -6 to 260
- forget_gate_logits: float32 [4, 4096], P('tp', 'ep'), may hold values from -1 to 20
- forget_log_boosts: float32 [4, 4096], P('tp', 'ep'), may hold values from -0.7 to 0
- head_norm_scale: float32 [1024], P('tp'), may hold values from 0.1 to 1.9
- memory_output_matrix: bfloat16 [1024, 2048], replicated, may hold values from -0.1875 to 0.1875
- projection_norm_scale: float32 [2048], replicated, may hold values from 0.1 to 1.9
- second_batch_rows: bfloat16 [6144, 2048], P(('ep', 'tp')), may hold values from -6 to 6
- expert_prenorm_scale: float32 [2048], replicated, may hold values from 0.1 to 1.9
- selected_expert_index: int32 [6144, 2], P(('ep', 'tp')), may hold values from 0 to 7, all different within a row; in each aligned block of 192 rows (0 to 191, 192 to 383, ...) at most 96 rows name the same one
- group_route_probability: float32 [6144], P(('ep', 'tp')), may hold values from 0.2 to 1
- expert_choice_scores: float32 [6144, 2], P(('ep', 'tp')), may hold values from -6 to 6
- expert_gate_matrix: bfloat16 [8, 2048, 512], P('ep'), may hold values from -0.125 to 0.125
- expert_up_matrix: bfloat16 [8, 2048, 512], P('ep'), may hold values from -0.125 to 0.125
- expert_down_matrix: bfloat16 [8, 512, 2048], P('ep'), may hold values from -0.25 to 0.25
Outputs:
- mixed_rows: bfloat16 [4096, 2048], P(('ep', 'tp'))
- routed_rows: bfloat16 [6144, 2048], P(('ep', 'tp'))
The draws below stay inside these ranges and needn't reach their ends.
Inputs may be any that keep to these rules, and one draw needn't show every extreme that they name: `selected_expert_index`: each row names 2 different experts; among the rows of one device no expert is named more than 96 times, and in some device one expert is named exactly that often.
All inputs are finite; a program needn't handle non-finite values.
Results may differ from the reference program's by a relative error of at most 0.013.
Values may be sent and summed in bfloat16 or wider, within the bound.
A program may use at most 128 MiB of HBM per device.

```python
import math
import jax
import jax.numpy as jnp
import numpy as np
from jax import lax

D = 2048
HEADS = 4
HEAD_SIZE = 256
CELL_WIDTH = 1024
SPAN = 128
MIX_DEV = 512
SEQ_LEN = 4096
EXPERT_HIDDEN = 512
TOPK = 2
ROUTED_DEV = 192
ROUTED = 6144
EXPERTS = 8
CAPACITY = 96


def draw_forget_gate_logits(key, part):
    keys = jax.random.split(jax.random.fold_in(key, 71), 3)
    order = jax.random.permutation(keys[0], HEADS)
    quick = HEADS // 2
    slow_bias = math.log(SEQ_LEN) + 0.6
    bias = jnp.where(order < quick, 4.2, slow_bias).astype(jnp.float32)
    pieces = SEQ_LEN // MIX_DEV
    offset = jax.random.uniform(keys[1], (HEADS, pieces, 1), jnp.float32, -0.7, 0.7)
    offset = jnp.broadcast_to(offset, (HEADS, pieces, MIX_DEV)).reshape(HEADS, SEQ_LEN)
    noise = jnp.clip(jax.random.normal(keys[2], (HEADS, SEQ_LEN), jnp.float32), -4.0, 4.0)
    return bias[:, None] + offset + noise


def draw_forget_log_boosts(key, part):
    keys = jax.random.split(jax.random.fold_in(key, 83), 2)
    spots = jax.random.randint(keys[0], (HEADS, 3), 0, SEQ_LEN)
    depth = jax.random.uniform(keys[1], (HEADS, 3), jnp.float32, -0.69, -0.22)
    places = jnp.arange(SEQ_LEN, dtype=jnp.int32)
    hits = places[None, None, :] == spots[:, :, None]
    return jnp.min(jnp.where(hits, depth[:, :, None], 0.0), axis=1)


def draw_input_gate_logits(key, part):
    keys = jax.random.split(jax.random.fold_in(key, 97), 1)
    return jnp.clip(jax.random.normal(keys[0], (HEADS, SEQ_LEN), jnp.float32), -6.0, 6.0)


def shard_levels(stream_key, dims, shards, least, high):
    def one(dim, shards_of):
        heights = jax.random.uniform(jax.random.fold_in(jax.random.fold_in(stream_key, 6), dim), (shards_of,), jnp.float32, least / len(shards), high / len(shards))
        return jnp.repeat(jnp.exp(heights), dims[dim] // shards_of).reshape((-1,) + (1,) * (len(dims) - dim - 1))

    loudness = one(*shards[0])
    for cut in shards[1:]:
        loudness = loudness * one(*cut)
    return loudness


def shared_out(own_key, own, number, rows, count, top, most, skew):
    order = jax.random.permutation(own_key, count)
    packed, ordinary = portions_of(count, rows * top, most, skew, True), portions_of(count, rows * top, most, skew, False)
    places = jnp.arange(count)

    def named(sizes, turn):
        used = int((sizes > 0).sum())
        fixed = max(1, used // 4)
        passed = fixed + (places - fixed + turn * (used - fixed)) % max(1, count - fixed)
        return jnp.zeros((count,), jnp.int32).at[order[jnp.where(places < fixed, places, passed)]].set(jnp.asarray(sizes, jnp.int32))

    sizes = jnp.where(number % 4 == 0, named(packed, number // 4), named(ordinary, number - number // 4 - 1))
    mixed = jax.random.permutation(jax.random.fold_in(own, 3), count)
    giver, sink = mixed[0:count // 2 * 2:2], mixed[1:count // 2 * 2:2]
    slack = jnp.minimum(sizes[giver] - 1, most - sizes[sink]) // 2
    slack = jnp.where((giver == order[0]) | (sink == order[0]) | (sizes[sink] == 0), 0, jnp.maximum(slack, 0))
    passed = jax.random.randint(jax.random.fold_in(own, 4), (count // 2,), 0, 1 << 20) % (slack + 1)
    sizes = sizes.at[giver].add(-passed).at[sink].add(passed)
    items = jnp.searchsorted(jnp.cumsum(sizes), jnp.arange(rows * top), side="right").astype(jnp.int32)
    table = items.reshape(top, rows).T
    table = table[jax.random.permutation(jax.random.fold_in(own, 1), rows)]
    turn = jax.random.randint(jax.random.fold_in(own, 2), (rows, 1), 0, top)
    return jnp.take_along_axis(table, (jnp.arange(top)[None, :] + turn) % top, axis=1)


def portions_of(count, total, most, lean, full):
    portions = [(1 << 20) // math.isqrt(standing ** lean) + 1 for standing in range(1, count + 1)]
    largest = most if full else min(most, max(-(-total // count), total * portions[0] // sum(portions)))
    least = 1 if total - largest >= count - 1 else 0
    given, surplus = [largest] + [least] * (count - 1), total - largest - least * (count - 1)
    while surplus > 0:
        free = [i for i in range(1, count) if given[i] < largest] or [i for i in range(1, count) if given[i] < most]
        mass, left = sum([portions[i] for i in free]), surplus
        for i in free:
            extra = min(most - given[i], max(1, left * portions[i] // mass), surplus)
            given[i] = given[i] + extra
            surplus = surplus - extra
    return np.array(given)


def bell_draw(own_key, dims, deviation, limit, cuts=(), held_as=jnp.bfloat16):
    array = deviation * jax.random.normal(own_key, dims, jnp.float32)
    if cuts:
        array = array * shard_levels(own_key, dims, cuts, -0.22, 0.18)
    return jnp.clip(array, -limit, limit).astype(held_as)


def setup_inputs(seed: int = 0) -> dict:
    key_of = jax.random.split(jax.random.key(seed), 18)
    memory_query_matrix = jnp.clip(-0.59765625 + 2.5976562 * jax.random.uniform(key_of[0], (SEQ_LEN, CELL_WIDTH), jnp.float32) ** shard_levels(key_of[0], (SEQ_LEN, CELL_WIDTH), ((0, 8), (1, 4)), -0.2, 0.2), -0.59765625, 2.0).astype(jnp.bfloat16)
    memory_key_matrix = jnp.clip(-0.59765625 + 2.5976562 * jax.random.uniform(key_of[1], (SEQ_LEN, CELL_WIDTH), jnp.float32) ** shard_levels(key_of[1], (SEQ_LEN, CELL_WIDTH), ((0, 8), (1, 4)), -0.2, 0.2), -0.59765625, 2.0).astype(jnp.bfloat16)
    memory_value_matrix = bell_draw(key_of[2], (SEQ_LEN, CELL_WIDTH), 1.0, 6.0, ((0, 8), (1, 4)))
    input_gate_logits = draw_input_gate_logits(jax.random.fold_in(key_of[17], 71), 0)
    forget_gate_logits = draw_forget_gate_logits(jax.random.fold_in(key_of[17], 71), 0)
    forget_log_boosts = draw_forget_log_boosts(jax.random.fold_in(key_of[17], 71), 0)
    head_norm_scale = jnp.clip(1.0 + 0.18 * jax.random.normal(key_of[6], (CELL_WIDTH,), jnp.float32), 0.1, 1.9)
    memory_output_matrix = bell_draw(key_of[7], (CELL_WIDTH, D), CELL_WIDTH ** -0.5, 0.1875)
    projection_norm_scale = jnp.clip(1.0 + 0.18 * jax.random.normal(key_of[8], (D,), jnp.float32), 0.1, 1.9)
    second_batch_rows = bell_draw(key_of[9], (ROUTED, D), 1.0, 6.0, ((0, 32),))
    expert_prenorm_scale = jnp.clip(1.0 + 0.18 * jax.random.normal(key_of[10], (D,), jnp.float32), 0.1, 1.9)
    selected_expert_index_keys = jax.random.split(jax.random.fold_in(key_of[11], 1), ROUTED // ROUTED_DEV)
    selected_expert_index_turns = jax.random.permutation(jax.random.fold_in(key_of[11], 3), ROUTED // ROUTED_DEV)
    selected_expert_index = jax.vmap(lambda own, number: shared_out(jax.random.fold_in(key_of[11], 2), own, number, ROUTED_DEV, EXPERTS, TOPK, CAPACITY, 1))(selected_expert_index_keys, selected_expert_index_turns).reshape((ROUTED, TOPK))
    group_route_probability = jnp.clip(0.2 + 0.8 * jax.random.uniform(key_of[12], (ROUTED,), jnp.float32) ** shard_levels(key_of[12], (ROUTED,), ((0, 32),), -0.2, 0.2), 0.2, 1.0)
    expert_choice_scores = bell_draw(key_of[13], (ROUTED, TOPK), 1.5, 6.0, ((0, 32),), jnp.float32)
    expert_gate_matrix = bell_draw(key_of[14], (EXPERTS, D, EXPERT_HIDDEN), D ** -0.5, 0.125, ((0, 8),))
    expert_up_matrix = bell_draw(key_of[15], (EXPERTS, D, EXPERT_HIDDEN), D ** -0.5, 0.125, ((0, 8),))
    expert_down_matrix = bell_draw(key_of[16], (EXPERTS, EXPERT_HIDDEN, D), EXPERT_HIDDEN ** -0.5, 0.25, ((0, 8),))
    return dict(memory_query_matrix=memory_query_matrix, memory_key_matrix=memory_key_matrix, memory_value_matrix=memory_value_matrix, input_gate_logits=input_gate_logits, forget_gate_logits=forget_gate_logits, forget_log_boosts=forget_log_boosts, head_norm_scale=head_norm_scale, memory_output_matrix=memory_output_matrix, projection_norm_scale=projection_norm_scale, second_batch_rows=second_batch_rows, expert_prenorm_scale=expert_prenorm_scale, selected_expert_index=selected_expert_index, group_route_probability=group_route_probability, expert_choice_scores=expert_choice_scores, expert_gate_matrix=expert_gate_matrix, expert_up_matrix=expert_up_matrix, expert_down_matrix=expert_down_matrix)


floor_log = -1e+30
norm_eps = 1e-06
exact = lax.Precision.HIGHEST

def rms_scale(values, gain):
    squares = lax.optimization_barrier(jnp.mean(values * values, axis=-1, keepdims=True))
    return values * lax.rsqrt(squares + norm_eps) * gain

def span_step(carry, inputs):
    memory, normer, stabil = carry
    query, keyrow, valrow, in_gate, log_retain_factor = inputs
    key_scale = query.shape[-1] ** (-0.5)
    length = query.shape[1]
    causal = jnp.tril(jnp.ones((length, length), dtype=bool))
    cumulative = jnp.cumsum(log_retain_factor, axis=-1)
    decay_map = cumulative[:, :, None] - cumulative[:, None, :] + in_gate[:, None, :]
    decay_map = jnp.where(causal[None], decay_map, -jnp.inf)
    carried = cumulative + stabil[:, None]
    peak = jnp.maximum(carried, lax.optimization_barrier(jnp.max(decay_map, axis=-1)))
    within = jnp.exp(decay_map - peak[:, :, None])
    across = jnp.exp(carried - peak)
    qfloat = query.astype(jnp.float32)
    products = jnp.einsum('htd,hsd->hts', qfloat, keyrow.astype(jnp.float32))
    scores = products * key_scale * within
    denominator = lax.optimization_barrier(jnp.sum(scores, axis=-1)) + across * jnp.einsum('hd,htd->ht', normer, qfloat, precision=exact)
    weights = scores.astype(jnp.bfloat16)
    numerator = jnp.einsum('hts,hsd->htd', weights.astype(jnp.float32), valrow.astype(jnp.float32))
    numerator = numerator + across[:, :, None] * jnp.einsum('hed,htd->hte', memory, qfloat, precision=exact)
    output = numerator / jnp.maximum(jnp.abs(denominator), jnp.exp(-peak))[:, :, None]
    span_end = cumulative[:, -1]
    gap_log = span_end[:, None] - cumulative + in_gate
    new_peak = jnp.maximum(span_end + stabil, lax.optimization_barrier(jnp.max(gap_log, axis=-1)))
    shrink = jnp.exp(span_end + stabil - new_peak)
    spread = jnp.exp(gap_log - new_peak[:, None]) * key_scale
    keys_weighted = keyrow.astype(jnp.float32) * spread[:, :, None]
    memory = shrink[:, None, None] * memory + jnp.einsum('hse,hsd->hed', valrow.astype(jnp.float32), keys_weighted, precision=exact)
    normer = shrink[:, None] * normer + lax.optimization_barrier(jnp.sum(keys_weighted, axis=1))
    return ((memory, normer, new_peak), output)

def reference(memory_query_matrix, memory_key_matrix, memory_value_matrix, input_gate_logits, forget_gate_logits, forget_log_boosts, head_norm_scale, memory_output_matrix, projection_norm_scale, second_batch_rows, expert_prenorm_scale, selected_expert_index, group_route_probability, expert_choice_scores, expert_gate_matrix, expert_up_matrix, expert_down_matrix):
    spans = SEQ_LEN // SPAN

    def by_head(rows):
        return rows.reshape(SEQ_LEN, HEADS, HEAD_SIZE).transpose(1, 0, 2)

    def to_spans(values):
        shaped = values.reshape((HEADS, spans, SPAN) + values.shape[2:])
        return jnp.moveaxis(shaped, 1, 0)
    log_retain_factor = jax.nn.log_sigmoid(forget_gate_logits) + forget_log_boosts
    start = (jnp.zeros((HEADS, HEAD_SIZE, HEAD_SIZE), jnp.float32), jnp.zeros((HEADS, HEAD_SIZE), jnp.float32), jnp.full((HEADS,), floor_log, jnp.float32))
    inputs = (to_spans(by_head(memory_query_matrix)), to_spans(by_head(memory_key_matrix)), to_spans(by_head(memory_value_matrix)), to_spans(input_gate_logits), to_spans(log_retain_factor))
    _, cells = lax.scan(span_step, start, inputs)
    cells = jnp.moveaxis(cells, 0, 1).reshape(HEADS, SEQ_LEN, HEAD_SIZE)
    scaled = (cells * head_norm_scale.reshape(HEADS, 1, HEAD_SIZE)).astype(jnp.bfloat16)
    head_out = scaled.transpose(1, 0, 2).reshape(SEQ_LEN, CELL_WIDTH)
    projected = jnp.dot(head_out, memory_output_matrix, preferred_element_type=jnp.float32)
    mixed_rows = rms_scale(projected, projection_norm_scale).astype(jnp.bfloat16)
    ffn_rows = rms_scale(second_batch_rows.astype(jnp.float32), expert_prenorm_scale).astype(jnp.bfloat16)
    flat_ids = selected_expert_index.reshape(-1).astype(jnp.int32)
    owners = jnp.repeat(jnp.arange(ROUTED, dtype=jnp.int32), TOPK)
    onehot = (flat_ids[:, None] == jnp.arange(EXPERTS, dtype=jnp.int32)[None, :]).astype(jnp.int32)
    rank = lax.optimization_barrier(jnp.sum((jnp.cumsum(onehot, axis=0) - onehot) * onehot, axis=1)).astype(jnp.int32)
    slots = ROUTED // ROUTED_DEV * CAPACITY
    route_weight = group_route_probability[:, None] * jax.nn.softmax(expert_choice_scores, axis=-1)
    members = jnp.zeros((EXPERTS, slots), jnp.int32).at[flat_ids, rank].set(owners)
    shares = jnp.zeros((EXPERTS, slots), jnp.float32).at[flat_ids, rank].set(route_weight.reshape(-1))

    def one_expert(total, inputs):
        w_gate, w_up, w_down, member_rows, member_shares = inputs
        chosen = ffn_rows[member_rows]
        gate = jnp.dot(chosen, w_gate, preferred_element_type=jnp.float32)
        upper = jnp.dot(chosen, w_up, preferred_element_type=jnp.float32)
        hidden = (jax.nn.silu(gate) * upper).astype(jnp.bfloat16)
        answer = jnp.dot(hidden, w_down, preferred_element_type=jnp.float32).astype(jnp.bfloat16)
        total = total.at[member_rows].add(member_shares[:, None] * answer.astype(jnp.float32))
        return (total, None)
    total, _ = lax.scan(one_expert, jnp.zeros((ROUTED, D), jnp.float32), (expert_gate_matrix, expert_up_matrix, expert_down_matrix, members, shares))
    routed_rows = total.astype(jnp.bfloat16)
    return (mixed_rows, routed_rows)
```

```python
import functools

import jax
import jax.numpy as jnp
from jax import lax
from jax.experimental import pallas as pl
from jax.experimental.pallas import tpu as pltpu
from jax.sharding import PartitionSpec as P

FLOOR = -1e30
EPS = 1e-06
MESH = pl.DeviceIdType.MESH
F32 = jnp.float32
BF16 = jnp.bfloat16


def rms(values, gain):
    squares = jnp.mean(values * values, axis=-1, keepdims=True)
    return values * lax.rsqrt(squares + EPS) * gain


def dot(a, b, dims=((1,), (0,)), precision=None):
    return lax.dot_general(a, b, (dims, ((), ())), preferred_element_type=F32, precision=precision)


def join(early, late):
    total_e, peak_e, mem_e, nor_e = early
    total_l, peak_l, mem_l, nor_l = late
    peak = jnp.maximum(total_l + peak_e, peak_l)
    fe = jnp.exp(total_l + peak_e - peak)
    fl = jnp.exp(peak_l - peak)
    return (total_e + total_l, peak, fe * mem_e + fl * mem_l, fe * nor_e + fl * nor_l)


def kernel(
    n, nt, cap,
    q_ref, k_ref, v_ref, ig_ref, fg_ref, fb_ref, hs_ref, wo_hbm, ps_ref,
    x_ref, es_ref, ids_ref, grp_ref, sc_ref, wg_hbm, wu_hbm, wd_hbm,
    mixed_ref, routed_ref,
    wg, wu, wd, wo, out, recv, ans, back, ffn, acc,
    cpair, spair, cgrp, sgrp, ent, head, pout, prec,
    wsem, d_ss, d_rs, a_ss, a_rs, c1s, c1r, s1s, s1r, c2s, c2r, s2s, s2r, p_ss, p_rs,
):
    me = lax.axis_index("ep")
    tp = lax.axis_index("tp")
    groups = n // 2
    grp = me // 2
    par = lax.rem(me, 2)
    partner = me + 1 - 2 * par
    tokens, width = x_ref.shape
    length, hd = q_ref.shape
    rows = mixed_ref.shape[0]

    barrier = pltpu.get_barrier_semaphore()

    def greet(i, c):
        pl.semaphore_signal(barrier, inc=1, device_id=(lax.rem(me + i, n), tp), device_id_type=MESH)
        return c

    lax.fori_loop(1, n, greet, 0)
    for j in range(1, nt):
        pl.semaphore_signal(barrier, inc=1, device_id=(me, lax.rem(tp + j, nt)), device_id_type=MESH)

    loads = [
        pltpu.make_async_copy(wg_hbm.at[0], wg, wsem.at[0]),
        pltpu.make_async_copy(wu_hbm.at[0], wu, wsem.at[1]),
        pltpu.make_async_copy(wd_hbm.at[0], wd, wsem.at[2]),
        pltpu.make_async_copy(wo_hbm.at[pl.ds(pl.multiple_of(tp * hd, hd), hd)], wo, wsem.at[3]),
    ]
    for load in loads:
        load.start()

    fg = fg_ref[...]
    lk = jnp.minimum(fg, 0.0) - jnp.log1p(jnp.exp(-jnp.abs(fg))) + fb_ref[...]
    rid = lax.broadcasted_iota(jnp.int32, (length, length), 0)
    cid = lax.broadcasted_iota(jnp.int32, (length, length), 1)
    upper = (rid <= cid).astype(F32)
    b_row = dot(jnp.broadcast_to(lk, (8, length)), upper, precision=lax.Precision.HIGHEST)[0:1]
    i_row = ig_ref[...]
    last = b_row[:, length - 1 : length]
    g_row = last - b_row + i_row
    m_loc = jnp.max(g_row, axis=-1, keepdims=True)
    which = lax.broadcasted_iota(jnp.int32, (128, length), 0)
    cols = jnp.where(which == 0, b_row, g_row).T
    b_col = cols[:, 0:1]
    g_col = cols[:, 1:2]
    kw = k_ref[...].astype(F32) * (jnp.exp(g_col - m_loc) * (hd**-0.5))
    c_loc = dot(kw.astype(BF16), v_ref[...], ((0,), (0,)))
    n_loc = jnp.sum(kw, axis=0, keepdims=True)
    stat_id = lax.broadcasted_iota(jnp.int32, (8, hd), 0)

    def stats(total, peak, nor):
        return jnp.where(stat_id == 0, nor, jnp.where(stat_id == 1, peak, total))

    cpair[par] = c_loc.astype(BF16)
    spair[par] = stats(last, m_loc, n_loc)

    pl.semaphore_wait(barrier, n - 1 + nt - 1)

    def pair_copies():
        return [
            pltpu.make_async_remote_copy(
                src_ref=cpair.at[par], dst_ref=cpair.at[par], send_sem=c1s, recv_sem=c1r,
                device_id=(partner, tp), device_id_type=MESH),
            pltpu.make_async_remote_copy(
                src_ref=spair.at[par], dst_ref=spair.at[par], send_sem=s1s, recv_sem=s1r,
                device_id=(partner, tp), device_id_type=MESH),
        ]

    for copy in pair_copies():
        copy.start()

    ffn[...] = rms(x_ref[...].astype(F32), es_ref[...]).astype(BF16)
    ids = ids_ref[...]
    first, second = ids[:, 0:1], ids[:, 1:2]
    lane_e = lax.broadcasted_iota(jnp.int32, (tokens, n), 1)
    named = ((lane_e == first) | (lane_e == second)).astype(F32)
    tr = lax.broadcasted_iota(jnp.int32, (tokens, tokens), 0)
    tc = lax.broadcasted_iota(jnp.int32, (tokens, tokens), 1)
    rank = dot((tc < tr).astype(BF16), named.astype(BF16))
    slot_a = first * cap + jnp.sum(jnp.where(lane_e == first, rank, 0.0), axis=1, keepdims=True).astype(jnp.int32)
    slot_b = second * cap + jnp.sum(jnp.where(lane_e == second, rank, 0.0), axis=1, keepdims=True).astype(jnp.int32)
    score = sc_ref[...]
    ex = jnp.exp(score - jnp.max(score, axis=-1, keepdims=True))
    route = grp_ref[...] * (ex / jnp.sum(ex, axis=-1, keepdims=True))
    rw_a, rw_b = route[:, 0:1], route[:, 1:2]
    lane_c = lax.broadcasted_iota(jnp.int32, (tokens, cap), 1)

    def pack(e):
        lane = lane_c + e * cap
        place = ((lane == slot_a) | (lane == slot_b)).astype(BF16)
        out[e] = dot(place, ffn[...], ((0,), (0,))).astype(BF16)

    def offset(i):
        return n // 2 + jnp.where(lax.rem(i, 2) == 0, i // 2, -((i + 1) // 2))

    def dispatch_copy(e):
        return pltpu.make_async_remote_copy(
            src_ref=out.at[e], dst_ref=recv.at[me], send_sem=d_ss.at[e], recv_sem=d_rs.at[me],
            device_id=(e, tp), device_id_type=MESH)

    def dispatch_arrival(s):
        return pltpu.make_async_remote_copy(
            src_ref=out.at[s], dst_ref=recv.at[s], send_sem=d_ss.at[s], recv_sem=d_rs.at[s],
            device_id=(s, tp), device_id_type=MESH)

    def answer_copy(s):
        return pltpu.make_async_remote_copy(
            src_ref=ans.at[s], dst_ref=back.at[me], send_sem=a_ss.at[s], recv_sem=a_rs.at[me],
            device_id=(s, tp), device_id_type=MESH)

    def answer_arrival(e):
        return pltpu.make_async_remote_copy(
            src_ref=ans.at[e], dst_ref=back.at[e], send_sem=a_ss.at[e], recv_sem=a_rs.at[e],
            device_id=(e, tp), device_id_type=MESH)

    for copy in pair_copies():
        copy.wait_send()
    def pair_arrival():
        return [
            pltpu.make_async_remote_copy(
                src_ref=cpair.at[1 - par], dst_ref=cpair.at[1 - par], send_sem=c1s, recv_sem=c1r,
                device_id=(partner, tp), device_id_type=MESH),
            pltpu.make_async_remote_copy(
                src_ref=spair.at[1 - par], dst_ref=spair.at[1 - par], send_sem=s1s, recv_sem=s1r,
                device_id=(partner, tp), device_id_type=MESH),
        ]

    for copy in pair_arrival():
        copy.wait_recv()

    def unpack(c, s):
        return (s[2:3], s[1:2], c.astype(F32), s[0:1])

    both = join(unpack(cpair[0], spair[0]), unpack(cpair[1], spair[1]))
    cgrp[grp] = both[2].astype(BF16)
    sgrp[grp] = stats(both[0], both[1], both[3])

    def group_copies(g):
        to = (g * 2 + par, tp)
        return [
            pltpu.make_async_remote_copy(
                src_ref=cgrp.at[grp], dst_ref=cgrp.at[grp], send_sem=c2s.at[g], recv_sem=c2r.at[grp],
                device_id=to, device_id_type=MESH),
            pltpu.make_async_remote_copy(
                src_ref=sgrp.at[grp], dst_ref=sgrp.at[grp], send_sem=s2s.at[g], recv_sem=s2r.at[grp],
                device_id=to, device_id_type=MESH),
        ]

    def group_arrivals(g):
        at = (g * 2 + par, tp)
        return [
            pltpu.make_async_remote_copy(
                src_ref=cgrp.at[g], dst_ref=cgrp.at[g], send_sem=c2s.at[g], recv_sem=c2r.at[g],
                device_id=at, device_id_type=MESH),
            pltpu.make_async_remote_copy(
                src_ref=sgrp.at[g], dst_ref=sgrp.at[g], send_sem=s2s.at[g], recv_sem=s2r.at[g],
                device_id=at, device_id_type=MESH),
        ]

    def send_group(g, c):
        for copy in group_copies(g):
            copy.start()
        return c

    lax.fori_loop(grp + 1, groups, send_group, 0)

    def send_tokens(i, c):
        e = lax.rem(me + offset(i), n)
        pack(e)
        dispatch_copy(e).start()
        return c

    lax.fori_loop(0, n - 1, send_tokens, 0)
    pack(me)
    for load in loads:
        load.wait()

    def expert(chosen):
        gate = dot(chosen, wg[...])
        up = dot(chosen, wu[...])
        hidden = (gate / (1.0 + jnp.exp(-gate)) * up).astype(BF16)
        return dot(hidden, wd[...]).astype(BF16)

    ans[me] = expert(out[me])

    ent[...] = jnp.zeros(ent.shape, F32)
    row1 = jnp.zeros((1, hd), F32)

    def enter(g, carry):
        total, peak, nor = carry
        for copy in group_arrivals(g):
            copy.wait_recv()
        total, peak, mem, nor = join((total, peak, ent[...], nor), unpack(cgrp[g], sgrp[g]))
        ent[...] = mem
        return total, peak, nor

    total, peak, nor = lax.fori_loop(0, grp, enter, (row1, row1 + FLOOR, row1))
    joined = join((total, peak, ent[...], nor), unpack(cpair[0], spair[0]))
    odd = par == 1
    m_in = jnp.where(odd, joined[1], peak)
    n_in = jnp.where(odd, joined[3], nor)
    c_in = jnp.where(odd, joined[2], ent[...])

    carried = b_col + m_in[:, 0:1]
    decay = jnp.where(cid <= rid, b_col - b_row + i_row, -jnp.inf)
    peaks = jnp.maximum(carried, jnp.max(decay, axis=-1, keepdims=True))
    across = jnp.exp(carried - peaks)
    scores = dot(q_ref[...], k_ref[...], ((1,), (1,))) * (hd**-0.5) * jnp.exp(decay - peaks)
    qf = q_ref[...].astype(F32)
    den = jnp.sum(scores, axis=-1, keepdims=True) + across * jnp.sum(qf * n_in, axis=-1, keepdims=True)
    num = dot(scores.astype(BF16), v_ref[...]) + across * dot(q_ref[...], c_in.astype(BF16))
    cell = num / jnp.maximum(jnp.abs(den), jnp.exp(-peaks))
    head[...] = (cell * hs_ref[...]).astype(BF16)

    def part_copy(j):
        return pltpu.make_async_remote_copy(
            src_ref=pout.at[j], dst_ref=prec.at[tp], send_sem=p_ss.at[j], recv_sem=p_rs.at[tp],
            device_id=(me, j), device_id_type=MESH)

    def part_arrival(j):
        return pltpu.make_async_remote_copy(
            src_ref=pout.at[j], dst_ref=prec.at[j], send_sem=p_ss.at[j], recv_sem=p_rs.at[j],
            device_id=(me, j), device_id_type=MESH)

    def project(j):
        pout[j] = dot(head[pl.ds(pl.multiple_of(j * rows, rows), rows), :], wo[...]).astype(BF16)

    def send_part(i, c):
        j = lax.rem(tp + i, nt)
        project(j)
        part_copy(j).start()
        return c

    lax.fori_loop(1, nt, send_part, 0)
    project(tp)

    def serve(i, c):
        s = lax.rem(me - offset(i) + n, n)
        dispatch_arrival(s).wait_recv()
        ans[s] = expert(recv[s])
        answer_copy(s).start()
        return c

    lax.fori_loop(0, n - 1, serve, 0)

    def mix(i, total):
        j = lax.rem(tp + i, nt)
        part_arrival(j).wait_recv()
        return total + prec[j].astype(F32)

    projected = pout[tp].astype(F32)
    for i in range(1, nt):
        projected = mix(i, projected)
    mixed_ref[...] = rms(projected, ps_ref[...]).astype(BF16)

    def weigh(e, block):
        lane = lane_c + e * cap
        w = jnp.where(lane == slot_a, rw_a, jnp.where(lane == slot_b, rw_b, 0.0))
        high = w.astype(BF16)
        low = (w - high.astype(F32)).astype(BF16)
        return dot(high, block) + dot(low, block)

    acc[...] = weigh(me, ans[me])

    def collect(i, c):
        e = lax.rem(me + offset(i), n)
        answer_arrival(e).wait_recv()
        acc[...] += weigh(e, back[e])
        return c

    lax.fori_loop(0, n - 1, collect, 0)
    routed_ref[...] = acc[...].astype(BF16)

    def finish(i, c):
        e = lax.rem(me + i, n)
        dispatch_copy(e).wait_send()
        answer_copy(e).wait_send()
        return c

    lax.fori_loop(1, n, finish, 0)

    def finish_group(g, c):
        for copy in group_copies(g):
            copy.wait_send()
        return c

    lax.fori_loop(grp + 1, groups, finish_group, 0)
    for i in range(1, nt):
        part_copy(lax.rem(tp + i, nt)).wait_send()


def plane_kernel(
    n, nt, cap, nc,
    q_ref, k_ref, v_ref, ig_ref, fg_ref, fb_ref, hs_ref, wo_hbm, ps_ref,
    x_ref, es_ref, ids_ref, grp_ref, sc_ref, wg_hbm, wu_hbm, wd_hbm,
    mixed_ref, routed_ref,
    wg, wu, wd, wo, tok, info, chosen, hid, ans, cin, rout, rin, acc,
    cpair, spair, cgrp, sgrp, cpre, spre, ent, num, stat, head, pout, prec,
    wsem, x_ss, y_ss, k_ss, w_rs, t_ss, t_rs, i_ss, i_rs, c_ss, c_rs, r_ss, r_rs,
    c1s, c1r, s1s, s1r, c2s, c2r, s2s, s2r, p_ss, p_rs,
):
    me = lax.axis_index("ep")
    tp = lax.axis_index("tp")
    groups = n // 2
    z = me // 2
    par = lax.rem(me, 2)
    partner = me + 1 - 2 * par
    other = tp + 1 - 2 * lax.rem(tp, 2)
    tokens, width = x_ref.shape
    length, hd = q_ref.shape
    rows = mixed_ref.shape[0]
    cw = width // nc
    pieces = 3 * nc

    def remote(src, dst, ss, rs, to):
        return pltpu.make_async_remote_copy(
            src_ref=src, dst_ref=dst, send_sem=ss, recv_sem=rs, device_id=to, device_id_type=MESH)

    barrier = pltpu.get_barrier_semaphore()

    def greet(i, c):
        pl.semaphore_signal(barrier, inc=1, device_id=(lax.rem(me + i, n), tp), device_id_type=MESH)
        return c

    lax.fori_loop(1, n, greet, 0)
    for j in range(1, nt):
        pl.semaphore_signal(barrier, inc=1, device_id=(me, lax.rem(tp + j, nt)), device_id_type=MESH)

    loads = [
        pltpu.make_async_copy(wg_hbm.at[0], wg.at[0], wsem.at[0]),
        pltpu.make_async_copy(wu_hbm.at[0], wu.at[0], wsem.at[1]),
        pltpu.make_async_copy(wd_hbm.at[0], wd.at[0], wsem.at[2]),
        pltpu.make_async_copy(wo_hbm.at[pl.ds(pl.multiple_of(tp * hd, hd), hd)], wo, wsem.at[3]),
    ]
    for load in loads:
        load.start()

    def piece(ref, lead, part, j):
        which, at = divmod(j, nc)
        if which < 2:
            quarter = ref[which].shape[1] // nt
            step = quarter // nc
            return ref[which].at[lead, pl.ds(pl.multiple_of(part * quarter + at * step, step), step)]
        quarter = ref[2].shape[1] // nt
        step = width // nc
        return ref[2].at[lead, pl.ds(pl.multiple_of(part * quarter, quarter), quarter), pl.ds(at * step, step)]

    held = (wg, wu, wd)
    given = (wg_hbm, wu_hbm, wd_hbm)

    def x_copy(j):
        return remote(piece(given, 0, tp, j), piece(held, 1, tp, j), x_ss.at[j], w_rs.at[tp, j], (partner, tp))

    def y_copy(o, j):
        here = piece(held, 1, tp, j)
        return remote(here, here, y_ss.at[o, j], w_rs.at[tp, j], (me, lax.rem(tp + 2 * o, nt)))

    def core_copy(part, j):
        here = piece(held, 1, part, j)
        return remote(here, here, k_ss.at[part // 2, j], w_rs.at[part, j], (me, other))

    def weight_wait(part, j):
        here = piece(held, 1, part, j)
        remote(here, here, x_ss.at[j], w_rs.at[part, j], (me, other)).wait_recv()

    def from_partner(j):
        weight_wait(tp, j)
        for o in range(1, nt // 2):
            y_copy(o, j).start()
        core_copy(tp, j).start()

    def from_peers(j):
        for o in range(1, nt // 2):
            part = lax.rem(tp + 2 * o, nt)
            weight_wait(part, j)
            core_copy(part, j).start()

    def from_core(j):
        for o in range(nt // 2):
            weight_wait(lax.rem(other + 2 * o, nt), j)

    def tok_copy(up, s, c):
        here = tok.at[s, c]
        return remote(here, here, t_ss.at[up, s, c], t_rs.at[s, c], ((z - 1 + 2 * up) * 2 + par, tp))

    def tok_wait(s, c):
        here = tok.at[s, c]
        remote(here, here, t_ss.at[0, s, c], t_rs.at[s, c], (me, other)).wait_recv()

    def send_own(c):
        @pl.when(z + 1 < groups)
        def _():
            tok_copy(1, z, c).start()

        @pl.when(z > 0)
        def _():
            tok_copy(0, z, c).start()

    def forward(i, c):
        @pl.when((z - 1 - i >= 0) & (z + 1 < groups))
        def _():
            tok_wait(z - 1 - i, c)
            tok_copy(1, z - 1 - i, c).start()

        @pl.when((z + 1 + i < groups) & (z > 0))
        def _():
            tok_wait(z + 1 + i, c)
            tok_copy(0, z + 1 + i, c).start()

    normed = rms(x_ref[...].astype(F32), es_ref[...]).astype(BF16)
    for c in range(nc):
        tok[z, c] = normed[:, c * cw : (c + 1) * cw]

    pl.semaphore_wait(barrier, n - 1 + nt - 1)
    early = nc // 2
    for c in range(early):
        send_own(c)
    for j in range(2):
        x_copy(j).start()

    first, second = ids_ref[0:1, :], ids_ref[1:2, :]
    sub_e = lax.broadcasted_iota(jnp.int32, (n, tokens), 0)
    named = ((sub_e == first) | (sub_e == second)).astype(BF16)
    tr = lax.broadcasted_iota(jnp.int32, (tokens, tokens), 0)
    tc = lax.broadcasted_iota(jnp.int32, (tokens, tokens), 1)
    rank = dot(named, (tr < tc).astype(BF16))
    slot_a = first.astype(F32) * cap + jnp.sum(jnp.where(sub_e == first, rank, 0.0), axis=0, keepdims=True)
    slot_b = second.astype(F32) * cap + jnp.sum(jnp.where(sub_e == second, rank, 0.0), axis=0, keepdims=True)
    score_a, score_b = sc_ref[0:1, :], sc_ref[1:2, :]
    top = jnp.maximum(score_a, score_b)
    ex_a, ex_b = jnp.exp(score_a - top), jnp.exp(score_b - top)
    rw_a = grp_ref[...] * (ex_a / (ex_a + ex_b))
    rw_b = grp_ref[...] * (ex_b / (ex_a + ex_b))
    sub_i = lax.broadcasted_iota(jnp.int32, (8, tokens), 0)
    table = jnp.where(sub_i == 0, slot_a, jnp.where(sub_i == 1, slot_b,
        jnp.where(sub_i == 2, rw_a, jnp.where(sub_i == 3, rw_b, 0.0))))
    info[z] = jnp.zeros(info.shape[1:], F32)
    info[z, :, 0:tokens] = table

    def info_copy(g, s):
        return remote(info.at[s], info.at[s], i_ss.at[g], i_rs.at[s], (g * 2 + par, tp))

    def send_info(j, c):
        info_copy(lax.rem(z + j, groups), z).start()
        return c

    lax.fori_loop(1, groups, send_info, 0)

    fg = fg_ref[...]
    lk = jnp.minimum(fg, 0.0) - jnp.log1p(jnp.exp(-jnp.abs(fg))) + fb_ref[...]
    rid = lax.broadcasted_iota(jnp.int32, (length, length), 0)
    cid = lax.broadcasted_iota(jnp.int32, (length, length), 1)
    upper = (rid <= cid).astype(F32)
    b_row = dot(jnp.broadcast_to(lk, (8, length)), upper, precision=lax.Precision.HIGHEST)[0:1]
    i_row = ig_ref[...]
    last = b_row[:, length - 1 : length]
    g_row = last - b_row + i_row
    m_loc = jnp.max(g_row, axis=-1, keepdims=True)
    which_row = lax.broadcasted_iota(jnp.int32, (128, length), 0)
    stat[...] = jnp.where(which_row == 0, b_row, g_row).T
    kw = k_ref[...].astype(F32) * (jnp.exp(stat[:, 1:2] - m_loc) * (hd**-0.5))
    n_loc = jnp.sum(kw, axis=0, keepdims=True)
    stat_id = lax.broadcasted_iota(jnp.int32, (8, hd), 0)

    def stats(total, peak, nor):
        return jnp.where(stat_id == 0, nor, jnp.where(stat_id == 1, peak, total))

    def unpack(c, s):
        return (s[2:3], s[1:2], c.astype(F32), s[0:1])

    cpair[par] = dot(kw.astype(BF16), v_ref[...], ((0,), (0,))).astype(BF16)
    spair[par] = stats(last, m_loc, n_loc)

    def pair_copies(at):
        return [
            remote(cpair.at[at], cpair.at[at], c1s, c1r, (partner, tp)),
            remote(spair.at[at], spair.at[at], s1s, s1r, (partner, tp)),
        ]

    for copy in pair_copies(par):
        copy.start()
    for j in range(2, pieces):
        x_copy(j).start()
    for c in range(early, nc):
        send_own(c)

    def pre_copies():
        to = ((z + 1) * 2 + par, tp)
        return [
            remote(cpre.at[1], cpre.at[0], c2s, c2r, to),
            remote(spre.at[1], spre.at[0], s2s, s2r, to),
        ]

    def join_pair():
        for copy in pair_copies(1 - par):
            copy.wait_recv()
        both = join(unpack(cpair[0], spair[0]), unpack(cpair[1], spair[1]))
        cgrp[...] = both[2]
        sgrp[...] = stats(both[0], both[1], both[3])

    def hop(i):
        @pl.when(z == i)
        def _():
            if i:
                for copy in pre_copies():
                    copy.wait_recv()
                before = unpack(cpre[0], spre[0])
                ent[...] = before[2]
                sgate = spre[0]
            else:
                ent[...] = jnp.zeros(ent.shape, F32)
                row1 = jnp.zeros((1, hd), F32)
                sgate = stats(row1, row1 + FLOOR, row1)
                spre[0] = sgate
            if i + 1 < groups:
                out = join((sgate[2:3], sgate[1:2], ent[...], sgate[0:1]), unpack(cgrp[...], sgrp[...]))
                cpre[1] = out[2].astype(BF16)
                spre[1] = stats(out[0], out[1], out[3])
                for copy in pre_copies():
                    copy.start()

    rid_b = lax.broadcasted_iota(jnp.int32, (rows, length), 0)
    cid_b = lax.broadcasted_iota(jnp.int32, (rows, length), 1)

    def attend(r):
        at, end = r * rows, (r + 1) * rows
        decay = jnp.where(
            cid_b[:, :end] <= rid_b[:, :end] + at, stat[at:end, 0:1] - b_row[:, :end] + i_row[:, :end], -jnp.inf)
        peak = jnp.max(decay, axis=-1, keepdims=True)
        scores = dot(q_ref[at:end], k_ref[0:end], ((1,), (1,))) * (hd**-0.5) * jnp.exp(decay - peak)
        stat[at:end, 2:3] = peak
        stat[at:end, 3:4] = jnp.sum(scores, axis=-1, keepdims=True)
        num[at:end] = dot(scores.astype(BF16), v_ref[0:end])

    def attend_end():
        pre = (spre[0, 2:3], spre[0, 1:2], ent[...], spre[0, 0:1])
        joined = join(pre, unpack(cpair[0], spair[0]))
        odd = par == 1
        m_in = jnp.where(odd, joined[1], pre[1])
        n_in = jnp.where(odd, joined[3], pre[3])
        c_in = jnp.where(odd, joined[2], pre[2]).astype(BF16)
        for r in range(nt):
            at, end = r * rows, (r + 1) * rows
            carried = stat[at:end, 0:1] + m_in[:, 0:1]
            local = stat[at:end, 2:3]
            peaks = jnp.maximum(carried, local)
            across = jnp.exp(carried - peaks)
            within = jnp.exp(local - peaks)
            qf = q_ref[at:end].astype(F32)
            den = within * stat[at:end, 3:4] + across * jnp.sum(qf * n_in, axis=-1, keepdims=True)
            top = within * num[at:end] + across * dot(q_ref[at:end], c_in)
            cell = top / jnp.maximum(jnp.abs(den), jnp.exp(-peaks))
            head[at:end] = (cell * hs_ref[...]).astype(BF16)

    def part_copy(j):
        return remote(pout.at[j], prec.at[tp], p_ss.at[j], p_rs.at[tp], (me, j))

    def part_arrival(j):
        return remote(pout.at[j], prec.at[j], p_ss.at[j], p_rs.at[j], (me, j))

    def project(j):
        pout[j] = dot(head[pl.ds(pl.multiple_of(j * rows, rows), rows), :], wo[...]).astype(BF16)

    def send_part(i, c):
        j = lax.rem(tp + i, nt)
        project(j)
        part_copy(j).start()
        return c

    def mix():
        total = pout[tp].astype(F32)
        for i in range(1, nt):
            j = lax.rem(tp + i, nt)
            part_arrival(j).wait_recv()
            total = total + prec[j].astype(F32)
        mixed_ref[...] = rms(total, ps_ref[...]).astype(BF16)

    def masks(s, plane, start, count):
        table = info[s]
        slot = lax.broadcasted_iota(jnp.int32, (count, tokens), 0) + start
        own = (plane * 2 + par) * cap
        beside = (plane * 2 + 1 - par) * cap
        slot = jnp.where(slot < cap, own + slot, beside + slot - cap).astype(F32)
        return slot == table[0:1, 0:tokens], slot == table[1:2, 0:tokens], table[2:3, 0:tokens], table[3:4, 0:tokens]

    def hidden(s, e, at):
        is_a, is_b, _, _ = masks(s, z, e * cap, cap)
        place = (is_a | is_b).astype(BF16)
        for c in range(nc):
            chosen[:, c * cw : (c + 1) * cw] = dot(place, tok[s, c]).astype(BF16)
        gate = dot(chosen[...], wg[e])
        up = dot(chosen[...], wu[e])
        hid[at] = (gate / (1.0 + jnp.exp(-gate)) * up).astype(BF16)

    def share(s, e):
        is_a, is_b, w_a, w_b = masks(s, z, e * cap, cap)
        return jnp.sum(jnp.where(is_a, w_a, jnp.where(is_b, w_b, 0.0)), axis=1, keepdims=True)

    def half_of(e):
        return pl.ds(pl.multiple_of(e * cap, 16), cap)

    def down(s, e, at, c, weight):
        answer = dot(hid[at], wd[e, :, c * cw : (c + 1) * cw]) * weight
        ans[s, c, half_of(e), :] = answer.astype(BF16)

    def ret_to(s):
        below = s < z
        to = jnp.where(below, z - 1, z + 1)
        slot = jnp.where((to == s) & jnp.logical_not(below), groups, s)
        return below, to, slot

    def compact_copy(s, e, c):
        _, to, slot = ret_to(s)
        half = half_of(e)
        return remote(ans.at[s, c, half], cin.at[slot, c, half], c_ss.at[s, e, c], c_rs.at[slot, e, c], (to * 2 + par, tp))

    def compact_wait(slot, c):
        for e in range(2):
            half = half_of(e)
            remote(ans.at[0, c, half], cin.at[slot, c, half], c_ss.at[0, e, c], c_rs.at[slot, e, c], (me, other)).wait_recv()

    def sum_copy(s, c):
        _, to, slot = ret_to(s)
        return remote(rout.at[s, c], rin.at[slot, c], r_ss.at[s, c], r_rs.at[slot, c], (to * 2 + par, tp))

    def sum_wait(slot, c):
        remote(rout.at[0, c], rin.at[slot, c], r_ss.at[0, c], r_rs.at[slot, c], (me, other)).wait_recv()

    def at_end(s):
        return jnp.where(s < z, z == groups - 1, z == 0)

    def valid(s):
        return (s >= 0) & (s < groups)

    def arrive(s):
        @pl.when(at_end(s))
        def _():
            for c in range(nc):
                tok_wait(s, c)

        remote(info.at[s], info.at[s], i_ss.at[0], i_rs.at[s], (me, other)).wait_recv()

    def answer(s, e, at):
        hidden(s, e, at)
        weight = share(s, e)
        for c in range(nc):
            down(s, e, at, c, weight)

            @pl.when((s != z) & at_end(s))
            def _():
                compact_copy(s, e, c).start()

    def scatter(s, plane, block):
        is_a, is_b, _, _ = masks(s, plane, 0, 2 * cap)
        return dot((is_a | is_b).astype(BF16), block, ((0,), (0,)))

    def upstream(s, slot, near, last, c, put):
        @pl.when(near == last)
        def _():
            compact_wait(slot, c)
            put(scatter(s, last, cin[slot, c]))

        @pl.when(near != last)
        def _():
            sum_wait(slot, c)
            put(rin[slot, c].astype(F32))

    def pass_on(s, c):
        mine = scatter(s, z, ans[s, c])

        def put(more):
            rout[s, c] = (mine + more).astype(BF16)

        below = s < z
        upstream(s, s, jnp.where(below, z + 1, z - 1), jnp.where(below, groups - 1, 0), c, put)
        sum_copy(s, c).start()

    def own_end(c):
        acc[...] = scatter(z, z, ans[z, c])

        def put(more):
            acc[...] += more

        @pl.when(z < groups - 1)
        def _():
            upstream(z, z, z + 1, groups - 1, c, put)

        @pl.when(z > 0)
        def _():
            upstream(z, groups, z - 1, 0, c, put)

        routed_ref[:, c * cw : (c + 1) * cw] = acc[...].astype(BF16)

    def own_first():
        for load in loads:
            load.wait()
        answer(z, 0, 0)

    def near_first():
        def one(side, c):
            s = z + 2 * side - 1

            @pl.when(valid(s))
            def _():
                arrive(s)
                answer(s, 0, 0)

            return c

        lax.fori_loop(0, 2, one, 0)

    def near_hidden():
        for j in range(2 * nc):
            from_core(j)

        def one(side, c):
            s = z + 2 * side - 1

            @pl.when(valid(s))
            def _():
                hidden(s, 1, side)

            return c

        lax.fori_loop(0, 2, one, 0)

    def near_down(c):
        from_core(2 * nc + c)

        def one(side, carry):
            s = z + 2 * side - 1

            @pl.when(valid(s))
            def _():
                down(s, 1, side, c, share(s, 1))

                @pl.when(at_end(s))
                def _():
                    compact_copy(s, 1, c).start()

            return carry

        lax.fori_loop(0, 2, one, 0)

    def further(d):
        def one(i, c):
            s = z + d * (2 * (i // 2) - 1)
            e = lax.rem(i, 2)

            @pl.when(valid(s))
            def _():
                @pl.when(e == 0)
                def _():
                    arrive(s)

                answer(s, e, 0)

            return c

        lax.fori_loop(0, 4, one, 0)

    plan = {j: [] for j in range(pieces + 2)}

    def at(part, what, *args):
        plan[min(int(part * pieces), pieces + 1)].append((what, args))

    at(0.0, own_first)
    at(0.09, join_pair)
    at(0.09, hop, 0)
    for r in range(nt):
        at(0.17 + 0.26 * r / nt, attend, r)
    if groups > 2:
        for c in range(nc):
            at((0.42 * c + 0.42) / nc, forward, 0, c)
    at(0.51, near_first)
    at(0.51, hop, 1)
    for i in range(1, groups - 2):
        for c in range(nc):
            at(0.59 + 0.34 * c / nc, forward, i, c)
    for i in range(2, groups - 1):
        at(0.76, hop, i)
    at(0.8, near_hidden)
    for c in range(nc):
        plan[2 * nc + 2 + c].append((near_down, (c,)))

    for j in range(pieces + 2):
        if j < pieces:
            from_partner(j)
        if j >= 2:
            from_peers(j - 2)
        for what, args in plan[j]:
            what(*args)

    if groups > 2:
        further(2)
    if groups > 2:
        hop(groups - 1)
    attend_end()
    lax.fori_loop(1, nt, send_part, 0)
    project(tp)
    answer(z, 1, 0)
    for d in range(3, groups):
        further(d)

    for turn in range(1, groups):
        low, high = groups - 1 - turn, turn
        for t in range(nc + max(groups - 3, 0)):
            for h in range(1, min(turn, groups - 1)):
                c = t - (h - 1)
                if 0 <= c < nc:
                    @pl.when(z == groups - 1 - h)
                    def _():
                        pass_on(low, c)

                    @pl.when(z == h)
                    def _():
                        pass_on(high, c)

            if t < nc and turn >= 2:
                @pl.when(jnp.maximum(z, groups - 1 - z) == turn - 1)
                def _():
                    own_end(t)

            if turn == groups - 1 and t == 2:
                mix()

    for c in range(nc):
        @pl.when(jnp.maximum(z, groups - 1 - z) == groups - 1)
        def _():
            own_end(c)

    for j in range(pieces):
        x_copy(j).wait_send()
        core_copy(tp, j).wait_send()
        for o in range(1, nt // 2):
            y_copy(o, j).wait_send()
            core_copy(lax.rem(tp + 2 * o, nt), j).wait_send()
    for copy in pair_copies(par):
        copy.wait_send()

    @pl.when(z + 1 < groups)
    def _():
        for copy in pre_copies():
            copy.wait_send()

    def finish(s, carry):
        for c in range(nc):
            @pl.when((s <= z) & (z + 1 < groups))
            def _():
                tok_copy(1, s, c).wait_send()

            @pl.when((s >= z) & (z > 0))
            def _():
                tok_copy(0, s, c).wait_send()

        @pl.when(s != z)
        def _():
            info_copy(s, z).wait_send()

            @pl.when(at_end(s))
            def _():
                for e in range(2):
                    for c in range(nc):
                        compact_copy(s, e, c).wait_send()

            @pl.when(jnp.logical_not(at_end(s)))
            def _():
                for c in range(nc):
                    sum_copy(s, c).wait_send()

        return carry

    lax.fori_loop(0, groups, finish, 0)
    for i in range(1, nt):
        part_copy(lax.rem(tp + i, nt)).wait_send()


def shards(
    n, nt,
    memory_query_matrix, memory_key_matrix, memory_value_matrix,
    input_gate_logits, forget_gate_logits, forget_log_boosts,
    head_norm_scale, memory_output_matrix, projection_norm_scale,
    second_batch_rows, expert_prenorm_scale, selected_expert_index,
    group_route_probability, expert_choice_scores,
    expert_gate_matrix, expert_up_matrix, expert_down_matrix,
):
    length, hd = memory_query_matrix.shape
    tokens, width = second_batch_rows.shape
    hidden = expert_gate_matrix.shape[2]
    cap = 2 * selected_expert_index.shape[1] * tokens // n
    cap = -(-cap // 16) * 16
    rows = length // nt
    vm = pl.BlockSpec(memory_space=pltpu.VMEM)
    hbm = pl.BlockSpec(memory_space=pl.ANY)
    dma = pltpu.SemaphoreType.DMA
    slots = pltpu.VMEM((n, cap, width), BF16)
    groups = n // 2
    nc = 4
    cw = width // nc
    wide = -(-tokens // 128) * 128
    near = groups * tokens * width * 6 < 24 * 1024 * 1024 and nt % 2 == 0
    if near:
        pair_w = (2, width, hidden)
        pieces = 3 * nc
        slot = (groups, nc, 2 * cap, cw)
        slot_in = (groups + 1, nc, 2 * cap, cw)
        line = (groups, nc, tokens, cw)
        line_in = (groups + 1, nc, tokens, cw)
        return pl.pallas_call(
            functools.partial(plane_kernel, n, nt, cap, nc),
            out_shape=(
                jax.ShapeDtypeStruct((rows, width), BF16),
                jax.ShapeDtypeStruct((tokens, width), BF16),
            ),
            in_specs=[vm] * 7 + [hbm] + [vm] * 6 + [hbm] * 3,
            out_specs=(vm, vm),
            scratch_shapes=[
                pltpu.VMEM(pair_w, BF16),
                pltpu.VMEM(pair_w, BF16),
                pltpu.VMEM((2, hidden, width), BF16),
                pltpu.VMEM((hd, width), BF16),
                pltpu.VMEM(line, BF16),
                pltpu.VMEM((groups, 8, wide), F32),
                pltpu.VMEM((cap, width), BF16),
                pltpu.VMEM((2, cap, hidden), BF16),
                pltpu.VMEM(slot, BF16),
                pltpu.VMEM(slot_in, BF16),
                pltpu.VMEM(line, BF16),
                pltpu.VMEM(line_in, BF16),
                pltpu.VMEM((tokens, cw), F32),
                pltpu.VMEM((2, hd, hd), BF16),
                pltpu.VMEM((2, 8, hd), F32),
                pltpu.VMEM((hd, hd), F32),
                pltpu.VMEM((8, hd), F32),
                pltpu.VMEM((2, hd, hd), BF16),
                pltpu.VMEM((2, 8, hd), F32),
                pltpu.VMEM((hd, hd), F32),
                pltpu.VMEM((length, hd), F32),
                pltpu.VMEM((length, 128), F32),
                pltpu.VMEM((length, hd), BF16),
                pltpu.VMEM((nt, rows, width), BF16),
                pltpu.VMEM((nt, rows, width), BF16),
                dma((4,)),
                dma((pieces,)), dma((nt // 2, pieces)), dma((nt // 2, pieces)), dma((nt, pieces)),
                dma((2, groups, nc)), dma((groups, nc)),
                dma((groups,)), dma((groups,)),
                dma((groups, 2, nc)), dma((groups + 1, 2, nc)),
                dma((groups, nc)), dma((groups + 1, nc)),
                dma, dma, dma, dma, dma, dma, dma, dma,
                dma((nt,)), dma((nt,)),
            ],
            compiler_params=pltpu.CompilerParams(
                collective_id=0, has_side_effects=True, vmem_limit_bytes=62 * 1024 * 1024
            ),
        )(
            memory_query_matrix, memory_key_matrix, memory_value_matrix,
            input_gate_logits, forget_gate_logits, forget_log_boosts,
            head_norm_scale[None], memory_output_matrix, projection_norm_scale[None],
            second_batch_rows, expert_prenorm_scale[None], selected_expert_index.T,
            group_route_probability[None], expert_choice_scores.T,
            expert_gate_matrix, expert_up_matrix, expert_down_matrix,
        )
    buffers = [
        slots, slots, slots, slots,
        pltpu.VMEM((tokens, width), BF16),
        pltpu.VMEM((tokens, width), F32),
    ]
    sems = [dma((n,))] * 4
    return pl.pallas_call(
        functools.partial(kernel, n, nt, cap),
        out_shape=(
            jax.ShapeDtypeStruct((rows, width), BF16),
            jax.ShapeDtypeStruct((tokens, width), BF16),
        ),
        in_specs=[vm] * 7 + [hbm] + [vm] * 6 + [hbm] * 3,
        out_specs=(vm, vm),
        scratch_shapes=[
            pltpu.VMEM((width, hidden), BF16),
            pltpu.VMEM((width, hidden), BF16),
            pltpu.VMEM((hidden, width), BF16),
            pltpu.VMEM((hd, width), BF16),
            *buffers,
            pltpu.VMEM((2, hd, hd), BF16),
            pltpu.VMEM((2, 8, hd), F32),
            pltpu.VMEM((n // 2, hd, hd), BF16),
            pltpu.VMEM((n // 2, 8, hd), F32),
            pltpu.VMEM((hd, hd), F32),
            pltpu.VMEM((length, hd), BF16),
            pltpu.VMEM((nt, rows, width), BF16),
            pltpu.VMEM((nt, rows, width), BF16),
            dma((4,)),
            *sems,
            dma, dma, dma, dma,
            dma((n // 2,)), dma((n // 2,)), dma((n // 2,)), dma((n // 2,)),
            dma((nt,)), dma((nt,)),
        ],
        compiler_params=pltpu.CompilerParams(
            collective_id=0, has_side_effects=True, vmem_limit_bytes=62 * 1024 * 1024
        ),
    )(
        memory_query_matrix, memory_key_matrix, memory_value_matrix,
        input_gate_logits, forget_gate_logits, forget_log_boosts,
        head_norm_scale[None], memory_output_matrix, projection_norm_scale[None],
        second_batch_rows, expert_prenorm_scale[None], selected_expert_index,
        group_route_probability[:, None], expert_choice_scores,
        expert_gate_matrix, expert_up_matrix, expert_down_matrix,
    )


def solution(mesh):
    return jax.shard_map(
        functools.partial(shards, mesh.shape["ep"], mesh.shape["tp"]),
        mesh=mesh,
        in_specs=(
            P("ep", "tp"), P("ep", "tp"), P("ep", "tp"),
            P("tp", "ep"), P("tp", "ep"), P("tp", "ep"),
            P("tp"), P(), P(),
            P(("ep", "tp"), None), P(), P(("ep", "tp"), None),
            P(("ep", "tp")), P(("ep", "tp"), None),
            P("ep", None, None), P("ep", None, None), P("ep", None, None),
        ),
        out_specs=(P(("ep", "tp"), None), P(("ep", "tp"), None)),
        check_vma=False,
    )
```

```python
import functools

import jax
import jax.numpy as jnp
from jax import lax
from jax.experimental import pallas as pl
from jax.experimental.pallas import tpu as pltpu
from jax.sharding import PartitionSpec as P

FLOOR = -1e30
EPS = 1e-06
MESH = pl.DeviceIdType.MESH
F32 = jnp.float32
BF16 = jnp.bfloat16


def rms(values, gain):
    squares = jnp.mean(values * values, axis=-1, keepdims=True)
    return values * lax.rsqrt(squares + EPS) * gain


def dot(a, b, dims=((1,), (0,)), precision=None):
    return lax.dot_general(a, b, (dims, ((), ())), preferred_element_type=F32, precision=precision)


def join(early, late):
    total_e, peak_e, mem_e, nor_e = early
    total_l, peak_l, mem_l, nor_l = late
    peak = jnp.maximum(total_l + peak_e, peak_l)
    fe = jnp.exp(total_l + peak_e - peak)
    fl = jnp.exp(peak_l - peak)
    return (total_e + total_l, peak, fe * mem_e + fl * mem_l, fe * nor_e + fl * nor_l)


def kernel(
    n, nt, cap,
    q_ref, k_ref, v_ref, ig_ref, fg_ref, fb_ref, hs_ref, wo_hbm, ps_ref,
    x_ref, es_ref, ids_ref, grp_ref, sc_ref, wg_hbm, wu_hbm, wd_hbm,
    mixed_ref, routed_ref,
    wg, wu, wd, wo, out, recv, ans, back, ffn, acc,
    cpair, spair, cgrp, sgrp, ent, head, pout, prec,
    wsem, d_ss, d_rs, a_ss, a_rs, c1s, c1r, s1s, s1r, c2s, c2r, s2s, s2r, p_ss, p_rs,
):
    me = lax.axis_index("ep")
    tp = lax.axis_index("tp")
    groups = n // 2
    grp = me // 2
    par = lax.rem(me, 2)
    partner = me + 1 - 2 * par
    tokens, width = x_ref.shape
    length, hd = q_ref.shape
    rows = mixed_ref.shape[0]

    barrier = pltpu.get_barrier_semaphore()

    def greet(i, c):
        pl.semaphore_signal(barrier, inc=1, device_id=(lax.rem(me + i, n), tp), device_id_type=MESH)
        return c

    lax.fori_loop(1, n, greet, 0)
    for j in range(1, nt):
        pl.semaphore_signal(barrier, inc=1, device_id=(me, lax.rem(tp + j, nt)), device_id_type=MESH)

    loads = [
        pltpu.make_async_copy(wg_hbm.at[0], wg, wsem.at[0]),
        pltpu.make_async_copy(wu_hbm.at[0], wu, wsem.at[1]),
        pltpu.make_async_copy(wd_hbm.at[0], wd, wsem.at[2]),
        pltpu.make_async_copy(wo_hbm.at[pl.ds(pl.multiple_of(tp * hd, hd), hd)], wo, wsem.at[3]),
    ]
    for load in loads:
        load.start()

    fg = fg_ref[...]
    lk = jnp.minimum(fg, 0.0) - jnp.log1p(jnp.exp(-jnp.abs(fg))) + fb_ref[...]
    rid = lax.broadcasted_iota(jnp.int32, (length, length), 0)
    cid = lax.broadcasted_iota(jnp.int32, (length, length), 1)
    upper = (rid <= cid).astype(F32)
    b_row = dot(jnp.broadcast_to(lk, (8, length)), upper, precision=lax.Precision.HIGHEST)[0:1]
    i_row = ig_ref[...]
    last = b_row[:, length - 1 : length]
    g_row = last - b_row + i_row
    m_loc = jnp.max(g_row, axis=-1, keepdims=True)
    which = lax.broadcasted_iota(jnp.int32, (128, length), 0)
    cols = jnp.where(which == 0, b_row, g_row).T
    b_col = cols[:, 0:1]
    g_col = cols[:, 1:2]
    kw = k_ref[...].astype(F32) * (jnp.exp(g_col - m_loc) * (hd**-0.5))
    c_loc = dot(kw.astype(BF16), v_ref[...], ((0,), (0,)))
    n_loc = jnp.sum(kw, axis=0, keepdims=True)
    stat_id = lax.broadcasted_iota(jnp.int32, (8, hd), 0)

    def stats(total, peak, nor):
        return jnp.where(stat_id == 0, nor, jnp.where(stat_id == 1, peak, total))

    cpair[par] = c_loc.astype(BF16)
    spair[par] = stats(last, m_loc, n_loc)

    pl.semaphore_wait(barrier, n - 1 + nt - 1)

    def pair_copies():
        return [
            pltpu.make_async_remote_copy(
                src_ref=cpair.at[par], dst_ref=cpair.at[par], send_sem=c1s, recv_sem=c1r,
                device_id=(partner, tp), device_id_type=MESH),
            pltpu.make_async_remote_copy(
                src_ref=spair.at[par], dst_ref=spair.at[par], send_sem=s1s, recv_sem=s1r,
                device_id=(partner, tp), device_id_type=MESH),
        ]

    for copy in pair_copies():
        copy.start()

    ffn[...] = rms(x_ref[...].astype(F32), es_ref[...]).astype(BF16)
    ids = ids_ref[...]
    first, second = ids[:, 0:1], ids[:, 1:2]
    lane_e = lax.broadcasted_iota(jnp.int32, (tokens, n), 1)
    named = ((lane_e == first) | (lane_e == second)).astype(F32)
    tr = lax.broadcasted_iota(jnp.int32, (tokens, tokens), 0)
    tc = lax.broadcasted_iota(jnp.int32, (tokens, tokens), 1)
    rank = dot((tc < tr).astype(BF16), named.astype(BF16))
    slot_a = first * cap + jnp.sum(jnp.where(lane_e == first, rank, 0.0), axis=1, keepdims=True).astype(jnp.int32)
    slot_b = second * cap + jnp.sum(jnp.where(lane_e == second, rank, 0.0), axis=1, keepdims=True).astype(jnp.int32)
    score = sc_ref[...]
    ex = jnp.exp(score - jnp.max(score, axis=-1, keepdims=True))
    route = grp_ref[...] * (ex / jnp.sum(ex, axis=-1, keepdims=True))
    rw_a, rw_b = route[:, 0:1], route[:, 1:2]
    lane_c = lax.broadcasted_iota(jnp.int32, (tokens, cap), 1)

    def pack(e):
        lane = lane_c + e * cap
        place = ((lane == slot_a) | (lane == slot_b)).astype(BF16)
        out[e] = dot(place, ffn[...], ((0,), (0,))).astype(BF16)

    def offset(i):
        return n // 2 + jnp.where(lax.rem(i, 2) == 0, i // 2, -((i + 1) // 2))

    def dispatch_copy(e):
        return pltpu.make_async_remote_copy(
            src_ref=out.at[e], dst_ref=recv.at[me], send_sem=d_ss.at[e], recv_sem=d_rs.at[me],
            device_id=(e, tp), device_id_type=MESH)

    def dispatch_arrival(s):
        return pltpu.make_async_remote_copy(
            src_ref=out.at[s], dst_ref=recv.at[s], send_sem=d_ss.at[s], recv_sem=d_rs.at[s],
            device_id=(s, tp), device_id_type=MESH)

    def answer_copy(s):
        return pltpu.make_async_remote_copy(
            src_ref=ans.at[s], dst_ref=back.at[me], send_sem=a_ss.at[s], recv_sem=a_rs.at[me],
            device_id=(s, tp), device_id_type=MESH)

    def answer_arrival(e):
        return pltpu.make_async_remote_copy(
            src_ref=ans.at[e], dst_ref=back.at[e], send_sem=a_ss.at[e], recv_sem=a_rs.at[e],
            device_id=(e, tp), device_id_type=MESH)

    for copy in pair_copies():
        copy.wait_send()
    def pair_arrival():
        return [
            pltpu.make_async_remote_copy(
                src_ref=cpair.at[1 - par], dst_ref=cpair.at[1 - par], send_sem=c1s, recv_sem=c1r,
                device_id=(partner, tp), device_id_type=MESH),
            pltpu.make_async_remote_copy(
                src_ref=spair.at[1 - par], dst_ref=spair.at[1 - par], send_sem=s1s, recv_sem=s1r,
                device_id=(partner, tp), device_id_type=MESH),
        ]

    for copy in pair_arrival():
        copy.wait_recv()

    def unpack(c, s):
        return (s[2:3], s[1:2], c.astype(F32), s[0:1])

    both = join(unpack(cpair[0], spair[0]), unpack(cpair[1], spair[1]))
    cgrp[grp] = both[2].astype(BF16)
    sgrp[grp] = stats(both[0], both[1], both[3])

    def group_copies(g):
        to = (g * 2 + par, tp)
        return [
            pltpu.make_async_remote_copy(
                src_ref=cgrp.at[grp], dst_ref=cgrp.at[grp], send_sem=c2s.at[g], recv_sem=c2r.at[grp],
                device_id=to, device_id_type=MESH),
            pltpu.make_async_remote_copy(
                src_ref=sgrp.at[grp], dst_ref=sgrp.at[grp], send_sem=s2s.at[g], recv_sem=s2r.at[grp],
                device_id=to, device_id_type=MESH),
        ]

    def group_arrivals(g):
        at = (g * 2 + par, tp)
        return [
            pltpu.make_async_remote_copy(
                src_ref=cgrp.at[g], dst_ref=cgrp.at[g], send_sem=c2s.at[g], recv_sem=c2r.at[g],
                device_id=at, device_id_type=MESH),
            pltpu.make_async_remote_copy(
                src_ref=sgrp.at[g], dst_ref=sgrp.at[g], send_sem=s2s.at[g], recv_sem=s2r.at[g],
                device_id=at, device_id_type=MESH),
        ]

    def send_group(g, c):
        for copy in group_copies(g):
            copy.start()
        return c

    lax.fori_loop(grp + 1, groups, send_group, 0)

    def send_tokens(i, c):
        e = lax.rem(me + offset(i), n)
        pack(e)
        dispatch_copy(e).start()
        return c

    lax.fori_loop(0, n - 1, send_tokens, 0)
    pack(me)
    for load in loads:
        load.wait()

    def expert(chosen):
        gate = dot(chosen, wg[...])
        up = dot(chosen, wu[...])
        hidden = (gate / (1.0 + jnp.exp(-gate)) * up).astype(BF16)
        return dot(hidden, wd[...]).astype(BF16)

    ans[me] = expert(out[me])

    ent[...] = jnp.zeros(ent.shape, F32)
    row1 = jnp.zeros((1, hd), F32)

    def enter(g, carry):
        total, peak, nor = carry
        for copy in group_arrivals(g):
            copy.wait_recv()
        total, peak, mem, nor = join((total, peak, ent[...], nor), unpack(cgrp[g], sgrp[g]))
        ent[...] = mem
        return total, peak, nor

    total, peak, nor = lax.fori_loop(0, grp, enter, (row1, row1 + FLOOR, row1))
    joined = join((total, peak, ent[...], nor), unpack(cpair[0], spair[0]))
    odd = par == 1
    m_in = jnp.where(odd, joined[1], peak)
    n_in = jnp.where(odd, joined[3], nor)
    c_in = jnp.where(odd, joined[2], ent[...])

    carried = b_col + m_in[:, 0:1]
    decay = jnp.where(cid <= rid, b_col - b_row + i_row, -jnp.inf)
    peaks = jnp.maximum(carried, jnp.max(decay, axis=-1, keepdims=True))
    across = jnp.exp(carried - peaks)
    scores = dot(q_ref[...], k_ref[...], ((1,), (1,))) * (hd**-0.5) * jnp.exp(decay - peaks)
    qf = q_ref[...].astype(F32)
    den = jnp.sum(scores, axis=-1, keepdims=True) + across * jnp.sum(qf * n_in, axis=-1, keepdims=True)
    num = dot(scores.astype(BF16), v_ref[...]) + across * dot(q_ref[...], c_in.astype(BF16))
    cell = num / jnp.maximum(jnp.abs(den), jnp.exp(-peaks))
    head[...] = (cell * hs_ref[...]).astype(BF16)

    def part_copy(j):
        return pltpu.make_async_remote_copy(
            src_ref=pout.at[j], dst_ref=prec.at[tp], send_sem=p_ss.at[j], recv_sem=p_rs.at[tp],
            device_id=(me, j), device_id_type=MESH)

    def part_arrival(j):
        return pltpu.make_async_remote_copy(
            src_ref=pout.at[j], dst_ref=prec.at[j], send_sem=p_ss.at[j], recv_sem=p_rs.at[j],
            device_id=(me, j), device_id_type=MESH)

    def project(j):
        pout[j] = dot(head[pl.ds(pl.multiple_of(j * rows, rows), rows), :], wo[...]).astype(BF16)

    def send_part(i, c):
        j = lax.rem(tp + i, nt)
        project(j)
        part_copy(j).start()
        return c

    lax.fori_loop(1, nt, send_part, 0)
    project(tp)

    def serve(i, c):
        s = lax.rem(me - offset(i) + n, n)
        dispatch_arrival(s).wait_recv()
        ans[s] = expert(recv[s])
        answer_copy(s).start()
        return c

    lax.fori_loop(0, n - 1, serve, 0)

    def mix(i, total):
        j = lax.rem(tp + i, nt)
        part_arrival(j).wait_recv()
        return total + prec[j].astype(F32)

    projected = pout[tp].astype(F32)
    for i in range(1, nt):
        projected = mix(i, projected)
    mixed_ref[...] = rms(projected, ps_ref[...]).astype(BF16)

    def weigh(e, block):
        lane = lane_c + e * cap
        w = jnp.where(lane == slot_a, rw_a, jnp.where(lane == slot_b, rw_b, 0.0))
        high = w.astype(BF16)
        low = (w - high.astype(F32)).astype(BF16)
        return dot(high, block) + dot(low, block)

    acc[...] = weigh(me, ans[me])

    def collect(i, c):
        e = lax.rem(me + offset(i), n)
        answer_arrival(e).wait_recv()
        acc[...] += weigh(e, back[e])
        return c

    lax.fori_loop(0, n - 1, collect, 0)
    routed_ref[...] = acc[...].astype(BF16)

    def finish(i, c):
        e = lax.rem(me + i, n)
        dispatch_copy(e).wait_send()
        answer_copy(e).wait_send()
        return c

    lax.fori_loop(1, n, finish, 0)

    def finish_group(g, c):
        for copy in group_copies(g):
            copy.wait_send()
        return c

    lax.fori_loop(grp + 1, groups, finish_group, 0)
    for i in range(1, nt):
        part_copy(lax.rem(tp + i, nt)).wait_send()


def plane_kernel(
    n, nt, cap, nc, wc,
    q_ref, k_ref, v_ref, ig_ref, fg_ref, fb_ref, hs_ref, wo_hbm, ps_ref,
    x_ref, es_ref, ids_ref, grp_ref, sc_ref, wg_hbm, wu_hbm, wd_hbm,
    mixed_ref, routed_ref,
    wg, wu, wd, wo, tok, info, chosen, hid, ans, cin, rout, rin, acc,
    cpair, spair, cgrp, sgrp, cpre, spre, ent, num, stat, head, pout, prec,
    wsem, x_ss, y_ss, k_ss, w_rs, t_ss, t_rs, i_ss, i_rs, c_ss, r_ss, r_rs,
    c1s, c1r, s1s, s1r, c2s, c2r, s2s, s2r, p_ss, p_rs,
):
    me = lax.axis_index("ep")
    tp = lax.axis_index("tp")
    groups = n // 2
    z = me // 2
    par = lax.rem(me, 2)
    partner = me + 1 - 2 * par
    other = tp + 1 - 2 * lax.rem(tp, 2)
    tokens, width = x_ref.shape
    length, hd = q_ref.shape
    rows = mixed_ref.shape[0]
    cw = width // nc
    pieces = 3 * wc

    def remote(src, dst, ss, rs, to):
        return pltpu.make_async_remote_copy(
            src_ref=src, dst_ref=dst, send_sem=ss, recv_sem=rs, device_id=to, device_id_type=MESH)

    barrier = pltpu.get_barrier_semaphore()

    def greet(i, c):
        pl.semaphore_signal(barrier, inc=1, device_id=(lax.rem(me + i, n), tp), device_id_type=MESH)
        return c

    lax.fori_loop(1, n, greet, 0)
    for j in range(1, nt):
        pl.semaphore_signal(barrier, inc=1, device_id=(me, lax.rem(tp + j, nt)), device_id_type=MESH)

    loads = [
        pltpu.make_async_copy(wg_hbm.at[0], wg.at[0], wsem.at[0]),
        pltpu.make_async_copy(wu_hbm.at[0], wu.at[0], wsem.at[1]),
        pltpu.make_async_copy(wd_hbm.at[0], wd.at[0], wsem.at[2]),
        pltpu.make_async_copy(wo_hbm.at[pl.ds(pl.multiple_of(tp * hd, hd), hd)], wo, wsem.at[3]),
    ]
    for load in loads:
        load.start()

    def piece(ref, lead, part, j):
        which, at = divmod(j, wc)
        if which < 2:
            quarter = ref[which].shape[1] // nt
            step = quarter // wc
            return ref[which].at[lead, pl.ds(pl.multiple_of(part * quarter + at * step, step), step)]
        quarter = ref[2].shape[1] // nt
        step = width // wc
        return ref[2].at[lead, pl.ds(pl.multiple_of(part * quarter, quarter), quarter), pl.ds(at * step, step)]

    held = (wg, wu, wd)
    given = (wg_hbm, wu_hbm, wd_hbm)

    def x_copy(j):
        return remote(piece(given, 0, tp, j), piece(held, 1, tp, j), x_ss.at[j // wc], w_rs.at[tp, j], (partner, tp))

    def y_copy(o, j):
        here = piece(held, 1, tp, j)
        return remote(here, here, y_ss.at[o, j // wc], w_rs.at[tp, j], (me, lax.rem(tp + 2 * o, nt)))

    def core_copy(part, j):
        here = piece(held, 1, part, j)
        sem = w_rs.at[part, j // wc * wc if j < 2 * wc else j]
        return remote(here, here, k_ss.at[part // 2, j // wc], sem, (me, other))

    def weight_wait(part, j):
        here = piece(held, 1, part, j)
        remote(here, here, x_ss.at[j // wc], w_rs.at[part, j], (me, other)).wait_recv()

    def quarter(which, part):
        step = held[which].shape[1] // nt
        return held[which].at[1, pl.ds(pl.multiple_of(part * step, step), step)]

    def from_partner(j):
        weight_wait(tp, j)
        for o in range(1, nt // 2):
            y_copy(o, j).start()
        core_copy(tp, j).start()

    def from_peers(j):
        for o in range(1, nt // 2):
            part = lax.rem(tp + 2 * o, nt)
            weight_wait(part, j)
            core_copy(part, j).start()

    def from_core(j):
        for o in range(nt // 2):
            part = lax.rem(other + 2 * o, nt)
            if j < 2 * wc:
                here = quarter(j // wc, part)
                remote(here, here, x_ss.at[0], w_rs.at[part, j], (me, other)).wait_recv()
            else:
                weight_wait(part, j)

    def tok_copy(up, s, c):
        here = tok.at[s, c]
        return remote(here, here, t_ss.at[up, s], t_rs.at[s, c], ((z - 1 + 2 * up) * 2 + par, tp))

    def tok_wait(s, c):
        here = tok.at[s, c]
        remote(here, here, t_ss.at[0, s], t_rs.at[s, c], (me, other)).wait_recv()

    def send_own(c):
        @pl.when(z + 1 < groups)
        def _():
            tok_copy(1, z, c).start()

        @pl.when(z > 0)
        def _():
            tok_copy(0, z, c).start()

    def near_arrive(c):
        @pl.when(z > 0)
        def _():
            tok_wait(z - 1, c)

            @pl.when((z == 1) & (z + 1 < groups))
            def _():
                tok_copy(1, z - 1, c).start()

        @pl.when(z + 1 < groups)
        def _():
            tok_wait(z + 1, c)

            @pl.when((z == groups - 2) & (z > 0))
            def _():
                tok_copy(0, z + 1, c).start()

    def near_forward(c):
        @pl.when((z >= 2) & (z + 1 < groups))
        def _():
            tok_copy(1, z - 1, c).start()

        @pl.when((z <= groups - 3) & (z > 0))
        def _():
            tok_copy(0, z + 1, c).start()

    def far_forward(i, c):
        @pl.when((i < z) & (z + 1 < groups))
        def _():
            tok_wait(i - 1, c)
            tok_copy(1, i - 1, c).start()

        @pl.when((i < groups - 1 - z) & (z > 0))
        def _():
            tok_wait(groups - i, c)
            tok_copy(0, groups - i, c).start()

    normed = rms(x_ref[...].astype(F32), es_ref[...]).astype(BF16)
    for c in range(nc):
        tok[z, c] = normed[:, c * cw : (c + 1) * cw]

    pl.semaphore_wait(barrier, n - 1 + nt - 1)
    early = 5 * nc // 8
    for c in range(early):
        send_own(c)
    for j in range(2):
        x_copy(j).start()

    first, second = ids_ref[0:1, :], ids_ref[1:2, :]
    sub_e = lax.broadcasted_iota(jnp.int32, (n, tokens), 0)
    named = ((sub_e == first) | (sub_e == second)).astype(BF16)
    tr = lax.broadcasted_iota(jnp.int32, (tokens, tokens), 0)
    tc = lax.broadcasted_iota(jnp.int32, (tokens, tokens), 1)
    rank = dot(named, (tr < tc).astype(BF16))
    slot_a = first.astype(F32) * cap + jnp.sum(jnp.where(sub_e == first, rank, 0.0), axis=0, keepdims=True)
    slot_b = second.astype(F32) * cap + jnp.sum(jnp.where(sub_e == second, rank, 0.0), axis=0, keepdims=True)
    score_a, score_b = sc_ref[0:1, :], sc_ref[1:2, :]
    top = jnp.maximum(score_a, score_b)
    ex_a, ex_b = jnp.exp(score_a - top), jnp.exp(score_b - top)
    rw_a = grp_ref[...] * (ex_a / (ex_a + ex_b))
    rw_b = grp_ref[...] * (ex_b / (ex_a + ex_b))
    sub_i = lax.broadcasted_iota(jnp.int32, (8, tokens), 0)
    table = jnp.where(sub_i == 0, slot_a, jnp.where(sub_i == 1, slot_b,
        jnp.where(sub_i == 2, rw_a, jnp.where(sub_i == 3, rw_b, 0.0))))
    info[z] = jnp.zeros(info.shape[1:], F32)
    info[z, :, 0:tokens] = table

    def info_copy(g, s):
        return remote(info.at[s], info.at[s], i_ss.at[g], i_rs.at[s], (g * 2 + par, tp))

    def send_info(j, c):
        info_copy(lax.rem(z + j, groups), z).start()
        return c

    lax.fori_loop(1, groups, send_info, 0)

    fg = fg_ref[...]
    lk = jnp.minimum(fg, 0.0) - jnp.log1p(jnp.exp(-jnp.abs(fg))) + fb_ref[...]
    rid = lax.broadcasted_iota(jnp.int32, (length, length), 0)
    cid = lax.broadcasted_iota(jnp.int32, (length, length), 1)
    upper = (rid <= cid).astype(F32)
    b_row = dot(jnp.broadcast_to(lk, (8, length)), upper, precision=lax.Precision.HIGHEST)[0:1]
    i_row = ig_ref[...]
    last = b_row[:, length - 1 : length]
    g_row = last - b_row + i_row
    m_loc = jnp.max(g_row, axis=-1, keepdims=True)
    which_row = lax.broadcasted_iota(jnp.int32, (128, length), 0)
    stat[...] = jnp.where(which_row == 0, b_row, g_row).T
    kw = k_ref[...].astype(F32) * (jnp.exp(stat[:, 1:2] - m_loc) * (hd**-0.5))
    n_loc = jnp.sum(kw, axis=0, keepdims=True)
    stat_id = lax.broadcasted_iota(jnp.int32, (8, hd), 0)

    def stats(total, peak, nor):
        return jnp.where(stat_id == 0, nor, jnp.where(stat_id == 1, peak, total))

    def unpack(c, s):
        return (s[2:3], s[1:2], c.astype(F32), s[0:1])

    cpair[par] = dot(kw.astype(BF16), v_ref[...], ((0,), (0,))).astype(BF16)
    spair[par] = stats(last, m_loc, n_loc)

    def pair_copies(at):
        return [
            remote(cpair.at[at], cpair.at[at], c1s, c1r, (partner, tp)),
            remote(spair.at[at], spair.at[at], s1s, s1r, (partner, tp)),
        ]

    for copy in pair_copies(par):
        copy.start()
    for j in range(2, pieces):
        x_copy(j).start()
    def send_rest():
        for c in range(early, nc):
            send_own(c)

    def pre_copies():
        to = ((z + 1) * 2 + par, tp)
        return [
            remote(cpre.at[1], cpre.at[0], c2s, c2r, to),
            remote(spre.at[1], spre.at[0], s2s, s2r, to),
        ]

    def join_pair():
        for copy in pair_copies(1 - par):
            copy.wait_recv()
        both = join(unpack(cpair[0], spair[0]), unpack(cpair[1], spair[1]))
        cgrp[...] = both[2]
        sgrp[...] = stats(both[0], both[1], both[3])

    def hop(i):
        @pl.when(z == i)
        def _():
            if i:
                for copy in pre_copies():
                    copy.wait_recv()
                before = unpack(cpre[0], spre[0])
                ent[...] = before[2]
                sgate = spre[0]
            else:
                ent[...] = jnp.zeros(ent.shape, F32)
                row1 = jnp.zeros((1, hd), F32)
                sgate = stats(row1, row1 + FLOOR, row1)
                spre[0] = sgate
            if i + 1 < groups:
                out = join((sgate[2:3], sgate[1:2], ent[...], sgate[0:1]), unpack(cgrp[...], sgrp[...]))
                cpre[1] = out[2].astype(BF16)
                spre[1] = stats(out[0], out[1], out[3])
                for copy in pre_copies():
                    copy.start()

    rid_b = lax.broadcasted_iota(jnp.int32, (rows, length), 0)
    cid_b = lax.broadcasted_iota(jnp.int32, (rows, length), 1)

    def attend(r):
        at, end = r * rows, (r + 1) * rows
        decay = jnp.where(
            cid_b[:, :end] <= rid_b[:, :end] + at, stat[at:end, 0:1] - b_row[:, :end] + i_row[:, :end], -jnp.inf)
        peak = jnp.max(decay, axis=-1, keepdims=True)
        scores = dot(q_ref[at:end], k_ref[0:end], ((1,), (1,))) * (hd**-0.5) * jnp.exp(decay - peak)
        stat[at:end, 2:3] = peak
        stat[at:end, 3:4] = jnp.sum(scores, axis=-1, keepdims=True)
        num[at:end] = dot(scores.astype(BF16), v_ref[0:end])

    def attend_end():
        pre = (spre[0, 2:3], spre[0, 1:2], ent[...], spre[0, 0:1])
        joined = join(pre, unpack(cpair[0], spair[0]))
        odd = par == 1
        m_in = jnp.where(odd, joined[1], pre[1])
        n_in = jnp.where(odd, joined[3], pre[3])
        c_in = jnp.where(odd, joined[2], pre[2]).astype(BF16)
        for r in range(nt):
            at, end = r * rows, (r + 1) * rows
            carried = stat[at:end, 0:1] + m_in[:, 0:1]
            local = stat[at:end, 2:3]
            peaks = jnp.maximum(carried, local)
            across = jnp.exp(carried - peaks)
            within = jnp.exp(local - peaks)
            qf = q_ref[at:end].astype(F32)
            den = within * stat[at:end, 3:4] + across * jnp.sum(qf * n_in, axis=-1, keepdims=True)
            top = within * num[at:end] + across * dot(q_ref[at:end], c_in)
            cell = top / jnp.maximum(jnp.abs(den), jnp.exp(-peaks))
            head[at:end] = (cell * hs_ref[...]).astype(BF16)

    def part_copy(j):
        return remote(pout.at[j], prec.at[tp], p_ss.at[j], p_rs.at[tp], (me, j))

    def part_arrival(j):
        return remote(pout.at[j], prec.at[j], p_ss.at[j], p_rs.at[j], (me, j))

    def project(j):
        pout[j] = dot(head[pl.ds(pl.multiple_of(j * rows, rows), rows), :], wo[...]).astype(BF16)

    def send_part(i, c):
        j = lax.rem(tp + i, nt)
        project(j)
        part_copy(j).start()
        return c

    def send_parts():
        lax.fori_loop(1, nt, send_part, 0)
        project(tp)

    def mix():
        total = pout[tp].astype(F32)
        for i in range(1, nt):
            j = lax.rem(tp + i, nt)
            part_arrival(j).wait_recv()
            total = total + prec[j].astype(F32)
        mixed_ref[...] = rms(total, ps_ref[...]).astype(BF16)

    def masks(s, plane, start, count):
        table = info[s]
        slot = lax.broadcasted_iota(jnp.int32, (count, tokens), 0) + start
        own = (plane * 2 + par) * cap
        beside = (plane * 2 + 1 - par) * cap
        slot = jnp.where(slot < cap, own + slot, beside + slot - cap).astype(F32)
        return slot == table[0:1, 0:tokens], slot == table[1:2, 0:tokens], table[2:3, 0:tokens], table[3:4, 0:tokens]

    def hidden(s, e, at):
        is_a, is_b, _, _ = masks(s, z, e * cap, cap)
        place = (is_a | is_b).astype(BF16)
        for c in range(nc):
            chosen[:, c * cw : (c + 1) * cw] = dot(place, tok[s, c]).astype(BF16)
        gate = dot(chosen[...], wg[e])
        up = dot(chosen[...], wu[e])
        hid[at] = (gate / (1.0 + jnp.exp(-gate)) * up).astype(BF16)

    def share(s, e):
        is_a, is_b, w_a, w_b = masks(s, z, e * cap, cap)
        return jnp.sum(jnp.where(is_a, w_a, jnp.where(is_b, w_b, 0.0)), axis=1, keepdims=True)

    def half_of(e):
        return pl.ds(pl.multiple_of(e * cap, 16), cap)

    def down(s, e, at, c, weight):
        answer = dot(hid[at], wd[e, :, c * cw : (c + 1) * cw]) * weight
        ans[s, c, half_of(e), :] = answer.astype(BF16)

    def ret_to(s):
        below = s < z
        to = jnp.where(below, z - 1, z + 1)
        slot = jnp.where((to == s) & jnp.logical_not(below), groups, s)
        return below, to, slot

    def compact_copy(s, e, c):
        _, to, slot = ret_to(s)
        half = half_of(e)
        return remote(ans.at[s, c, half], cin.at[slot, c, half], c_ss.at[s], r_rs.at[slot, c], (to * 2 + par, tp))

    def compact_wait(slot, c):
        remote(ans.at[0, c], cin.at[slot, c], c_ss.at[0], r_rs.at[slot, c], (me, other)).wait_recv()

    def sum_copy(s, c):
        _, to, slot = ret_to(s)
        return remote(rout.at[s, c], rin.at[slot, c], r_ss.at[s], r_rs.at[slot, c], (to * 2 + par, tp))

    def sum_wait(slot, c):
        remote(rout.at[0, c], rin.at[slot, c], r_ss.at[0], r_rs.at[slot, c], (me, other)).wait_recv()

    def at_end(s):
        return jnp.where(s < z, z == groups - 1, z == 0)

    def valid(s):
        return (s >= 0) & (s < groups)

    def arrive(s, rows_too):
        if rows_too:
            @pl.when(at_end(s))
            def _():
                for c in range(nc):
                    tok_wait(s, c)

        remote(info.at[s], info.at[s], i_ss.at[0], i_rs.at[s], (me, other)).wait_recv()

    def answer(s, e, at):
        hidden(s, e, at)
        weight = share(s, e)
        for c in range(nc):
            down(s, e, at, c, weight)

            @pl.when((s != z) & at_end(s))
            def _():
                compact_copy(s, e, c).start()

    def scatter(s, plane, block):
        is_a, is_b, _, _ = masks(s, plane, 0, 2 * cap)
        return dot((is_a | is_b).astype(BF16), block, ((0,), (0,)))

    def upstream(s, slot, near, last, c, put):
        @pl.when(near == last)
        def _():
            compact_wait(slot, c)
            put(scatter(s, last, cin[slot, c]))

        @pl.when(near != last)
        def _():
            sum_wait(slot, c)
            put(rin[slot, c].astype(F32))

    def pass_on(s, c):
        mine = scatter(s, z, ans[s, c])

        def put(more):
            rout[s, c] = (mine + more).astype(BF16)

        below = s < z
        upstream(s, s, jnp.where(below, z + 1, z - 1), jnp.where(below, groups - 1, 0), c, put)
        sum_copy(s, c).start()

    def own_end(c):
        acc[...] = scatter(z, z, ans[z, c])

        def put(more):
            acc[...] += more

        @pl.when(z < groups - 1)
        def _():
            upstream(z, z, z + 1, groups - 1, c, put)

        @pl.when(z > 0)
        def _():
            upstream(z, groups, z - 1, 0, c, put)

        routed_ref[:, pl.ds(pl.multiple_of(c * cw, cw), cw)] = acc[...].astype(BF16)

    def own_first():
        for load in loads:
            load.wait()
        answer(z, 0, 0)

    def near_first():
        def one(side, c):
            s = z + 2 * side - 1

            @pl.when(valid(s))
            def _():
                arrive(s, False)
                answer(s, 0, 0)

            return c

        lax.fori_loop(0, 2, one, 0)

    def near_hidden():
        for j in (0, wc):
            from_core(j)

        def one(side, c):
            s = z + 2 * side - 1

            @pl.when(valid(s))
            def _():
                hidden(s, 1, side)

            return c

        lax.fori_loop(0, 2, one, 0)

    def near_down(c):
        if c % (nc // wc) == 0:
            from_core(2 * wc + c * wc // nc)

        def one(side, carry):
            s = z + 2 * side - 1

            @pl.when(valid(s))
            def _():
                down(s, 1, side, c, share(s, 1))

                @pl.when(at_end(s))
                def _():
                    compact_copy(s, 1, c).start()

            return carry

        lax.fori_loop(0, 2, one, 0)

    def further(d):
        def one(side, carry):
            s = z + d * (2 * side - 1)

            @pl.when(valid(s))
            def _():
                arrive(s, True)

                def first(e, c):
                    hidden(s, e, e)
                    return c

                lax.fori_loop(0, 2, first, 0)
                weights = [share(s, e) for e in range(2)]
                for c in range(nc):
                    for e in range(2):
                        down(s, e, e, c, weights[e])

                        @pl.when(at_end(s))
                        def _():
                            compact_copy(s, e, c).start()

            return carry

        lax.fori_loop(0, 2, one, 0)

    plan = {j: [] for j in range(pieces + 2)}

    def at(part, what, *args):
        plan[min(int(part * pieces / 12), pieces + 1)].append((what, args))

    def spread(start, end, what, *args, chunks=range(nc)):
        for c in chunks:
            at(start + (end - start) * c / nc, what, *args, c)

    at(0, own_first)
    at(1, join_pair)
    at(1, hop, 0)
    at(1, send_rest)
    for r in range(nt):
        at(2 + 2 * r / nt, attend, r)
    at(3, hop, 1)
    at(3, near_arrive, 0)
    spread(3, 5, near_arrive, chunks=range(1, nc))
    lead = nc // 4
    if groups > 3:
        spread(4, 4, near_forward, chunks=range(lead))
    for i in range(2, groups - 1):
        at(5, hop, i)
    at(5, near_first)
    for i in range(1, groups - 2):
        spread(6.3, 11.9, far_forward, i)
    if groups > 3:
        spread(11, 11, near_forward, chunks=range(lead, nc))
    at(8, hop, groups - 1)
    at(8, attend_end)
    at(9, near_hidden)
    for c in range(nc):
        at(10 + 4 * c / nc, near_down, c)
    at(12, send_parts)

    for j in range(pieces + 2):
        if j < pieces:
            from_partner(j)
        if j >= 2:
            from_peers(j - 2)
        for what, args in plan[j]:
            what(*args)

    turns = [1, *range(groups - 1, 1, -1)]
    lag = 3
    further(turns[1])

    @pl.when((z == 0) | (z == groups - 1))
    def _():
        answer(z, 1, 0)

    for d in turns[2:]:
        further(d)

    def last_turn(g):
        return max(turns.index(t) for t in (g, groups - 1 - g) if t)

    def events(t, carry):
        def during(start, what, *args):
            c = t - start

            @pl.when((c >= 0) & (c < nc))
            def _():
                what(*args, c)

        for step, turn in enumerate(turns[1:]):
            for h in range(1, min(turn, groups - 1)):
                @pl.when(z == groups - 1 - h)
                def _():
                    during(step * nc + lag * (h - 1), pass_on, groups - 1 - turn)

                @pl.when(z == h)
                def _():
                    during(step * nc + lag * (h - 1), pass_on, turn)

        @pl.when(t == 3)
        def _():
            @pl.when((z > 0) & (z < groups - 1))
            def _():
                answer(z, 1, 0)

        @pl.when(t == nc + 2)
        def _():
            mix()

        closing = jnp.int32(0)
        for g in range(groups):
            closing = jnp.where(z == g, (last_turn(g) - 1) * nc + lag * max(groups - 3, 1), closing)
        during(closing, own_end)
        return carry

    lax.fori_loop(0, max(groups - 2, 1) * nc + lag * max(groups - 3, 1), events, 0)

    for which in range(3):
        here = quarter(which, tp)
        remote(here, here, x_ss.at[which], w_rs.at[0, 0], (partner, tp)).wait_send()
        for o in range(nt // 2):
            if o:
                remote(here, here, y_ss.at[o, which], w_rs.at[0, 0], (partner, tp)).wait_send()
            remote(here, here, k_ss.at[o, which], w_rs.at[0, 0], (me, other)).wait_send()
    for copy in pair_copies(par):
        copy.wait_send()

    @pl.when(z + 1 < groups)
    def _():
        for copy in pre_copies():
            copy.wait_send()

    def sent(ref, sem):
        remote(ref, ref, sem, t_rs.at[0, 0], (me, other)).wait_send()

    def finish(s, carry):
        @pl.when((s <= z) & (z + 1 < groups))
        def _():
            sent(tok.at[s], t_ss.at[1, s])

        @pl.when((s >= z) & (z > 0))
        def _():
            sent(tok.at[s], t_ss.at[0, s])

        @pl.when(s != z)
        def _():
            info_copy(s, z).wait_send()

            @pl.when(at_end(s))
            def _():
                sent(ans.at[s], c_ss.at[s])

            @pl.when(jnp.logical_not(at_end(s)))
            def _():
                sent(rout.at[s], r_ss.at[s])

        return carry

    lax.fori_loop(0, groups, finish, 0)
    for i in range(1, nt):
        part_copy(lax.rem(tp + i, nt)).wait_send()


def shards(
    n, nt,
    memory_query_matrix, memory_key_matrix, memory_value_matrix,
    input_gate_logits, forget_gate_logits, forget_log_boosts,
    head_norm_scale, memory_output_matrix, projection_norm_scale,
    second_batch_rows, expert_prenorm_scale, selected_expert_index,
    group_route_probability, expert_choice_scores,
    expert_gate_matrix, expert_up_matrix, expert_down_matrix,
):
    length, hd = memory_query_matrix.shape
    tokens, width = second_batch_rows.shape
    hidden = expert_gate_matrix.shape[2]
    cap = 2 * selected_expert_index.shape[1] * tokens // n
    cap = -(-cap // 16) * 16
    rows = length // nt
    vm = pl.BlockSpec(memory_space=pltpu.VMEM)
    hbm = pl.BlockSpec(memory_space=pl.ANY)
    dma = pltpu.SemaphoreType.DMA
    slots = pltpu.VMEM((n, cap, width), BF16)
    groups = n // 2
    nc, wc = 8, 4
    cw = width // nc
    wide = -(-tokens // 128) * 128
    near = groups * tokens * width * 6 < 24 * 1024 * 1024 and nt % 2 == 0 and groups > 3
    if near:
        pair_w = (2, width, hidden)
        pieces = 3 * wc
        slot = (groups, nc, 2 * cap, cw)
        slot_in = (groups + 1, nc, 2 * cap, cw)
        line = (groups, nc, tokens, cw)
        line_in = (groups + 1, nc, tokens, cw)
        return pl.pallas_call(
            functools.partial(plane_kernel, n, nt, cap, nc, wc),
            out_shape=(
                jax.ShapeDtypeStruct((rows, width), BF16),
                jax.ShapeDtypeStruct((tokens, width), BF16),
            ),
            in_specs=[vm] * 7 + [hbm] + [vm] * 6 + [hbm] * 3,
            out_specs=(vm, vm),
            scratch_shapes=[
                pltpu.VMEM(pair_w, BF16),
                pltpu.VMEM(pair_w, BF16),
                pltpu.VMEM((2, hidden, width), BF16),
                pltpu.VMEM((hd, width), BF16),
                pltpu.VMEM(line, BF16),
                pltpu.VMEM((groups, 8, wide), F32),
                pltpu.VMEM((cap, width), BF16),
                pltpu.VMEM((2, cap, hidden), BF16),
                pltpu.VMEM(slot, BF16),
                pltpu.VMEM(slot_in, BF16),
                pltpu.VMEM(line, BF16),
                pltpu.VMEM(line_in, BF16),
                pltpu.VMEM((tokens, cw), F32),
                pltpu.VMEM((2, hd, hd), BF16),
                pltpu.VMEM((2, 8, hd), F32),
                pltpu.VMEM((hd, hd), F32),
                pltpu.VMEM((8, hd), F32),
                pltpu.VMEM((2, hd, hd), BF16),
                pltpu.VMEM((2, 8, hd), F32),
                pltpu.VMEM((hd, hd), F32),
                pltpu.VMEM((length, hd), F32),
                pltpu.VMEM((length, 128), F32),
                pltpu.VMEM((length, hd), BF16),
                pltpu.VMEM((nt, rows, width), BF16),
                pltpu.VMEM((nt, rows, width), BF16),
                dma((4,)),
                dma((3,)), dma((nt // 2, 3)), dma((nt // 2, 3)), dma((nt, pieces)),
                dma((2, groups)), dma((groups, nc)),
                dma((groups,)), dma((groups,)),
                dma((groups,)), dma((groups,)), dma((groups + 1, nc)),
                dma, dma, dma, dma, dma, dma, dma, dma,
                dma((nt,)), dma((nt,)),
            ],
            compiler_params=pltpu.CompilerParams(
                collective_id=0, has_side_effects=True, vmem_limit_bytes=62 * 1024 * 1024
            ),
        )(
            memory_query_matrix, memory_key_matrix, memory_value_matrix,
            input_gate_logits, forget_gate_logits, forget_log_boosts,
            head_norm_scale[None], memory_output_matrix, projection_norm_scale[None],
            second_batch_rows, expert_prenorm_scale[None], selected_expert_index.T,
            group_route_probability[None], expert_choice_scores.T,
            expert_gate_matrix, expert_up_matrix, expert_down_matrix,
        )
    buffers = [
        slots, slots, slots, slots,
        pltpu.VMEM((tokens, width), BF16),
        pltpu.VMEM((tokens, width), F32),
    ]
    sems = [dma((n,))] * 4
    return pl.pallas_call(
        functools.partial(kernel, n, nt, cap),
        out_shape=(
            jax.ShapeDtypeStruct((rows, width), BF16),
            jax.ShapeDtypeStruct((tokens, width), BF16),
        ),
        in_specs=[vm] * 7 + [hbm] + [vm] * 6 + [hbm] * 3,
        out_specs=(vm, vm),
        scratch_shapes=[
            pltpu.VMEM((width, hidden), BF16),
            pltpu.VMEM((width, hidden), BF16),
            pltpu.VMEM((hidden, width), BF16),
            pltpu.VMEM((hd, width), BF16),
            *buffers,
            pltpu.VMEM((2, hd, hd), BF16),
            pltpu.VMEM((2, 8, hd), F32),
            pltpu.VMEM((n // 2, hd, hd), BF16),
            pltpu.VMEM((n // 2, 8, hd), F32),
            pltpu.VMEM((hd, hd), F32),
            pltpu.VMEM((length, hd), BF16),
            pltpu.VMEM((nt, rows, width), BF16),
            pltpu.VMEM((nt, rows, width), BF16),
            dma((4,)),
            *sems,
            dma, dma, dma, dma,
            dma((n // 2,)), dma((n // 2,)), dma((n // 2,)), dma((n // 2,)),
            dma((nt,)), dma((nt,)),
        ],
        compiler_params=pltpu.CompilerParams(
            collective_id=0, has_side_effects=True, vmem_limit_bytes=62 * 1024 * 1024
        ),
    )(
        memory_query_matrix, memory_key_matrix, memory_value_matrix,
        input_gate_logits, forget_gate_logits, forget_log_boosts,
        head_norm_scale[None], memory_output_matrix, projection_norm_scale[None],
        second_batch_rows, expert_prenorm_scale[None], selected_expert_index,
        group_route_probability[:, None], expert_choice_scores,
        expert_gate_matrix, expert_up_matrix, expert_down_matrix,
    )


def solution(mesh):
    return jax.shard_map(
        functools.partial(shards, mesh.shape["ep"], mesh.shape["tp"]),
        mesh=mesh,
        in_specs=(
            P("ep", "tp"), P("ep", "tp"), P("ep", "tp"),
            P("tp", "ep"), P("tp", "ep"), P("tp", "ep"),
            P("tp"), P(), P(),
            P(("ep", "tp"), None), P(), P(("ep", "tp"), None),
            P(("ep", "tp")), P(("ep", "tp"), None),
            P("ep", None, None), P("ep", None, None), P("ep", None, None),
        ),
        out_specs=(P(("ep", "tp"), None), P(("ep", "tp"), None)),
        check_vma=False,
    )
```

```python
import functools

import jax
import jax.numpy as jnp
from jax import lax
from jax.experimental import pallas as pl
from jax.experimental.pallas import tpu as pltpu
from jax.sharding import PartitionSpec as P

FLOOR = -1e30
EPS = 1e-06
MESH = pl.DeviceIdType.MESH
F32 = jnp.float32
BF16 = jnp.bfloat16


def rms(values, gain):
    squares = jnp.mean(values * values, axis=-1, keepdims=True)
    return values * lax.rsqrt(squares + EPS) * gain


def dot(a, b, dims=((1,), (0,)), precision=None):
    return lax.dot_general(a, b, (dims, ((), ())), preferred_element_type=F32, precision=precision)


def join(early, late):
    total_e, peak_e, mem_e, nor_e = early
    total_l, peak_l, mem_l, nor_l = late
    peak = jnp.maximum(total_l + peak_e, peak_l)
    fe = jnp.exp(total_l + peak_e - peak)
    fl = jnp.exp(peak_l - peak)
    return (total_e + total_l, peak, fe * mem_e + fl * mem_l, fe * nor_e + fl * nor_l)


def kernel(
    n, nt, cap,
    q_ref, k_ref, v_ref, ig_ref, fg_ref, fb_ref, hs_ref, wo_hbm, ps_ref,
    x_ref, es_ref, ids_ref, grp_ref, sc_ref, wg_hbm, wu_hbm, wd_hbm,
    mixed_ref, routed_ref,
    wg, wu, wd, wo, out, recv, ans, back, ffn, acc,
    cpair, spair, cgrp, sgrp, ent, head, pout, prec,
    wsem, d_ss, d_rs, a_ss, a_rs, c1s, c1r, s1s, s1r, c2s, c2r, s2s, s2r, p_ss, p_rs,
):
    me = lax.axis_index("ep")
    tp = lax.axis_index("tp")
    groups = n // 2
    grp = me // 2
    par = lax.rem(me, 2)
    partner = me + 1 - 2 * par
    tokens, width = x_ref.shape
    length, hd = q_ref.shape
    rows = mixed_ref.shape[0]

    barrier = pltpu.get_barrier_semaphore()

    def greet(i, c):
        pl.semaphore_signal(barrier, inc=1, device_id=(lax.rem(me + i, n), tp), device_id_type=MESH)
        return c

    lax.fori_loop(1, n, greet, 0)
    for j in range(1, nt):
        pl.semaphore_signal(barrier, inc=1, device_id=(me, lax.rem(tp + j, nt)), device_id_type=MESH)

    loads = [
        pltpu.make_async_copy(wg_hbm.at[0], wg, wsem.at[0]),
        pltpu.make_async_copy(wu_hbm.at[0], wu, wsem.at[1]),
        pltpu.make_async_copy(wd_hbm.at[0], wd, wsem.at[2]),
        pltpu.make_async_copy(wo_hbm.at[pl.ds(pl.multiple_of(tp * hd, hd), hd)], wo, wsem.at[3]),
    ]
    for load in loads:
        load.start()

    fg = fg_ref[...]
    lk = jnp.minimum(fg, 0.0) - jnp.log1p(jnp.exp(-jnp.abs(fg))) + fb_ref[...]
    rid = lax.broadcasted_iota(jnp.int32, (length, length), 0)
    cid = lax.broadcasted_iota(jnp.int32, (length, length), 1)
    upper = (rid <= cid).astype(F32)
    b_row = dot(jnp.broadcast_to(lk, (8, length)), upper, precision=lax.Precision.HIGHEST)[0:1]
    i_row = ig_ref[...]
    last = b_row[:, length - 1 : length]
    g_row = last - b_row + i_row
    m_loc = jnp.max(g_row, axis=-1, keepdims=True)
    which = lax.broadcasted_iota(jnp.int32, (128, length), 0)
    cols = jnp.where(which == 0, b_row, g_row).T
    b_col = cols[:, 0:1]
    g_col = cols[:, 1:2]
    kw = k_ref[...].astype(F32) * (jnp.exp(g_col - m_loc) * (hd**-0.5))
    c_loc = dot(kw.astype(BF16), v_ref[...], ((0,), (0,)))
    n_loc = jnp.sum(kw, axis=0, keepdims=True)
    stat_id = lax.broadcasted_iota(jnp.int32, (8, hd), 0)

    def stats(total, peak, nor):
        return jnp.where(stat_id == 0, nor, jnp.where(stat_id == 1, peak, total))

    cpair[par] = c_loc.astype(BF16)
    spair[par] = stats(last, m_loc, n_loc)

    pl.semaphore_wait(barrier, n - 1 + nt - 1)

    def pair_copies():
        return [
            pltpu.make_async_remote_copy(
                src_ref=cpair.at[par], dst_ref=cpair.at[par], send_sem=c1s, recv_sem=c1r,
                device_id=(partner, tp), device_id_type=MESH),
            pltpu.make_async_remote_copy(
                src_ref=spair.at[par], dst_ref=spair.at[par], send_sem=s1s, recv_sem=s1r,
                device_id=(partner, tp), device_id_type=MESH),
        ]

    for copy in pair_copies():
        copy.start()

    ffn[...] = rms(x_ref[...].astype(F32), es_ref[...]).astype(BF16)
    ids = ids_ref[...]
    first, second = ids[:, 0:1], ids[:, 1:2]
    lane_e = lax.broadcasted_iota(jnp.int32, (tokens, n), 1)
    named = ((lane_e == first) | (lane_e == second)).astype(F32)
    tr = lax.broadcasted_iota(jnp.int32, (tokens, tokens), 0)
    tc = lax.broadcasted_iota(jnp.int32, (tokens, tokens), 1)
    rank = dot((tc < tr).astype(BF16), named.astype(BF16))
    slot_a = first * cap + jnp.sum(jnp.where(lane_e == first, rank, 0.0), axis=1, keepdims=True).astype(jnp.int32)
    slot_b = second * cap + jnp.sum(jnp.where(lane_e == second, rank, 0.0), axis=1, keepdims=True).astype(jnp.int32)
    score = sc_ref[...]
    ex = jnp.exp(score - jnp.max(score, axis=-1, keepdims=True))
    route = grp_ref[...] * (ex / jnp.sum(ex, axis=-1, keepdims=True))
    rw_a, rw_b = route[:, 0:1], route[:, 1:2]
    lane_c = lax.broadcasted_iota(jnp.int32, (tokens, cap), 1)

    def pack(e):
        lane = lane_c + e * cap
        place = ((lane == slot_a) | (lane == slot_b)).astype(BF16)
        out[e] = dot(place, ffn[...], ((0,), (0,))).astype(BF16)

    def offset(i):
        return n // 2 + jnp.where(lax.rem(i, 2) == 0, i // 2, -((i + 1) // 2))

    def dispatch_copy(e):
        return pltpu.make_async_remote_copy(
            src_ref=out.at[e], dst_ref=recv.at[me], send_sem=d_ss.at[e], recv_sem=d_rs.at[me],
            device_id=(e, tp), device_id_type=MESH)

    def dispatch_arrival(s):
        return pltpu.make_async_remote_copy(
            src_ref=out.at[s], dst_ref=recv.at[s], send_sem=d_ss.at[s], recv_sem=d_rs.at[s],
            device_id=(s, tp), device_id_type=MESH)

    def answer_copy(s):
        return pltpu.make_async_remote_copy(
            src_ref=ans.at[s], dst_ref=back.at[me], send_sem=a_ss.at[s], recv_sem=a_rs.at[me],
            device_id=(s, tp), device_id_type=MESH)

    def answer_arrival(e):
        return pltpu.make_async_remote_copy(
            src_ref=ans.at[e], dst_ref=back.at[e], send_sem=a_ss.at[e], recv_sem=a_rs.at[e],
            device_id=(e, tp), device_id_type=MESH)

    for copy in pair_copies():
        copy.wait_send()
    def pair_arrival():
        return [
            pltpu.make_async_remote_copy(
                src_ref=cpair.at[1 - par], dst_ref=cpair.at[1 - par], send_sem=c1s, recv_sem=c1r,
                device_id=(partner, tp), device_id_type=MESH),
            pltpu.make_async_remote_copy(
                src_ref=spair.at[1 - par], dst_ref=spair.at[1 - par], send_sem=s1s, recv_sem=s1r,
                device_id=(partner, tp), device_id_type=MESH),
        ]

    for copy in pair_arrival():
        copy.wait_recv()

    def unpack(c, s):
        return (s[2:3], s[1:2], c.astype(F32), s[0:1])

    both = join(unpack(cpair[0], spair[0]), unpack(cpair[1], spair[1]))
    cgrp[grp] = both[2].astype(BF16)
    sgrp[grp] = stats(both[0], both[1], both[3])

    def group_copies(g):
        to = (g * 2 + par, tp)
        return [
            pltpu.make_async_remote_copy(
                src_ref=cgrp.at[grp], dst_ref=cgrp.at[grp], send_sem=c2s.at[g], recv_sem=c2r.at[grp],
                device_id=to, device_id_type=MESH),
            pltpu.make_async_remote_copy(
                src_ref=sgrp.at[grp], dst_ref=sgrp.at[grp], send_sem=s2s.at[g], recv_sem=s2r.at[grp],
                device_id=to, device_id_type=MESH),
        ]

    def group_arrivals(g):
        at = (g * 2 + par, tp)
        return [
            pltpu.make_async_remote_copy(
                src_ref=cgrp.at[g], dst_ref=cgrp.at[g], send_sem=c2s.at[g], recv_sem=c2r.at[g],
                device_id=at, device_id_type=MESH),
            pltpu.make_async_remote_copy(
                src_ref=sgrp.at[g], dst_ref=sgrp.at[g], send_sem=s2s.at[g], recv_sem=s2r.at[g],
                device_id=at, device_id_type=MESH),
        ]

    def send_group(g, c):
        for copy in group_copies(g):
            copy.start()
        return c

    lax.fori_loop(grp + 1, groups, send_group, 0)

    def send_tokens(i, c):
        e = lax.rem(me + offset(i), n)
        pack(e)
        dispatch_copy(e).start()
        return c

    lax.fori_loop(0, n - 1, send_tokens, 0)
    pack(me)
    for load in loads:
        load.wait()

    def expert(chosen):
        gate = dot(chosen, wg[...])
        up = dot(chosen, wu[...])
        hidden = (gate / (1.0 + jnp.exp(-gate)) * up).astype(BF16)
        return dot(hidden, wd[...]).astype(BF16)

    ans[me] = expert(out[me])

    ent[...] = jnp.zeros(ent.shape, F32)
    row1 = jnp.zeros((1, hd), F32)

    def enter(g, carry):
        total, peak, nor = carry
        for copy in group_arrivals(g):
            copy.wait_recv()
        total, peak, mem, nor = join((total, peak, ent[...], nor), unpack(cgrp[g], sgrp[g]))
        ent[...] = mem
        return total, peak, nor

    total, peak, nor = lax.fori_loop(0, grp, enter, (row1, row1 + FLOOR, row1))
    joined = join((total, peak, ent[...], nor), unpack(cpair[0], spair[0]))
    odd = par == 1
    m_in = jnp.where(odd, joined[1], peak)
    n_in = jnp.where(odd, joined[3], nor)
    c_in = jnp.where(odd, joined[2], ent[...])

    carried = b_col + m_in[:, 0:1]
    decay = jnp.where(cid <= rid, b_col - b_row + i_row, -jnp.inf)
    peaks = jnp.maximum(carried, jnp.max(decay, axis=-1, keepdims=True))
    across = jnp.exp(carried - peaks)
    scores = dot(q_ref[...], k_ref[...], ((1,), (1,))) * (hd**-0.5) * jnp.exp(decay - peaks)
    qf = q_ref[...].astype(F32)
    den = jnp.sum(scores, axis=-1, keepdims=True) + across * jnp.sum(qf * n_in, axis=-1, keepdims=True)
    num = dot(scores.astype(BF16), v_ref[...]) + across * dot(q_ref[...], c_in.astype(BF16))
    cell = num / jnp.maximum(jnp.abs(den), jnp.exp(-peaks))
    head[...] = (cell * hs_ref[...]).astype(BF16)

    def part_copy(j):
        return pltpu.make_async_remote_copy(
            src_ref=pout.at[j], dst_ref=prec.at[tp], send_sem=p_ss.at[j], recv_sem=p_rs.at[tp],
            device_id=(me, j), device_id_type=MESH)

    def part_arrival(j):
        return pltpu.make_async_remote_copy(
            src_ref=pout.at[j], dst_ref=prec.at[j], send_sem=p_ss.at[j], recv_sem=p_rs.at[j],
            device_id=(me, j), device_id_type=MESH)

    def project(j):
        pout[j] = dot(head[pl.ds(pl.multiple_of(j * rows, rows), rows), :], wo[...]).astype(BF16)

    def send_part(i, c):
        j = lax.rem(tp + i, nt)
        project(j)
        part_copy(j).start()
        return c

    lax.fori_loop(1, nt, send_part, 0)
    project(tp)

    def serve(i, c):
        s = lax.rem(me - offset(i) + n, n)
        dispatch_arrival(s).wait_recv()
        ans[s] = expert(recv[s])
        answer_copy(s).start()
        return c

    lax.fori_loop(0, n - 1, serve, 0)

    def mix(i, total):
        j = lax.rem(tp + i, nt)
        part_arrival(j).wait_recv()
        return total + prec[j].astype(F32)

    projected = pout[tp].astype(F32)
    for i in range(1, nt):
        projected = mix(i, projected)
    mixed_ref[...] = rms(projected, ps_ref[...]).astype(BF16)

    def weigh(e, block):
        lane = lane_c + e * cap
        w = jnp.where(lane == slot_a, rw_a, jnp.where(lane == slot_b, rw_b, 0.0))
        high = w.astype(BF16)
        low = (w - high.astype(F32)).astype(BF16)
        return dot(high, block) + dot(low, block)

    acc[...] = weigh(me, ans[me])

    def collect(i, c):
        e = lax.rem(me + offset(i), n)
        answer_arrival(e).wait_recv()
        acc[...] += weigh(e, back[e])
        return c

    lax.fori_loop(0, n - 1, collect, 0)
    routed_ref[...] = acc[...].astype(BF16)

    def finish(i, c):
        e = lax.rem(me + i, n)
        dispatch_copy(e).wait_send()
        answer_copy(e).wait_send()
        return c

    lax.fori_loop(1, n, finish, 0)

    def finish_group(g, c):
        for copy in group_copies(g):
            copy.wait_send()
        return c

    lax.fori_loop(grp + 1, groups, finish_group, 0)
    for i in range(1, nt):
        part_copy(lax.rem(tp + i, nt)).wait_send()


def plane_kernel(
    n, nt, cap, nc, wc,
    q_ref, k_ref, v_ref, ig_ref, fg_ref, fb_ref, hs_ref, wo_hbm, ps_ref,
    x_ref, es_ref, ids_ref, grp_ref, sc_ref, wg_hbm, wu_hbm, wd_hbm,
    mixed_ref, routed_ref,
    wg, wu, wd, wo, tok, info, chosen, hid, ans, cin, rout, rin, acc, gu,
    cpair, spair, cgrp, sgrp, cpre, spre, ent, num, stat, head, pout, prec,
    wsem, x_ss, y_ss, k_ss, w_rs, t_ss, t_rs, i_ss, i_rs, c_ss, r_ss, r_rs,
    c1s, c1r, s1s, s1r, c2s, c2r, s2s, s2r, p_ss, p_rs,
):
    me = lax.axis_index("ep")
    tp = lax.axis_index("tp")
    groups = n // 2
    z = me // 2
    par = lax.rem(me, 2)
    partner = me + 1 - 2 * par
    other = tp + 1 - 2 * lax.rem(tp, 2)
    tokens, width = x_ref.shape
    length, hd = q_ref.shape
    rows = mixed_ref.shape[0]
    cw = width // nc
    pieces = 3 * wc

    def remote(src, dst, ss, rs, to):
        return pltpu.make_async_remote_copy(
            src_ref=src, dst_ref=dst, send_sem=ss, recv_sem=rs, device_id=to, device_id_type=MESH)

    barrier = pltpu.get_barrier_semaphore()

    def greet(i, c):
        pl.semaphore_signal(barrier, inc=1, device_id=(lax.rem(me + i, n), tp), device_id_type=MESH)
        return c

    lax.fori_loop(1, n, greet, 0)
    for j in range(1, nt):
        pl.semaphore_signal(barrier, inc=1, device_id=(me, lax.rem(tp + j, nt)), device_id_type=MESH)

    loads = [
        pltpu.make_async_copy(wg_hbm.at[0], wg.at[0], wsem.at[0]),
        pltpu.make_async_copy(wu_hbm.at[0], wu.at[0], wsem.at[1]),
        pltpu.make_async_copy(wd_hbm.at[0], wd.at[0], wsem.at[2]),
        pltpu.make_async_copy(wo_hbm.at[pl.ds(pl.multiple_of(tp * hd, hd), hd)], wo, wsem.at[3]),
    ]
    for load in loads:
        load.start()

    def piece(ref, lead, part, j):
        which, at = divmod(j, wc)
        if which < 2:
            quarter = ref[which].shape[1] // nt
            step = quarter // wc
            return ref[which].at[lead, pl.ds(pl.multiple_of(part * quarter + at * step, step), step)]
        quarter = ref[2].shape[1] // nt
        step = width // wc
        return ref[2].at[lead, pl.ds(pl.multiple_of(part * quarter, quarter), quarter), pl.ds(at * step, step)]

    held = (wg, wu, wd)
    given = (wg_hbm, wu_hbm, wd_hbm)

    def x_copy(j):
        return remote(piece(given, 0, tp, j), piece(held, 1, tp, j), x_ss.at[j // wc], w_rs.at[tp, j], (partner, tp))

    def y_copy(o, j):
        here = piece(held, 1, tp, j)
        return remote(here, here, y_ss.at[o, j // wc], w_rs.at[tp, j], (me, lax.rem(tp + 2 * o, nt)))

    def core_copy(part, j):
        here = piece(held, 1, part, j)
        sem = w_rs.at[part, j // wc * wc if j < 2 * wc else j]
        return remote(here, here, k_ss.at[part // 2, j // wc], sem, (me, other))

    def weight_wait(part, j):
        here = piece(held, 1, part, j)
        remote(here, here, x_ss.at[j // wc], w_rs.at[part, j], (me, other)).wait_recv()

    def quarter(which, part):
        step = held[which].shape[1] // nt
        return held[which].at[1, pl.ds(pl.multiple_of(part * step, step), step)]

    def from_partner(j):
        weight_wait(tp, j)
        for o in range(1, nt // 2):
            y_copy(o, j).start()
        core_copy(tp, j).start()

    def from_peers(j):
        for o in range(1, nt // 2):
            part = lax.rem(tp + 2 * o, nt)
            weight_wait(part, j)
            core_copy(part, j).start()

    def from_core(j):
        for o in range(nt // 2):
            part = lax.rem(other + 2 * o, nt)
            if j < 2 * wc:
                here = quarter(j // wc, part)
                remote(here, here, x_ss.at[0], w_rs.at[part, j], (me, other)).wait_recv()
            else:
                weight_wait(part, j)

    def tok_copy(up, s, c):
        here = tok.at[s, c]
        return remote(here, here, t_ss.at[up, s], t_rs.at[s, c], ((z - 1 + 2 * up) * 2 + par, tp))

    def tok_wait(s, c):
        here = tok.at[s, c]
        remote(here, here, t_ss.at[0, s], t_rs.at[s, c], (me, other)).wait_recv()

    def send_own(c):
        @pl.when(z + 1 < groups)
        def _():
            tok_copy(1, z, c).start()

        @pl.when(z > 0)
        def _():
            tok_copy(0, z, c).start()

    def near_arrive(c):
        @pl.when(z > 0)
        def _():
            tok_wait(z - 1, c)

            @pl.when((z == 1) & (z + 1 < groups))
            def _():
                tok_copy(1, z - 1, c).start()

        @pl.when(z + 1 < groups)
        def _():
            tok_wait(z + 1, c)

            @pl.when((z == groups - 2) & (z > 0))
            def _():
                tok_copy(0, z + 1, c).start()

    def near_forward(c):
        @pl.when((z >= 2) & (z + 1 < groups))
        def _():
            tok_copy(1, z - 1, c).start()

        @pl.when((z <= groups - 3) & (z > 0))
        def _():
            tok_copy(0, z + 1, c).start()

    def far_forward(i, c):
        @pl.when((i < z) & (z + 1 < groups))
        def _():
            tok_wait(i - 1, c)
            tok_copy(1, i - 1, c).start()

        @pl.when((i < groups - 1 - z) & (z > 0))
        def _():
            tok_wait(groups - i, c)
            tok_copy(0, groups - i, c).start()

    normed = rms(x_ref[...].astype(F32), es_ref[...]).astype(BF16)
    for c in range(nc):
        tok[z, c] = normed[:, c * cw : (c + 1) * cw]

    pl.semaphore_wait(barrier, n - 1 + nt - 1)
    early = 5 * nc // 8
    for c in range(early):
        send_own(c)
    for j in range(2):
        x_copy(j).start()

    first, second = ids_ref[0:1, :], ids_ref[1:2, :]
    sub_e = lax.broadcasted_iota(jnp.int32, (n, tokens), 0)
    named = ((sub_e == first) | (sub_e == second)).astype(BF16)
    tr = lax.broadcasted_iota(jnp.int32, (tokens, tokens), 0)
    tc = lax.broadcasted_iota(jnp.int32, (tokens, tokens), 1)
    rank = dot(named, (tr < tc).astype(BF16))
    slot_a = first.astype(F32) * cap + jnp.sum(jnp.where(sub_e == first, rank, 0.0), axis=0, keepdims=True)
    slot_b = second.astype(F32) * cap + jnp.sum(jnp.where(sub_e == second, rank, 0.0), axis=0, keepdims=True)
    score_a, score_b = sc_ref[0:1, :], sc_ref[1:2, :]
    top = jnp.maximum(score_a, score_b)
    ex_a, ex_b = jnp.exp(score_a - top), jnp.exp(score_b - top)
    rw_a = grp_ref[...] * (ex_a / (ex_a + ex_b))
    rw_b = grp_ref[...] * (ex_b / (ex_a + ex_b))
    sub_i = lax.broadcasted_iota(jnp.int32, (8, tokens), 0)
    table = jnp.where(sub_i == 0, slot_a, jnp.where(sub_i == 1, slot_b,
        jnp.where(sub_i == 2, rw_a, jnp.where(sub_i == 3, rw_b, 0.0))))
    info[z] = jnp.zeros(info.shape[1:], F32)
    info[z, :, 0:tokens] = table

    def info_copy(g, s):
        return remote(info.at[s], info.at[s], i_ss.at[g], i_rs.at[s], (g * 2 + par, tp))

    def send_info(j, c):
        info_copy(lax.rem(z + j, groups), z).start()
        return c

    lax.fori_loop(1, groups, send_info, 0)

    fg = fg_ref[...]
    lk = jnp.minimum(fg, 0.0) - jnp.log1p(jnp.exp(-jnp.abs(fg))) + fb_ref[...]
    rid = lax.broadcasted_iota(jnp.int32, (length, length), 0)
    cid = lax.broadcasted_iota(jnp.int32, (length, length), 1)
    upper = (rid <= cid).astype(F32)
    b_row = dot(jnp.broadcast_to(lk, (8, length)), upper, precision=lax.Precision.HIGHEST)[0:1]
    i_row = ig_ref[...]
    last = b_row[:, length - 1 : length]
    g_row = last - b_row + i_row
    m_loc = jnp.max(g_row, axis=-1, keepdims=True)
    which_row = lax.broadcasted_iota(jnp.int32, (128, length), 0)
    stat[...] = jnp.where(which_row == 0, b_row, g_row).T
    kw = k_ref[...].astype(F32) * (jnp.exp(stat[:, 1:2] - m_loc) * (hd**-0.5))
    n_loc = jnp.sum(kw, axis=0, keepdims=True)
    stat_id = lax.broadcasted_iota(jnp.int32, (8, hd), 0)

    def stats(total, peak, nor):
        return jnp.where(stat_id == 0, nor, jnp.where(stat_id == 1, peak, total))

    def unpack(c, s):
        return (s[2:3], s[1:2], c.astype(F32), s[0:1])

    cpair[par] = dot(kw.astype(BF16), v_ref[...], ((0,), (0,))).astype(BF16)
    spair[par] = stats(last, m_loc, n_loc)

    def pair_copies(at):
        return [
            remote(cpair.at[at], cpair.at[at], c1s, c1r, (partner, tp)),
            remote(spair.at[at], spair.at[at], s1s, s1r, (partner, tp)),
        ]

    for copy in pair_copies(par):
        copy.start()
    for j in range(2, pieces):
        x_copy(j).start()
    def send_rest():
        for c in range(early, nc):
            send_own(c)

    def pre_copies():
        to = ((z + 1) * 2 + par, tp)
        return [
            remote(cpre.at[1], cpre.at[0], c2s, c2r, to),
            remote(spre.at[1], spre.at[0], s2s, s2r, to),
        ]

    def join_pair():
        for copy in pair_copies(1 - par):
            copy.wait_recv()
        both = join(unpack(cpair[0], spair[0]), unpack(cpair[1], spair[1]))
        cgrp[...] = both[2]
        sgrp[...] = stats(both[0], both[1], both[3])

    def hop(i):
        @pl.when(z == i)
        def _():
            if i:
                for copy in pre_copies():
                    copy.wait_recv()
                before = unpack(cpre[0], spre[0])
                ent[...] = before[2]
                sgate = spre[0]
            else:
                ent[...] = jnp.zeros(ent.shape, F32)
                row1 = jnp.zeros((1, hd), F32)
                sgate = stats(row1, row1 + FLOOR, row1)
                spre[0] = sgate
            if i + 1 < groups:
                out = join((sgate[2:3], sgate[1:2], ent[...], sgate[0:1]), unpack(cgrp[...], sgrp[...]))
                cpre[1] = out[2].astype(BF16)
                spre[1] = stats(out[0], out[1], out[3])
                for copy in pre_copies():
                    copy.start()

    rid_b = lax.broadcasted_iota(jnp.int32, (rows, length), 0)
    cid_b = lax.broadcasted_iota(jnp.int32, (rows, length), 1)

    def attend(r):
        at, end = r * rows, (r + 1) * rows
        decay = jnp.where(
            cid_b[:, :end] <= rid_b[:, :end] + at, stat[at:end, 0:1] - b_row[:, :end] + i_row[:, :end], -jnp.inf)
        peak = jnp.max(decay, axis=-1, keepdims=True)
        scores = dot(q_ref[at:end], k_ref[0:end], ((1,), (1,))) * (hd**-0.5) * jnp.exp(decay - peak)
        stat[at:end, 2:3] = peak
        stat[at:end, 3:4] = jnp.sum(scores, axis=-1, keepdims=True)
        num[at:end] = dot(scores.astype(BF16), v_ref[0:end])

    def attend_end():
        pre = (spre[0, 2:3], spre[0, 1:2], ent[...], spre[0, 0:1])
        joined = join(pre, unpack(cpair[0], spair[0]))
        odd = par == 1
        m_in = jnp.where(odd, joined[1], pre[1])
        n_in = jnp.where(odd, joined[3], pre[3])
        c_in = jnp.where(odd, joined[2], pre[2]).astype(BF16)
        for r in range(nt):
            at, end = r * rows, (r + 1) * rows
            carried = stat[at:end, 0:1] + m_in[:, 0:1]
            local = stat[at:end, 2:3]
            peaks = jnp.maximum(carried, local)
            across = jnp.exp(carried - peaks)
            within = jnp.exp(local - peaks)
            qf = q_ref[at:end].astype(F32)
            den = within * stat[at:end, 3:4] + across * jnp.sum(qf * n_in, axis=-1, keepdims=True)
            top = within * num[at:end] + across * dot(q_ref[at:end], c_in)
            cell = top / jnp.maximum(jnp.abs(den), jnp.exp(-peaks))
            head[at:end] = (cell * hs_ref[...]).astype(BF16)

    def part_copy(j):
        return remote(pout.at[j], prec.at[tp], p_ss.at[j], p_rs.at[tp], (me, j))

    def part_arrival(j):
        return remote(pout.at[j], prec.at[j], p_ss.at[j], p_rs.at[j], (me, j))

    def project(j):
        pout[j] = dot(head[pl.ds(pl.multiple_of(j * rows, rows), rows), :], wo[...]).astype(BF16)

    def send_part(i, c):
        j = lax.rem(tp + i, nt)
        project(j)
        part_copy(j).start()
        return c

    def send_parts():
        lax.fori_loop(1, nt, send_part, 0)
        project(tp)

    def mix():
        total = pout[tp].astype(F32)
        for i in range(1, nt):
            j = lax.rem(tp + i, nt)
            part_arrival(j).wait_recv()
            total = total + prec[j].astype(F32)
        mixed_ref[...] = rms(total, ps_ref[...]).astype(BF16)

    def masks(s, plane, start, count):
        table = info[s]
        slot = lax.broadcasted_iota(jnp.int32, (count, tokens), 0) + start
        own = (plane * 2 + par) * cap
        beside = (plane * 2 + 1 - par) * cap
        slot = jnp.where(slot < cap, own + slot, beside + slot - cap).astype(F32)
        return slot == table[0:1, 0:tokens], slot == table[1:2, 0:tokens], table[2:3, 0:tokens], table[3:4, 0:tokens]

    def hidden(s, e, at):
        is_a, is_b, _, _ = masks(s, z, e * cap, cap)
        place = (is_a | is_b).astype(BF16)
        for c in range(nc):
            chosen[:, c * cw : (c + 1) * cw] = dot(place, tok[s, c]).astype(BF16)
        gate = dot(chosen[...], wg[e])
        up = dot(chosen[...], wu[e])
        hid[at] = (gate / (1.0 + jnp.exp(-gate)) * up).astype(BF16)

    def share(s, e):
        is_a, is_b, w_a, w_b = masks(s, z, e * cap, cap)
        return jnp.sum(jnp.where(is_a, w_a, jnp.where(is_b, w_b, 0.0)), axis=1, keepdims=True)

    def half_of(e):
        return pl.ds(pl.multiple_of(e * cap, 16), cap)

    def down(s, e, at, c, weight):
        answer = dot(hid[at], wd[e, :, c * cw : (c + 1) * cw]) * weight
        ans[s, c, half_of(e), :] = answer.astype(BF16)

    def ret_to(s):
        below = s < z
        to = jnp.where(below, z - 1, z + 1)
        slot = jnp.where((to == s) & jnp.logical_not(below), groups, s)
        return below, to, slot

    def compact_copy(s, e, c):
        _, to, slot = ret_to(s)
        half = half_of(e)
        return remote(ans.at[s, c, half], cin.at[slot, c, half], c_ss.at[s], r_rs.at[slot, c], (to * 2 + par, tp))

    def compact_wait(slot, c):
        remote(ans.at[0, c], cin.at[slot, c], c_ss.at[0], r_rs.at[slot, c], (me, other)).wait_recv()

    def sum_copy(s, c):
        _, to, slot = ret_to(s)
        return remote(rout.at[s, c], rin.at[slot, c], r_ss.at[s], r_rs.at[slot, c], (to * 2 + par, tp))

    def sum_wait(slot, c):
        remote(rout.at[0, c], rin.at[slot, c], r_ss.at[0], r_rs.at[slot, c], (me, other)).wait_recv()

    def at_end(s):
        return jnp.where(s < z, z == groups - 1, z == 0)

    def valid(s):
        return (s >= 0) & (s < groups)

    def arrive(s, rows_too):
        if rows_too:
            @pl.when(at_end(s))
            def _():
                for c in range(nc):
                    tok_wait(s, c)

        remote(info.at[s], info.at[s], i_ss.at[0], i_rs.at[s], (me, other)).wait_recv()

    def answer(s, e, at):
        hidden(s, e, at)
        weight = share(s, e)
        for g in range(wc):
            for c in group(g):
                down(s, e, at, c, weight)

            @pl.when((s != z) & at_end(s))
            def _():
                for c in group(g):
                    compact_copy(s, e, c).start()

    def scatter(s, plane, block):
        is_a, is_b, _, _ = masks(s, plane, 0, 2 * cap)
        return dot((is_a | is_b).astype(BF16), block, ((0,), (0,)))

    def upstream(s, slot, near, last, c, put):
        @pl.when(near == last)
        def _():
            compact_wait(slot, c)
            put(scatter(s, last, cin[slot, c]))

        @pl.when(near != last)
        def _():
            sum_wait(slot, c)
            put(rin[slot, c].astype(F32))

    def pass_on(s, c):
        mine = scatter(s, z, ans[s, c])

        def put(more):
            rout[s, c] = (mine + more).astype(BF16)

        below = s < z
        upstream(s, s, jnp.where(below, z + 1, z - 1), jnp.where(below, groups - 1, 0), c, put)
        sum_copy(s, c).start()

    def own_end(c):
        acc[...] = scatter(z, z, ans[z, c])

        def put(more):
            acc[...] += more

        @pl.when(z < groups - 1)
        def _():
            upstream(z, z, z + 1, groups - 1, c, put)

        @pl.when(z > 0)
        def _():
            upstream(z, groups, z - 1, 0, c, put)

        routed_ref[:, pl.ds(pl.multiple_of(c * cw, cw), cw)] = acc[...].astype(BF16)

    def own_first():
        for load in loads:
            load.wait()
        answer(z, 0, 0)

    def near_first():
        def one(side, c):
            s = z + 2 * side - 1

            @pl.when(valid(s))
            def _():
                arrive(s, False)
                answer(s, 0, 0)

            return c

        lax.fori_loop(0, 2, one, 0)

    def near_hidden():
        for j in (0, wc):
            from_core(j)

        def one(side, c):
            s = z + 2 * side - 1

            @pl.when(valid(s))
            def _():
                hidden(s, 1, side)

            return c

        lax.fori_loop(0, 2, one, 0)

    def near_send(s, g):
        @pl.when(valid(s) & at_end(s))
        def _():
            for c in group(g):
                compact_copy(s, 1, c).start()

    def near_down(g):
        from_core(2 * wc + g)

        def one(side, carry):
            s = z + 2 * side - 1

            @pl.when(valid(s))
            def _():
                weight = share(s, 1)
                for c in group(g):
                    down(s, 1, side, c, weight)

                if g < wc - 1:
                    near_send(s, g)

            return carry

        lax.fori_loop(0, 2, one, 0)

    def group(g):
        return range(g * (nc // wc), (g + 1) * (nc // wc))

    far = jnp.where(z < groups // 2, groups - 1, 0)

    def far_step(g):
        size = nc // wc
        span = slice(g * size * cw, (g + 1) * size * cw)

        @pl.when(at_end(far))
        def _():
            for c in group(g):
                tok_wait(far, c)

        if g == 0:
            arrive(far, False)

        def one(e, carry):
            is_a, is_b, _, _ = masks(far, z, e * cap, cap)
            place = (is_a | is_b).astype(BF16)
            for c in group(g):
                chosen[:, c * cw : (c + 1) * cw] = dot(place, tok[far, c]).astype(BF16)
            for which, ref in enumerate((wg, wu)):
                part = dot(chosen[:, span], ref[e, span, :])
                gu[e, which] = part if g == 0 else gu[e, which] + part
            return carry

        lax.fori_loop(0, 2, one, 0)

    def far_hidden():
        def one(e, carry):
            gate = gu[e, 0]
            hid[2 + e] = (gate / (1.0 + jnp.exp(-gate)) * gu[e, 1]).astype(BF16)
            return carry

        lax.fori_loop(0, 2, one, 0)

    def both_down(s, at, g):
        weights = [share(s, e) for e in range(2)]
        for c in group(g):
            for e in range(2):
                down(s, e, at + e, c, weights[e])

        @pl.when(at_end(s))
        def _():
            for c in group(g):
                for e in range(2):
                    compact_copy(s, e, c).start()

    def far_down(g):
        both_down(far, 2, g)

    def further(d):
        def one(side, carry):
            s = z + d * (2 * side - 1)

            @pl.when(valid(s) & (s != far))
            def _():
                arrive(s, True)

                def first(e, c):
                    hidden(s, e, e)
                    return c

                lax.fori_loop(0, 2, first, 0)
                for g in range(wc):
                    both_down(s, 0, g)

            return carry

        lax.fori_loop(0, 2, one, 0)

    plan = {j: [] for j in range(pieces + 2)}

    def at(part, what, *args):
        plan[min(int(part * pieces / 12), pieces + 1)].append((what, args))

    def spread(start, end, what, *args, chunks=range(nc)):
        for c in chunks:
            at(start + (end - start) * c / nc, what, *args, c)

    at(0, own_first)
    at(1, send_rest)
    at(1, join_pair)
    at(1, hop, 0)
    for r in range(nt):
        at(2 + 2 * r / nt, attend, r)
    spread(3, 5, near_arrive)
    lead = 3 * nc // 8
    spread(3, 3, near_forward, chunks=range(lead))
    at(5, hop, 1)
    for i in range(1, groups - 2):
        spread(5.6, 11.2, far_forward, i)
    at(5, near_first)
    for i in range(2, groups - 1):
        at(11, hop, i)
    spread(11, 11, near_forward, chunks=range(lead, nc))
    at(9, near_hidden)
    for g in range(wc - 1):
        plan[2 * wc + 2 + g].append((near_down, (g,)))
        at(11, far_step, g)
    last = pieces + 1
    plan[last - 1] += [(far_step, (wc - 1,)), (far_hidden, ())]
    plan[last - 1] += [(far_down, (g,)) for g in range(wc // 2)]
    plan[last] += [(far_down, (g,)) for g in range(wc // 2, wc - 1)]
    plan[last] += [(near_down, (wc - 1,)), (far_down, (wc - 1,)), (hop, (groups - 1,))]

    for j in range(pieces + 2):
        if j < pieces:
            from_partner(j)
        if j >= 2:
            from_peers(j - 2)
        for what, args in plan[j]:
            what(*args)

    turns = [1, *range(groups - 1, 1, -1)]
    lag = 3

    @pl.when((z == 0) | (z == groups - 1))
    def _():
        attend_end()
        send_parts()
        answer(z, 1, 0)

    for d in turns[2:]:
        further(d)

    for s in (z - 1, z + 1):
        near_send(s, wc - 1)

    def last_turn(g):
        return max(turns.index(t) for t in (g, groups - 1 - g) if t)

    def events(t, carry):
        def during(start, what, *args):
            c = t - start

            @pl.when((c >= 0) & (c < nc))
            def _():
                what(*args, c)

        for step, turn in enumerate(turns[1:]):
            for h in range(1, min(turn, groups - 1)):
                @pl.when(z == groups - 1 - h)
                def _():
                    during(step * nc + lag * (h - 1), pass_on, groups - 1 - turn)

                @pl.when(z == h)
                def _():
                    during(step * nc + lag * (h - 1), pass_on, turn)

        @pl.when((z > 0) & (z < groups - 1))
        def _():
            for when, what in ((1, attend_end), (2, send_parts), (4, lambda: answer(z, 1, 0))):
                pl.when(t == when)(what)

        @pl.when(t == nc + 4)
        def _():
            mix()

        closing = jnp.int32(0)
        for g in range(groups):
            closing = jnp.where(z == g, (last_turn(g) - 1) * nc + lag * max(groups - 3, 1), closing)
        during(closing, own_end)
        return carry

    lax.fori_loop(0, max(groups - 2, 1) * nc + lag * max(groups - 3, 1), events, 0)

    for which in range(3):
        here = quarter(which, tp)
        remote(here, here, x_ss.at[which], w_rs.at[0, 0], (partner, tp)).wait_send()
        for o in range(nt // 2):
            if o:
                remote(here, here, y_ss.at[o, which], w_rs.at[0, 0], (partner, tp)).wait_send()
            remote(here, here, k_ss.at[o, which], w_rs.at[0, 0], (me, other)).wait_send()
    for copy in pair_copies(par):
        copy.wait_send()

    @pl.when(z + 1 < groups)
    def _():
        for copy in pre_copies():
            copy.wait_send()

    def sent(ref, sem):
        remote(ref, ref, sem, t_rs.at[0, 0], (me, other)).wait_send()

    def finish(s, carry):
        @pl.when((s <= z) & (z + 1 < groups))
        def _():
            sent(tok.at[s], t_ss.at[1, s])

        @pl.when((s >= z) & (z > 0))
        def _():
            sent(tok.at[s], t_ss.at[0, s])

        @pl.when(s != z)
        def _():
            info_copy(s, z).wait_send()

            @pl.when(at_end(s))
            def _():
                sent(ans.at[s], c_ss.at[s])

            @pl.when(jnp.logical_not(at_end(s)))
            def _():
                sent(rout.at[s], r_ss.at[s])

        return carry

    lax.fori_loop(0, groups, finish, 0)
    for i in range(1, nt):
        part_copy(lax.rem(tp + i, nt)).wait_send()


def shards(
    n, nt,
    memory_query_matrix, memory_key_matrix, memory_value_matrix,
    input_gate_logits, forget_gate_logits, forget_log_boosts,
    head_norm_scale, memory_output_matrix, projection_norm_scale,
    second_batch_rows, expert_prenorm_scale, selected_expert_index,
    group_route_probability, expert_choice_scores,
    expert_gate_matrix, expert_up_matrix, expert_down_matrix,
):
    length, hd = memory_query_matrix.shape
    tokens, width = second_batch_rows.shape
    hidden = expert_gate_matrix.shape[2]
    cap = 2 * selected_expert_index.shape[1] * tokens // n
    cap = -(-cap // 16) * 16
    rows = length // nt
    vm = pl.BlockSpec(memory_space=pltpu.VMEM)
    hbm = pl.BlockSpec(memory_space=pl.ANY)
    dma = pltpu.SemaphoreType.DMA
    slots = pltpu.VMEM((n, cap, width), BF16)
    groups = n // 2
    nc, wc = 8, 4
    cw = width // nc
    wide = -(-tokens // 128) * 128
    near = groups * tokens * width * 6 < 24 * 1024 * 1024 and nt % 2 == 0 and groups > 3
    if near:
        pair_w = (2, width, hidden)
        pieces = 3 * wc
        slot = (groups, nc, 2 * cap, cw)
        slot_in = (groups + 1, nc, 2 * cap, cw)
        line = (groups, nc, tokens, cw)
        line_in = (groups + 1, nc, tokens, cw)
        return pl.pallas_call(
            functools.partial(plane_kernel, n, nt, cap, nc, wc),
            out_shape=(
                pltpu.VMEM((rows, width), BF16),
                pltpu.VMEM((tokens, width), BF16),
            ),
            in_specs=[vm] * 7 + [hbm] + [vm] * 6 + [hbm] * 3,
            out_specs=(vm, vm),
            scratch_shapes=[
                pltpu.VMEM(pair_w, BF16),
                pltpu.VMEM(pair_w, BF16),
                pltpu.VMEM((2, hidden, width), BF16),
                pltpu.VMEM((hd, width), BF16),
                pltpu.VMEM(line, BF16),
                pltpu.VMEM((groups, 8, wide), F32),
                pltpu.VMEM((cap, width), BF16),
                pltpu.VMEM((4, cap, hidden), BF16),
                pltpu.VMEM(slot, BF16),
                pltpu.VMEM(slot_in, BF16),
                pltpu.VMEM(line, BF16),
                pltpu.VMEM(line_in, BF16),
                pltpu.VMEM((tokens, cw), F32),
                pltpu.VMEM((2, 2, cap, hidden), F32),
                pltpu.VMEM((2, hd, hd), BF16),
                pltpu.VMEM((2, 8, hd), F32),
                pltpu.VMEM((hd, hd), F32),
                pltpu.VMEM((8, hd), F32),
                pltpu.VMEM((2, hd, hd), BF16),
                pltpu.VMEM((2, 8, hd), F32),
                pltpu.VMEM((hd, hd), F32),
                pltpu.VMEM((length, hd), F32),
                pltpu.VMEM((length, 128), F32),
                pltpu.VMEM((length, hd), BF16),
                pltpu.VMEM((nt, rows, width), BF16),
                pltpu.VMEM((nt, rows, width), BF16),
                dma((4,)),
                dma((3,)), dma((nt // 2, 3)), dma((nt // 2, 3)), dma((nt, pieces)),
                dma((2, groups)), dma((groups, nc)),
                dma((groups,)), dma((groups,)),
                dma((groups,)), dma((groups,)), dma((groups + 1, nc)),
                dma, dma, dma, dma, dma, dma, dma, dma,
                dma((nt,)), dma((nt,)),
            ],
            compiler_params=pltpu.CompilerParams(
                collective_id=0, has_side_effects=True, vmem_limit_bytes=56 * 1024 * 1024
            ),
        )(
            memory_query_matrix, memory_key_matrix, memory_value_matrix,
            input_gate_logits, forget_gate_logits, forget_log_boosts,
            head_norm_scale[None], memory_output_matrix, projection_norm_scale[None],
            second_batch_rows, expert_prenorm_scale[None], selected_expert_index.T,
            group_route_probability[None], expert_choice_scores.T,
            expert_gate_matrix, expert_up_matrix, expert_down_matrix,
        )
    buffers = [
        slots, slots, slots, slots,
        pltpu.VMEM((tokens, width), BF16),
        pltpu.VMEM((tokens, width), F32),
    ]
    sems = [dma((n,))] * 4
    return pl.pallas_call(
        functools.partial(kernel, n, nt, cap),
        out_shape=(
            jax.ShapeDtypeStruct((rows, width), BF16),
            jax.ShapeDtypeStruct((tokens, width), BF16),
        ),
        in_specs=[vm] * 7 + [hbm] + [vm] * 6 + [hbm] * 3,
        out_specs=(vm, vm),
        scratch_shapes=[
            pltpu.VMEM((width, hidden), BF16),
            pltpu.VMEM((width, hidden), BF16),
            pltpu.VMEM((hidden, width), BF16),
            pltpu.VMEM((hd, width), BF16),
            *buffers,
            pltpu.VMEM((2, hd, hd), BF16),
            pltpu.VMEM((2, 8, hd), F32),
            pltpu.VMEM((n // 2, hd, hd), BF16),
            pltpu.VMEM((n // 2, 8, hd), F32),
            pltpu.VMEM((hd, hd), F32),
            pltpu.VMEM((length, hd), BF16),
            pltpu.VMEM((nt, rows, width), BF16),
            pltpu.VMEM((nt, rows, width), BF16),
            dma((4,)),
            *sems,
            dma, dma, dma, dma,
            dma((n // 2,)), dma((n // 2,)), dma((n // 2,)), dma((n // 2,)),
            dma((nt,)), dma((nt,)),
        ],
        compiler_params=pltpu.CompilerParams(
            collective_id=0, has_side_effects=True, vmem_limit_bytes=62 * 1024 * 1024
        ),
    )(
        memory_query_matrix, memory_key_matrix, memory_value_matrix,
        input_gate_logits, forget_gate_logits, forget_log_boosts,
        head_norm_scale[None], memory_output_matrix, projection_norm_scale[None],
        second_batch_rows, expert_prenorm_scale[None], selected_expert_index,
        group_route_probability[:, None], expert_choice_scores,
        expert_gate_matrix, expert_up_matrix, expert_down_matrix,
    )


def solution(mesh):
    return jax.shard_map(
        functools.partial(shards, mesh.shape["ep"], mesh.shape["tp"]),
        mesh=mesh,
        in_specs=(
            P("ep", "tp"), P("ep", "tp"), P("ep", "tp"),
            P("tp", "ep"), P("tp", "ep"), P("tp", "ep"),
            P("tp"), P(), P(),
            P(("ep", "tp"), None), P(), P(("ep", "tp"), None),
            P(("ep", "tp")), P(("ep", "tp"), None),
            P("ep", None, None), P("ep", None, None), P("ep", None, None),
        ),
        out_specs=(P(("ep", "tp"), None), P(("ep", "tp"), None)),
        check_vma=False,
    )
```

```python
import functools

import jax
import jax.numpy as jnp
from jax import lax
from jax.experimental import pallas as pl
from jax.experimental.pallas import tpu as pltpu
from jax.sharding import PartitionSpec as P

FLOOR = -1e30
EPS = 1e-06
MESH = pl.DeviceIdType.MESH
F32 = jnp.float32
BF16 = jnp.bfloat16


def rms(values, gain):
    squares = jnp.mean(values * values, axis=-1, keepdims=True)
    return values * lax.rsqrt(squares + EPS) * gain


def dot(a, b, dims=((1,), (0,)), precision=None):
    return lax.dot_general(a, b, (dims, ((), ())), preferred_element_type=F32, precision=precision)


def join(early, late):
    total_e, peak_e, mem_e, nor_e = early
    total_l, peak_l, mem_l, nor_l = late
    peak = jnp.maximum(total_l + peak_e, peak_l)
    fe = jnp.exp(total_l + peak_e - peak)
    fl = jnp.exp(peak_l - peak)
    return (total_e + total_l, peak, fe * mem_e + fl * mem_l, fe * nor_e + fl * nor_l)


def kernel(
    n, nt, cap,
    q_ref, k_ref, v_ref, ig_ref, fg_ref, fb_ref, hs_ref, wo_hbm, ps_ref,
    x_ref, es_ref, ids_ref, grp_ref, sc_ref, wg_hbm, wu_hbm, wd_hbm,
    mixed_ref, routed_ref,
    wg, wu, wd, wo, out, recv, ans, back, ffn, acc,
    cpair, spair, cgrp, sgrp, ent, head, pout, prec,
    wsem, d_ss, d_rs, a_ss, a_rs, c1s, c1r, s1s, s1r, c2s, c2r, s2s, s2r, p_ss, p_rs,
):
    me = lax.axis_index("ep")
    tp = lax.axis_index("tp")
    groups = n // 2
    grp = me // 2
    par = lax.rem(me, 2)
    partner = me + 1 - 2 * par
    tokens, width = x_ref.shape
    length, hd = q_ref.shape
    rows = mixed_ref.shape[0]

    barrier = pltpu.get_barrier_semaphore()

    def greet(i, c):
        pl.semaphore_signal(barrier, inc=1, device_id=(lax.rem(me + i, n), tp), device_id_type=MESH)
        return c

    lax.fori_loop(1, n, greet, 0)
    for j in range(1, nt):
        pl.semaphore_signal(barrier, inc=1, device_id=(me, lax.rem(tp + j, nt)), device_id_type=MESH)

    loads = [
        pltpu.make_async_copy(wg_hbm.at[0], wg, wsem.at[0]),
        pltpu.make_async_copy(wu_hbm.at[0], wu, wsem.at[1]),
        pltpu.make_async_copy(wd_hbm.at[0], wd, wsem.at[2]),
        pltpu.make_async_copy(wo_hbm.at[pl.ds(pl.multiple_of(tp * hd, hd), hd)], wo, wsem.at[3]),
    ]
    for load in loads:
        load.start()

    fg = fg_ref[...]
    lk = jnp.minimum(fg, 0.0) - jnp.log1p(jnp.exp(-jnp.abs(fg))) + fb_ref[...]
    rid = lax.broadcasted_iota(jnp.int32, (length, length), 0)
    cid = lax.broadcasted_iota(jnp.int32, (length, length), 1)
    upper = (rid <= cid).astype(F32)
    b_row = dot(jnp.broadcast_to(lk, (8, length)), upper, precision=lax.Precision.HIGHEST)[0:1]
    i_row = ig_ref[...]
    last = b_row[:, length - 1 : length]
    g_row = last - b_row + i_row
    m_loc = jnp.max(g_row, axis=-1, keepdims=True)
    which = lax.broadcasted_iota(jnp.int32, (128, length), 0)
    cols = jnp.where(which == 0, b_row, g_row).T
    b_col = cols[:, 0:1]
    g_col = cols[:, 1:2]
    kw = k_ref[...].astype(F32) * (jnp.exp(g_col - m_loc) * (hd**-0.5))
    c_loc = dot(kw.astype(BF16), v_ref[...], ((0,), (0,)))
    n_loc = jnp.sum(kw, axis=0, keepdims=True)
    stat_id = lax.broadcasted_iota(jnp.int32, (8, hd), 0)

    def stats(total, peak, nor):
        return jnp.where(stat_id == 0, nor, jnp.where(stat_id == 1, peak, total))

    cpair[par] = c_loc.astype(BF16)
    spair[par] = stats(last, m_loc, n_loc)

    pl.semaphore_wait(barrier, n - 1 + nt - 1)

    def pair_copies():
        return [
            pltpu.make_async_remote_copy(
                src_ref=cpair.at[par], dst_ref=cpair.at[par], send_sem=c1s, recv_sem=c1r,
                device_id=(partner, tp), device_id_type=MESH),
            pltpu.make_async_remote_copy(
                src_ref=spair.at[par], dst_ref=spair.at[par], send_sem=s1s, recv_sem=s1r,
                device_id=(partner, tp), device_id_type=MESH),
        ]

    for copy in pair_copies():
        copy.start()

    ffn[...] = rms(x_ref[...].astype(F32), es_ref[...]).astype(BF16)
    ids = ids_ref[...]
    first, second = ids[:, 0:1], ids[:, 1:2]
    lane_e = lax.broadcasted_iota(jnp.int32, (tokens, n), 1)
    named = ((lane_e == first) | (lane_e == second)).astype(F32)
    tr = lax.broadcasted_iota(jnp.int32, (tokens, tokens), 0)
    tc = lax.broadcasted_iota(jnp.int32, (tokens, tokens), 1)
    rank = dot((tc < tr).astype(BF16), named.astype(BF16))
    slot_a = first * cap + jnp.sum(jnp.where(lane_e == first, rank, 0.0), axis=1, keepdims=True).astype(jnp.int32)
    slot_b = second * cap + jnp.sum(jnp.where(lane_e == second, rank, 0.0), axis=1, keepdims=True).astype(jnp.int32)
    score = sc_ref[...]
    ex = jnp.exp(score - jnp.max(score, axis=-1, keepdims=True))
    route = grp_ref[...] * (ex / jnp.sum(ex, axis=-1, keepdims=True))
    rw_a, rw_b = route[:, 0:1], route[:, 1:2]
    lane_c = lax.broadcasted_iota(jnp.int32, (tokens, cap), 1)

    def pack(e):
        lane = lane_c + e * cap
        place = ((lane == slot_a) | (lane == slot_b)).astype(BF16)
        out[e] = dot(place, ffn[...], ((0,), (0,))).astype(BF16)

    def offset(i):
        return n // 2 + jnp.where(lax.rem(i, 2) == 0, i // 2, -((i + 1) // 2))

    def dispatch_copy(e):
        return pltpu.make_async_remote_copy(
            src_ref=out.at[e], dst_ref=recv.at[me], send_sem=d_ss.at[e], recv_sem=d_rs.at[me],
            device_id=(e, tp), device_id_type=MESH)

    def dispatch_arrival(s):
        return pltpu.make_async_remote_copy(
            src_ref=out.at[s], dst_ref=recv.at[s], send_sem=d_ss.at[s], recv_sem=d_rs.at[s],
            device_id=(s, tp), device_id_type=MESH)

    def answer_copy(s):
        return pltpu.make_async_remote_copy(
            src_ref=ans.at[s], dst_ref=back.at[me], send_sem=a_ss.at[s], recv_sem=a_rs.at[me],
            device_id=(s, tp), device_id_type=MESH)

    def answer_arrival(e):
        return pltpu.make_async_remote_copy(
            src_ref=ans.at[e], dst_ref=back.at[e], send_sem=a_ss.at[e], recv_sem=a_rs.at[e],
            device_id=(e, tp), device_id_type=MESH)

    for copy in pair_copies():
        copy.wait_send()
    def pair_arrival():
        return [
            pltpu.make_async_remote_copy(
                src_ref=cpair.at[1 - par], dst_ref=cpair.at[1 - par], send_sem=c1s, recv_sem=c1r,
                device_id=(partner, tp), device_id_type=MESH),
            pltpu.make_async_remote_copy(
                src_ref=spair.at[1 - par], dst_ref=spair.at[1 - par], send_sem=s1s, recv_sem=s1r,
                device_id=(partner, tp), device_id_type=MESH),
        ]

    for copy in pair_arrival():
        copy.wait_recv()

    def unpack(c, s):
        return (s[2:3], s[1:2], c.astype(F32), s[0:1])

    both = join(unpack(cpair[0], spair[0]), unpack(cpair[1], spair[1]))
    cgrp[grp] = both[2].astype(BF16)
    sgrp[grp] = stats(both[0], both[1], both[3])

    def group_copies(g):
        to = (g * 2 + par, tp)
        return [
            pltpu.make_async_remote_copy(
                src_ref=cgrp.at[grp], dst_ref=cgrp.at[grp], send_sem=c2s.at[g], recv_sem=c2r.at[grp],
                device_id=to, device_id_type=MESH),
            pltpu.make_async_remote_copy(
                src_ref=sgrp.at[grp], dst_ref=sgrp.at[grp], send_sem=s2s.at[g], recv_sem=s2r.at[grp],
                device_id=to, device_id_type=MESH),
        ]

    def group_arrivals(g):
        at = (g * 2 + par, tp)
        return [
            pltpu.make_async_remote_copy(
                src_ref=cgrp.at[g], dst_ref=cgrp.at[g], send_sem=c2s.at[g], recv_sem=c2r.at[g],
                device_id=at, device_id_type=MESH),
            pltpu.make_async_remote_copy(
                src_ref=sgrp.at[g], dst_ref=sgrp.at[g], send_sem=s2s.at[g], recv_sem=s2r.at[g],
                device_id=at, device_id_type=MESH),
        ]

    def send_group(g, c):
        for copy in group_copies(g):
            copy.start()
        return c

    lax.fori_loop(grp + 1, groups, send_group, 0)

    def send_tokens(i, c):
        e = lax.rem(me + offset(i), n)
        pack(e)
        dispatch_copy(e).start()
        return c

    lax.fori_loop(0, n - 1, send_tokens, 0)
    pack(me)
    for load in loads:
        load.wait()

    def expert(chosen):
        gate = dot(chosen, wg[...])
        up = dot(chosen, wu[...])
        hidden = (gate / (1.0 + jnp.exp(-gate)) * up).astype(BF16)
        return dot(hidden, wd[...]).astype(BF16)

    ans[me] = expert(out[me])

    ent[...] = jnp.zeros(ent.shape, F32)
    row1 = jnp.zeros((1, hd), F32)

    def enter(g, carry):
        total, peak, nor = carry
        for copy in group_arrivals(g):
            copy.wait_recv()
        total, peak, mem, nor = join((total, peak, ent[...], nor), unpack(cgrp[g], sgrp[g]))
        ent[...] = mem
        return total, peak, nor

    total, peak, nor = lax.fori_loop(0, grp, enter, (row1, row1 + FLOOR, row1))
    joined = join((total, peak, ent[...], nor), unpack(cpair[0], spair[0]))
    odd = par == 1
    m_in = jnp.where(odd, joined[1], peak)
    n_in = jnp.where(odd, joined[3], nor)
    c_in = jnp.where(odd, joined[2], ent[...])

    carried = b_col + m_in[:, 0:1]
    decay = jnp.where(cid <= rid, b_col - b_row + i_row, -jnp.inf)
    peaks = jnp.maximum(carried, jnp.max(decay, axis=-1, keepdims=True))
    across = jnp.exp(carried - peaks)
    scores = dot(q_ref[...], k_ref[...], ((1,), (1,))) * (hd**-0.5) * jnp.exp(decay - peaks)
    qf = q_ref[...].astype(F32)
    den = jnp.sum(scores, axis=-1, keepdims=True) + across * jnp.sum(qf * n_in, axis=-1, keepdims=True)
    num = dot(scores.astype(BF16), v_ref[...]) + across * dot(q_ref[...], c_in.astype(BF16))
    cell = num / jnp.maximum(jnp.abs(den), jnp.exp(-peaks))
    head[...] = (cell * hs_ref[...]).astype(BF16)

    def part_copy(j):
        return pltpu.make_async_remote_copy(
            src_ref=pout.at[j], dst_ref=prec.at[tp], send_sem=p_ss.at[j], recv_sem=p_rs.at[tp],
            device_id=(me, j), device_id_type=MESH)

    def part_arrival(j):
        return pltpu.make_async_remote_copy(
            src_ref=pout.at[j], dst_ref=prec.at[j], send_sem=p_ss.at[j], recv_sem=p_rs.at[j],
            device_id=(me, j), device_id_type=MESH)

    def project(j):
        pout[j] = dot(head[pl.ds(pl.multiple_of(j * rows, rows), rows), :], wo[...]).astype(BF16)

    def send_part(i, c):
        j = lax.rem(tp + i, nt)
        project(j)
        part_copy(j).start()
        return c

    lax.fori_loop(1, nt, send_part, 0)
    project(tp)

    def serve(i, c):
        s = lax.rem(me - offset(i) + n, n)
        dispatch_arrival(s).wait_recv()
        ans[s] = expert(recv[s])
        answer_copy(s).start()
        return c

    lax.fori_loop(0, n - 1, serve, 0)

    def mix(i, total):
        j = lax.rem(tp + i, nt)
        part_arrival(j).wait_recv()
        return total + prec[j].astype(F32)

    projected = pout[tp].astype(F32)
    for i in range(1, nt):
        projected = mix(i, projected)
    mixed_ref[...] = rms(projected, ps_ref[...]).astype(BF16)

    def weigh(e, block):
        lane = lane_c + e * cap
        w = jnp.where(lane == slot_a, rw_a, jnp.where(lane == slot_b, rw_b, 0.0))
        high = w.astype(BF16)
        low = (w - high.astype(F32)).astype(BF16)
        return dot(high, block) + dot(low, block)

    acc[...] = weigh(me, ans[me])

    def collect(i, c):
        e = lax.rem(me + offset(i), n)
        answer_arrival(e).wait_recv()
        acc[...] += weigh(e, back[e])
        return c

    lax.fori_loop(0, n - 1, collect, 0)
    routed_ref[...] = acc[...].astype(BF16)

    def finish(i, c):
        e = lax.rem(me + i, n)
        dispatch_copy(e).wait_send()
        answer_copy(e).wait_send()
        return c

    lax.fori_loop(1, n, finish, 0)

    def finish_group(g, c):
        for copy in group_copies(g):
            copy.wait_send()
        return c

    lax.fori_loop(grp + 1, groups, finish_group, 0)
    for i in range(1, nt):
        part_copy(lax.rem(tp + i, nt)).wait_send()


def plane_kernel(
    n, nt, cap, nc, wc,
    q_ref, k_ref, v_ref, ig_ref, fg_ref, fb_ref, hs_ref, wo_hbm, ps_ref,
    x_ref, es_ref, ids_ref, grp_ref, sc_ref, wg_hbm, wu_hbm, wd_hbm,
    mixed_ref, routed_ref,
    wg, wu, wd, wo, tok, info, chosen, hid, ans, cin, rout, rin, acc, gu,
    cpair, spair, cgrp, sgrp, cpre, spre, ent, num, stat, head, pout, prec,
    wsem, x_ss, y_ss, k_ss, w_rs, t_ss, t_rs, i_ss, i_rs, c_ss, r_ss, r_rs,
    c1s, c1r, s1s, s1r, c2s, c2r, s2s, s2r, p_ss, p_rs,
):
    me = lax.axis_index("ep")
    tp = lax.axis_index("tp")
    groups = n // 2
    z = me // 2
    par = lax.rem(me, 2)
    partner = me + 1 - 2 * par
    other = tp + 1 - 2 * lax.rem(tp, 2)
    tokens, width = x_ref.shape
    length, hd = q_ref.shape
    rows = mixed_ref.shape[0]
    cw = width // nc
    pieces = 3 * wc

    def remote(src, dst, ss, rs, to):
        return pltpu.make_async_remote_copy(
            src_ref=src, dst_ref=dst, send_sem=ss, recv_sem=rs, device_id=to, device_id_type=MESH)

    barrier = pltpu.get_barrier_semaphore()

    def greet(i, c):
        pl.semaphore_signal(barrier, inc=1, device_id=(lax.rem(me + i, n), tp), device_id_type=MESH)
        return c

    lax.fori_loop(1, n, greet, 0)
    for j in range(1, nt):
        pl.semaphore_signal(barrier, inc=1, device_id=(me, lax.rem(tp + j, nt)), device_id_type=MESH)

    loads = [
        pltpu.make_async_copy(wg_hbm.at[0], wg.at[0], wsem.at[0]),
        pltpu.make_async_copy(wu_hbm.at[0], wu.at[0], wsem.at[1]),
        pltpu.make_async_copy(wd_hbm.at[0], wd.at[0], wsem.at[2]),
        pltpu.make_async_copy(wo_hbm.at[pl.ds(pl.multiple_of(tp * hd, hd), hd)], wo, wsem.at[3]),
    ]
    for load in loads:
        load.start()

    def piece(ref, lead, part, j):
        which, at = divmod(j, wc)
        if which < 2:
            quarter = ref[which].shape[1] // nt
            step = quarter // wc
            return ref[which].at[lead, pl.ds(pl.multiple_of(part * quarter + at * step, step), step)]
        quarter = ref[2].shape[1] // nt
        step = width // wc
        return ref[2].at[lead, pl.ds(pl.multiple_of(part * quarter, quarter), quarter), pl.ds(at * step, step)]

    held = (wg, wu, wd)
    given = (wg_hbm, wu_hbm, wd_hbm)

    def x_copy(j):
        return remote(piece(given, 0, tp, j), piece(held, 1, tp, j), x_ss.at[j // wc], w_rs.at[tp, j], (partner, tp))

    def y_copy(o, j):
        here = piece(held, 1, tp, j)
        return remote(here, here, y_ss.at[o, j // wc], w_rs.at[tp, j], (me, lax.rem(tp + 2 * o, nt)))

    def core_copy(part, j):
        here = piece(held, 1, part, j)
        sem = w_rs.at[part, j // wc * wc if j < 2 * wc else j]
        return remote(here, here, k_ss.at[part // 2, j // wc], sem, (me, other))

    def weight_wait(part, j):
        here = piece(held, 1, part, j)
        remote(here, here, x_ss.at[j // wc], w_rs.at[part, j], (me, other)).wait_recv()

    def quarter(which, part):
        step = held[which].shape[1] // nt
        return held[which].at[1, pl.ds(pl.multiple_of(part * step, step), step)]

    def from_partner(j):
        weight_wait(tp, j)
        for o in range(1, nt // 2):
            y_copy(o, j).start()
        core_copy(tp, j).start()

    def from_peers(j):
        for o in range(1, nt // 2):
            part = lax.rem(tp + 2 * o, nt)
            weight_wait(part, j)
            core_copy(part, j).start()

    def from_core(j):
        for o in range(nt // 2):
            part = lax.rem(other + 2 * o, nt)
            if j < 2 * wc:
                here = quarter(j // wc, part)
                remote(here, here, x_ss.at[0], w_rs.at[part, j], (me, other)).wait_recv()
            else:
                weight_wait(part, j)

    def tok_copy(up, s, c):
        here = tok.at[s, c]
        return remote(here, here, t_ss.at[up, s], t_rs.at[s, c], ((z - 1 + 2 * up) * 2 + par, tp))

    def tok_wait(s, c):
        here = tok.at[s, c]
        remote(here, here, t_ss.at[0, s], t_rs.at[s, c], (me, other)).wait_recv()

    def send_own(c):
        @pl.when(z + 1 < groups)
        def _():
            tok_copy(1, z, c).start()

        @pl.when(z > 0)
        def _():
            tok_copy(0, z, c).start()

    def near_arrive(c):
        @pl.when(z > 0)
        def _():
            tok_wait(z - 1, c)

            @pl.when((z == 1) & (z + 1 < groups))
            def _():
                tok_copy(1, z - 1, c).start()

        @pl.when(z + 1 < groups)
        def _():
            tok_wait(z + 1, c)

            @pl.when((z == groups - 2) & (z > 0))
            def _():
                tok_copy(0, z + 1, c).start()

    def near_forward(c):
        @pl.when((z >= 2) & (z + 1 < groups))
        def _():
            tok_copy(1, z - 1, c).start()

        @pl.when((z <= groups - 3) & (z > 0))
        def _():
            tok_copy(0, z + 1, c).start()

    def far_forward(i, c):
        @pl.when((i < z) & (z + 1 < groups))
        def _():
            tok_wait(i - 1, c)
            tok_copy(1, i - 1, c).start()

        @pl.when((i < groups - 1 - z) & (z > 0))
        def _():
            tok_wait(groups - i, c)
            tok_copy(0, groups - i, c).start()

    normed = rms(x_ref[...].astype(F32), es_ref[...]).astype(BF16)
    for c in range(nc):
        tok[z, c] = normed[:, c * cw : (c + 1) * cw]

    pl.semaphore_wait(barrier, n - 1 + nt - 1)
    early = 5 * nc // 8
    for c in range(early):
        send_own(c)
    for j in range(2):
        x_copy(j).start()

    first, second = ids_ref[0:1, :], ids_ref[1:2, :]
    sub_e = lax.broadcasted_iota(jnp.int32, (n, tokens), 0)
    named = ((sub_e == first) | (sub_e == second)).astype(BF16)
    tr = lax.broadcasted_iota(jnp.int32, (tokens, tokens), 0)
    tc = lax.broadcasted_iota(jnp.int32, (tokens, tokens), 1)
    rank = dot(named, (tr < tc).astype(BF16))
    slot_a = first.astype(F32) * cap + jnp.sum(jnp.where(sub_e == first, rank, 0.0), axis=0, keepdims=True)
    slot_b = second.astype(F32) * cap + jnp.sum(jnp.where(sub_e == second, rank, 0.0), axis=0, keepdims=True)
    score_a, score_b = sc_ref[0:1, :], sc_ref[1:2, :]
    top = jnp.maximum(score_a, score_b)
    ex_a, ex_b = jnp.exp(score_a - top), jnp.exp(score_b - top)
    rw_a = grp_ref[...] * (ex_a / (ex_a + ex_b))
    rw_b = grp_ref[...] * (ex_b / (ex_a + ex_b))
    sub_i = lax.broadcasted_iota(jnp.int32, (8, tokens), 0)
    table = jnp.where(sub_i == 0, slot_a, jnp.where(sub_i == 1, slot_b,
        jnp.where(sub_i == 2, rw_a, jnp.where(sub_i == 3, rw_b, 0.0))))
    info[z] = jnp.zeros(info.shape[1:], F32)
    info[z, :, 0:tokens] = table

    def info_copy(g, s):
        return remote(info.at[s], info.at[s], i_ss.at[g], i_rs.at[s], (g * 2 + par, tp))

    def send_info(j, c):
        info_copy(lax.rem(z + j, groups), z).start()
        return c

    lax.fori_loop(1, groups, send_info, 0)

    fg = fg_ref[...]
    lk = jnp.minimum(fg, 0.0) - jnp.log1p(jnp.exp(-jnp.abs(fg))) + fb_ref[...]
    rid = lax.broadcasted_iota(jnp.int32, (length, length), 0)
    cid = lax.broadcasted_iota(jnp.int32, (length, length), 1)
    upper = (rid <= cid).astype(F32)
    b_row = dot(jnp.broadcast_to(lk, (8, length)), upper, precision=lax.Precision.HIGHEST)[0:1]
    i_row = ig_ref[...]
    last = b_row[:, length - 1 : length]
    g_row = last - b_row + i_row
    m_loc = jnp.max(g_row, axis=-1, keepdims=True)
    which_row = lax.broadcasted_iota(jnp.int32, (128, length), 0)
    stat[...] = jnp.where(which_row == 0, b_row, g_row).T
    kw = k_ref[...].astype(F32) * (jnp.exp(stat[:, 1:2] - m_loc) * (hd**-0.5))
    n_loc = jnp.sum(kw, axis=0, keepdims=True)
    stat_id = lax.broadcasted_iota(jnp.int32, (8, hd), 0)

    def stats(total, peak, nor):
        return jnp.where(stat_id == 0, nor, jnp.where(stat_id == 1, peak, total))

    def unpack(c, s):
        return (s[2:3], s[1:2], c.astype(F32), s[0:1])

    cpair[par] = dot(kw.astype(BF16), v_ref[...], ((0,), (0,))).astype(BF16)
    spair[par] = stats(last, m_loc, n_loc)

    def pair_copies(at):
        return [
            remote(cpair.at[at], cpair.at[at], c1s, c1r, (partner, tp)),
            remote(spair.at[at], spair.at[at], s1s, s1r, (partner, tp)),
        ]

    for copy in pair_copies(par):
        copy.start()
    for j in range(2, pieces):
        x_copy(j).start()
    def send_rest():
        for c in range(early, nc):
            send_own(c)

    def pre_copies():
        to = ((z + 1) * 2 + par, tp)
        return [
            remote(cpre.at[1], cpre.at[0], c2s, c2r, to),
            remote(spre.at[1], spre.at[0], s2s, s2r, to),
        ]

    def join_pair():
        for copy in pair_copies(1 - par):
            copy.wait_recv()
        both = join(unpack(cpair[0], spair[0]), unpack(cpair[1], spair[1]))
        cgrp[...] = both[2]
        sgrp[...] = stats(both[0], both[1], both[3])

    def hop(i):
        @pl.when(z == i)
        def _():
            if i:
                for copy in pre_copies():
                    copy.wait_recv()
                before = unpack(cpre[0], spre[0])
                ent[...] = before[2]
                sgate = spre[0]
            else:
                ent[...] = jnp.zeros(ent.shape, F32)
                row1 = jnp.zeros((1, hd), F32)
                sgate = stats(row1, row1 + FLOOR, row1)
                spre[0] = sgate
            if i + 1 < groups:
                out = join((sgate[2:3], sgate[1:2], ent[...], sgate[0:1]), unpack(cgrp[...], sgrp[...]))
                cpre[1] = out[2].astype(BF16)
                spre[1] = stats(out[0], out[1], out[3])
                for copy in pre_copies():
                    copy.start()

    rid_b = lax.broadcasted_iota(jnp.int32, (rows, length), 0)
    cid_b = lax.broadcasted_iota(jnp.int32, (rows, length), 1)

    def attend(r):
        at, end = r * rows, (r + 1) * rows
        decay = jnp.where(
            cid_b[:, :end] <= rid_b[:, :end] + at, stat[at:end, 0:1] - b_row[:, :end] + i_row[:, :end], -jnp.inf)
        peak = jnp.max(decay, axis=-1, keepdims=True)
        scores = dot(q_ref[at:end], k_ref[0:end], ((1,), (1,))) * (hd**-0.5) * jnp.exp(decay - peak)
        stat[at:end, 2:3] = peak
        stat[at:end, 3:4] = jnp.sum(scores, axis=-1, keepdims=True)
        num[at:end] = dot(scores.astype(BF16), v_ref[0:end])

    def attend_end():
        pre = (spre[0, 2:3], spre[0, 1:2], ent[...], spre[0, 0:1])
        joined = join(pre, unpack(cpair[0], spair[0]))
        odd = par == 1
        m_in = jnp.where(odd, joined[1], pre[1])
        n_in = jnp.where(odd, joined[3], pre[3])
        c_in = jnp.where(odd, joined[2], pre[2]).astype(BF16)
        for r in range(nt):
            at, end = r * rows, (r + 1) * rows
            carried = stat[at:end, 0:1] + m_in[:, 0:1]
            local = stat[at:end, 2:3]
            peaks = jnp.maximum(carried, local)
            across = jnp.exp(carried - peaks)
            within = jnp.exp(local - peaks)
            qf = q_ref[at:end].astype(F32)
            den = within * stat[at:end, 3:4] + across * jnp.sum(qf * n_in, axis=-1, keepdims=True)
            top = within * num[at:end] + across * dot(q_ref[at:end], c_in)
            cell = top / jnp.maximum(jnp.abs(den), jnp.exp(-peaks))
            head[at:end] = (cell * hs_ref[...]).astype(BF16)

    def part_copy(j):
        return remote(pout.at[j], prec.at[tp], p_ss.at[j], p_rs.at[tp], (me, j))

    def part_arrival(j):
        return remote(pout.at[j], prec.at[j], p_ss.at[j], p_rs.at[j], (me, j))

    def project(j):
        pout[j] = dot(head[pl.ds(pl.multiple_of(j * rows, rows), rows), :], wo[...]).astype(BF16)

    def send_part(i, c):
        j = lax.rem(tp + i, nt)
        project(j)
        part_copy(j).start()
        return c

    def send_parts():
        lax.fori_loop(1, nt, send_part, 0)
        project(tp)

    def mix():
        total = pout[tp].astype(F32)
        for i in range(1, nt):
            j = lax.rem(tp + i, nt)
            part_arrival(j).wait_recv()
            total = total + prec[j].astype(F32)
        mixed_ref[...] = rms(total, ps_ref[...]).astype(BF16)

    def masks(s, plane, start, count):
        table = info[s]
        slot = lax.broadcasted_iota(jnp.int32, (count, tokens), 0) + start
        own = (plane * 2 + par) * cap
        beside = (plane * 2 + 1 - par) * cap
        slot = jnp.where(slot < cap, own + slot, beside + slot - cap).astype(F32)
        return slot == table[0:1, 0:tokens], slot == table[1:2, 0:tokens], table[2:3, 0:tokens], table[3:4, 0:tokens]

    def hidden(s, e, at):
        is_a, is_b, _, _ = masks(s, z, e * cap, cap)
        place = (is_a | is_b).astype(BF16)
        for c in range(nc):
            chosen[:, c * cw : (c + 1) * cw] = dot(place, tok[s, c]).astype(BF16)
        gate = dot(chosen[...], wg[e])
        up = dot(chosen[...], wu[e])
        hid[at] = (gate / (1.0 + jnp.exp(-gate)) * up).astype(BF16)

    def share(s, e):
        is_a, is_b, w_a, w_b = masks(s, z, e * cap, cap)
        return jnp.sum(jnp.where(is_a, w_a, jnp.where(is_b, w_b, 0.0)), axis=1, keepdims=True)

    def half_of(e):
        return pl.ds(pl.multiple_of(e * cap, 16), cap)

    def down(s, e, at, c, weight):
        answer = dot(hid[at], wd[e, :, c * cw : (c + 1) * cw]) * weight
        ans[s, c, half_of(e), :] = answer.astype(BF16)

    def ret_to(s):
        below = s < z
        to = jnp.where(below, z - 1, z + 1)
        slot = jnp.where((to == s) & jnp.logical_not(below), groups, s)
        return below, to, slot

    def compact_copy(s, e, c):
        _, to, slot = ret_to(s)
        half = half_of(e)
        return remote(ans.at[s, c, half], cin.at[slot, c, half], c_ss.at[s], r_rs.at[slot, c], (to * 2 + par, tp))

    def compact_wait(slot, c):
        remote(ans.at[0, c], cin.at[slot, c], c_ss.at[0], r_rs.at[slot, c], (me, other)).wait_recv()

    def sum_copy(s, c):
        _, to, slot = ret_to(s)
        return remote(rout.at[s, c], rin.at[slot, c], r_ss.at[s], r_rs.at[slot, c], (to * 2 + par, tp))

    def sum_wait(slot, c):
        remote(rout.at[0, c], rin.at[slot, c], r_ss.at[0], r_rs.at[slot, c], (me, other)).wait_recv()

    def at_end(s):
        return jnp.where(s < z, z == groups - 1, z == 0)

    def valid(s):
        return (s >= 0) & (s < groups)

    def arrive(s, rows_too):
        if rows_too:
            @pl.when(at_end(s))
            def _():
                for c in range(nc):
                    tok_wait(s, c)

        remote(info.at[s], info.at[s], i_ss.at[0], i_rs.at[s], (me, other)).wait_recv()

    def answer(s, e, at):
        hidden(s, e, at)
        weight = share(s, e)
        for g in range(wc):
            for c in group(g):
                down(s, e, at, c, weight)

            @pl.when((s != z) & at_end(s))
            def _():
                for c in group(g):
                    compact_copy(s, e, c).start()

    def scatter(s, plane, block):
        is_a, is_b, _, _ = masks(s, plane, 0, 2 * cap)
        return dot((is_a | is_b).astype(BF16), block, ((0,), (0,)))

    def upstream(s, slot, near, last, c, put):
        @pl.when(near == last)
        def _():
            compact_wait(slot, c)
            put(scatter(s, last, cin[slot, c]))

        @pl.when(near != last)
        def _():
            sum_wait(slot, c)
            put(rin[slot, c].astype(F32))

    def pass_on(s, c):
        mine = scatter(s, z, ans[s, c])

        def put(more):
            rout[s, c] = (mine + more).astype(BF16)

        below = s < z
        upstream(s, s, jnp.where(below, z + 1, z - 1), jnp.where(below, groups - 1, 0), c, put)
        sum_copy(s, c).start()

    def own_end(c):
        acc[...] = scatter(z, z, ans[z, c])

        def put(more):
            acc[...] += more

        @pl.when(z < groups - 1)
        def _():
            upstream(z, z, z + 1, groups - 1, c, put)

        @pl.when(z > 0)
        def _():
            upstream(z, groups, z - 1, 0, c, put)

        routed_ref[:, pl.ds(pl.multiple_of(c * cw, cw), cw)] = acc[...].astype(BF16)

    def own_first():
        for load in loads:
            load.wait()
        answer(z, 0, 0)

    def near_first():
        def one(side, c):
            s = z + 2 * side - 1

            @pl.when(valid(s))
            def _():
                arrive(s, False)
                answer(s, 0, 0)

            return c

        lax.fori_loop(0, 2, one, 0)

    def near_hidden():
        for j in (0, wc):
            from_core(j)

        def one(side, c):
            s = z + 2 * side - 1

            @pl.when(valid(s))
            def _():
                hidden(s, 1, side)

            return c

        lax.fori_loop(0, 2, one, 0)

    def near_send(s, g):
        @pl.when(valid(s) & at_end(s))
        def _():
            for c in group(g):
                compact_copy(s, 1, c).start()

    def near_down(g):
        from_core(2 * wc + g)

        def one(side, carry):
            s = z + 2 * side - 1

            @pl.when(valid(s))
            def _():
                weight = share(s, 1)
                for c in group(g):
                    down(s, 1, side, c, weight)

                if g < wc - 2:
                    near_send(s, g)

            return carry

        lax.fori_loop(0, 2, one, 0)

    def group(g):
        return range(g * (nc // wc), (g + 1) * (nc // wc))

    far = jnp.where(z < groups // 2, groups - 1, 0)

    def far_step(g):
        size = nc // wc
        span = slice(g * size * cw, (g + 1) * size * cw)

        @pl.when(at_end(far))
        def _():
            for c in group(g):
                tok_wait(far, c)

        if g == 0:
            arrive(far, False)

        def one(e, carry):
            is_a, is_b, _, _ = masks(far, z, e * cap, cap)
            place = (is_a | is_b).astype(BF16)
            for c in group(g):
                chosen[:, c * cw : (c + 1) * cw] = dot(place, tok[far, c]).astype(BF16)
            for which, ref in enumerate((wg, wu)):
                part = dot(chosen[:, span], ref[e, span, :])
                gu[e, which] = part if g == 0 else gu[e, which] + part
            return carry

        lax.fori_loop(0, 2, one, 0)

    def far_hidden():
        def one(e, carry):
            gate = gu[e, 0]
            hid[2 + e] = (gate / (1.0 + jnp.exp(-gate)) * gu[e, 1]).astype(BF16)
            return carry

        lax.fori_loop(0, 2, one, 0)

    def both_down(s, at, g):
        weights = [share(s, e) for e in range(2)]
        for c in group(g):
            for e in range(2):
                down(s, e, at + e, c, weights[e])

        @pl.when(at_end(s))
        def _():
            for c in group(g):
                for e in range(2):
                    compact_copy(s, e, c).start()

    def far_down(g):
        both_down(far, 2, g)

    def further(d):
        def one(side, carry):
            s = z + d * (2 * side - 1)

            @pl.when(valid(s) & (s != far))
            def _():
                arrive(s, True)

                def first(e, c):
                    hidden(s, e, e)
                    return c

                lax.fori_loop(0, 2, first, 0)
                for g in range(wc):
                    both_down(s, 0, g)

            return carry

        lax.fori_loop(0, 2, one, 0)

    plan = {j: [] for j in range(pieces + 2)}

    def at(part, what, *args):
        plan[min(int(part * pieces / 12), pieces + 1)].append((what, args))

    def spread(start, end, what, *args, chunks=range(nc)):
        for c in chunks:
            at(start + (end - start) * c / nc, what, *args, c)

    at(0, own_first)
    at(1, send_rest)
    at(1, join_pair)
    at(1, hop, 0)
    for r in range(nt):
        at(2 + 2 * r / nt, attend, r)
    spread(3, 5, near_arrive)
    lead = 3 * nc // 8
    spread(3, 3, near_forward, chunks=range(lead))
    at(5, hop, 1)
    for i in range(1, groups - 2):
        spread(5.6, 11.2, far_forward, i)
    at(5, near_first)
    for i in range(2, groups - 1):
        at(11, hop, i)
    spread(11, 11, near_forward, chunks=range(lead, nc))
    at(9, near_hidden)
    for g in range(wc - 2):
        plan[2 * wc + 2 + g].append((near_down, (g,)))
    for g in range(wc - 1):
        plan[pieces - 3 + g].append((far_step, (g,)))
    last = pieces + 1
    plan[last - 2] += [(far_step, (wc - 1,)), (far_hidden, ())]
    plan[last - 2] += [(far_down, (g,)) for g in range(wc - 2)]
    plan[last - 1] += [(near_down, (wc - 2,))]
    plan[last] += [(far_down, (wc - 2,))]
    plan[last] += [(near_down, (wc - 1,)), (far_down, (wc - 1,)), (hop, (groups - 1,))]

    for j in range(pieces + 2):
        if j < pieces:
            from_partner(j)
        if j >= 2:
            from_peers(j - 2)
        for what, args in plan[j]:
            what(*args)

    turns = [1, *range(groups - 1, 1, -1)]
    lag = 3

    @pl.when((z == 0) | (z == groups - 1))
    def _():
        attend_end()
        send_parts()
        answer(z, 1, 0)

    for d in turns[2:]:
        further(d)

    for s in (z - 1, z + 1):
        for g in (wc - 2, wc - 1):
            near_send(s, g)

    def last_turn(g):
        return max(turns.index(t) for t in (g, groups - 1 - g) if t)

    def events(t, carry):
        def during(start, what, *args):
            c = t - start

            @pl.when((c >= 0) & (c < nc))
            def _():
                what(*args, c)

        for step, turn in enumerate(turns[1:]):
            for h in range(1, min(turn, groups - 1)):
                @pl.when(z == groups - 1 - h)
                def _():
                    during(step * nc + lag * (h - 1), pass_on, groups - 1 - turn)

                @pl.when(z == h)
                def _():
                    during(step * nc + lag * (h - 1), pass_on, turn)

        @pl.when((z > 0) & (z < groups - 1))
        def _():
            for when, what in ((1, attend_end), (2, send_parts), (4, lambda: answer(z, 1, 0))):
                pl.when(t == when)(what)

        @pl.when(t == nc + 4)
        def _():
            mix()

        closing = jnp.int32(0)
        for g in range(groups):
            closing = jnp.where(z == g, (last_turn(g) - 1) * nc + lag * max(groups - 3, 1), closing)
        during(closing, own_end)
        return carry

    lax.fori_loop(0, max(groups - 2, 1) * nc + lag * max(groups - 3, 1), events, 0)

    for which in range(3):
        here = quarter(which, tp)
        remote(here, here, x_ss.at[which], w_rs.at[0, 0], (partner, tp)).wait_send()
        for o in range(nt // 2):
            if o:
                remote(here, here, y_ss.at[o, which], w_rs.at[0, 0], (partner, tp)).wait_send()
            remote(here, here, k_ss.at[o, which], w_rs.at[0, 0], (me, other)).wait_send()
    for copy in pair_copies(par):
        copy.wait_send()

    @pl.when(z + 1 < groups)
    def _():
        for copy in pre_copies():
            copy.wait_send()

    def sent(ref, sem):
        remote(ref, ref, sem, t_rs.at[0, 0], (me, other)).wait_send()

    def finish(s, carry):
        @pl.when((s <= z) & (z + 1 < groups))
        def _():
            sent(tok.at[s], t_ss.at[1, s])

        @pl.when((s >= z) & (z > 0))
        def _():
            sent(tok.at[s], t_ss.at[0, s])

        @pl.when(s != z)
        def _():
            info_copy(s, z).wait_send()

            @pl.when(at_end(s))
            def _():
                sent(ans.at[s], c_ss.at[s])

            @pl.when(jnp.logical_not(at_end(s)))
            def _():
                sent(rout.at[s], r_ss.at[s])

        return carry

    lax.fori_loop(0, groups, finish, 0)
    for i in range(1, nt):
        part_copy(lax.rem(tp + i, nt)).wait_send()


def shards(
    n, nt,
    memory_query_matrix, memory_key_matrix, memory_value_matrix,
    input_gate_logits, forget_gate_logits, forget_log_boosts,
    head_norm_scale, memory_output_matrix, projection_norm_scale,
    second_batch_rows, expert_prenorm_scale, selected_expert_index,
    group_route_probability, expert_choice_scores,
    expert_gate_matrix, expert_up_matrix, expert_down_matrix,
):
    length, hd = memory_query_matrix.shape
    tokens, width = second_batch_rows.shape
    hidden = expert_gate_matrix.shape[2]
    cap = 2 * selected_expert_index.shape[1] * tokens // n
    cap = -(-cap // 16) * 16
    rows = length // nt
    vm = pl.BlockSpec(memory_space=pltpu.VMEM)
    hbm = pl.BlockSpec(memory_space=pl.ANY)
    dma = pltpu.SemaphoreType.DMA
    slots = pltpu.VMEM((n, cap, width), BF16)
    groups = n // 2
    nc, wc = 8, 4
    cw = width // nc
    wide = -(-tokens // 128) * 128
    near = groups * tokens * width * 6 < 24 * 1024 * 1024 and nt % 2 == 0 and groups > 3
    if near:
        pair_w = (2, width, hidden)
        pieces = 3 * wc
        slot = (groups, nc, 2 * cap, cw)
        slot_in = (groups + 1, nc, 2 * cap, cw)
        line = (groups, nc, tokens, cw)
        line_in = (groups + 1, nc, tokens, cw)
        return pl.pallas_call(
            functools.partial(plane_kernel, n, nt, cap, nc, wc),
            out_shape=(
                pltpu.VMEM((rows, width), BF16),
                pltpu.VMEM((tokens, width), BF16),
            ),
            in_specs=[vm] * 7 + [hbm] + [vm] * 6 + [hbm] * 3,
            out_specs=(vm, vm),
            scratch_shapes=[
                pltpu.VMEM(pair_w, BF16),
                pltpu.VMEM(pair_w, BF16),
                pltpu.VMEM((2, hidden, width), BF16),
                pltpu.VMEM((hd, width), BF16),
                pltpu.VMEM(line, BF16),
                pltpu.VMEM((groups, 8, wide), F32),
                pltpu.VMEM((cap, width), BF16),
                pltpu.VMEM((4, cap, hidden), BF16),
                pltpu.VMEM(slot, BF16),
                pltpu.VMEM(slot_in, BF16),
                pltpu.VMEM(line, BF16),
                pltpu.VMEM(line_in, BF16),
                pltpu.VMEM((tokens, cw), F32),
                pltpu.VMEM((2, 2, cap, hidden), F32),
                pltpu.VMEM((2, hd, hd), BF16),
                pltpu.VMEM((2, 8, hd), F32),
                pltpu.VMEM((hd, hd), F32),
                pltpu.VMEM((8, hd), F32),
                pltpu.VMEM((2, hd, hd), BF16),
                pltpu.VMEM((2, 8, hd), F32),
                pltpu.VMEM((hd, hd), F32),
                pltpu.VMEM((length, hd), F32),
                pltpu.VMEM((length, 128), F32),
                pltpu.VMEM((length, hd), BF16),
                pltpu.VMEM((nt, rows, width), BF16),
                pltpu.VMEM((nt, rows, width), BF16),
                dma((4,)),
                dma((3,)), dma((nt // 2, 3)), dma((nt // 2, 3)), dma((nt, pieces)),
                dma((2, groups)), dma((groups, nc)),
                dma((groups,)), dma((groups,)),
                dma((groups,)), dma((groups,)), dma((groups + 1, nc)),
                dma, dma, dma, dma, dma, dma, dma, dma,
                dma((nt,)), dma((nt,)),
            ],
            compiler_params=pltpu.CompilerParams(
                collective_id=0, has_side_effects=True, vmem_limit_bytes=56 * 1024 * 1024
            ),
        )(
            memory_query_matrix, memory_key_matrix, memory_value_matrix,
            input_gate_logits, forget_gate_logits, forget_log_boosts,
            head_norm_scale[None], memory_output_matrix, projection_norm_scale[None],
            second_batch_rows, expert_prenorm_scale[None], selected_expert_index.T,
            group_route_probability[None], expert_choice_scores.T,
            expert_gate_matrix, expert_up_matrix, expert_down_matrix,
        )
    buffers = [
        slots, slots, slots, slots,
        pltpu.VMEM((tokens, width), BF16),
        pltpu.VMEM((tokens, width), F32),
    ]
    sems = [dma((n,))] * 4
    return pl.pallas_call(
        functools.partial(kernel, n, nt, cap),
        out_shape=(
            jax.ShapeDtypeStruct((rows, width), BF16),
            jax.ShapeDtypeStruct((tokens, width), BF16),
        ),
        in_specs=[vm] * 7 + [hbm] + [vm] * 6 + [hbm] * 3,
        out_specs=(vm, vm),
        scratch_shapes=[
            pltpu.VMEM((width, hidden), BF16),
            pltpu.VMEM((width, hidden), BF16),
            pltpu.VMEM((hidden, width), BF16),
            pltpu.VMEM((hd, width), BF16),
            *buffers,
            pltpu.VMEM((2, hd, hd), BF16),
            pltpu.VMEM((2, 8, hd), F32),
            pltpu.VMEM((n // 2, hd, hd), BF16),
            pltpu.VMEM((n // 2, 8, hd), F32),
            pltpu.VMEM((hd, hd), F32),
            pltpu.VMEM((length, hd), BF16),
            pltpu.VMEM((nt, rows, width), BF16),
            pltpu.VMEM((nt, rows, width), BF16),
            dma((4,)),
            *sems,
            dma, dma, dma, dma,
            dma((n // 2,)), dma((n // 2,)), dma((n // 2,)), dma((n // 2,)),
            dma((nt,)), dma((nt,)),
        ],
        compiler_params=pltpu.CompilerParams(
            collective_id=0, has_side_effects=True, vmem_limit_bytes=62 * 1024 * 1024
        ),
    )(
        memory_query_matrix, memory_key_matrix, memory_value_matrix,
        input_gate_logits, forget_gate_logits, forget_log_boosts,
        head_norm_scale[None], memory_output_matrix, projection_norm_scale[None],
        second_batch_rows, expert_prenorm_scale[None], selected_expert_index,
        group_route_probability[:, None], expert_choice_scores,
        expert_gate_matrix, expert_up_matrix, expert_down_matrix,
    )


def solution(mesh):
    return jax.shard_map(
        functools.partial(shards, mesh.shape["ep"], mesh.shape["tp"]),
        mesh=mesh,
        in_specs=(
            P("ep", "tp"), P("ep", "tp"), P("ep", "tp"),
            P("tp", "ep"), P("tp", "ep"), P("tp", "ep"),
            P("tp"), P(), P(),
            P(("ep", "tp"), None), P(), P(("ep", "tp"), None),
            P(("ep", "tp")), P(("ep", "tp"), None),
            P("ep", None, None), P("ep", None, None), P("ep", None, None),
        ),
        out_specs=(P(("ep", "tp"), None), P(("ep", "tp"), None)),
        check_vma=False,
    )
```
